256 devices in a mesh: sp: 32 (over z, x), tp: 8 (over y, core).
Axes of the slice: x: 4, y: 4, z: 8, core: 2. Of those that a mesh axis runs over, the one named last changes fastest.
Arguments:
- activations: bfloat16 [16384, 1024], P(('sp', 'tp')), may hold values from -8 to 8, as said below
- input_gain: float32 [1024], replicated, may hold values from 0.5 to 1.5
- query_weight: bfloat16 [1024, 1024], P(None, 'tp'), may hold values from -0.1875 to 0.1875
- key_weight: bfloat16 [1024, 1024], P(None, 'tp'), may hold values from -0.375 to 0.375
- value_weight: bfloat16 [1024, 1024], P(None, 'tp'), may hold values from -0.1875 to 0.1875
- stop_offset: float32 [16], P('tp'), may hold values from -16 to 0, as said below
- output_weight: bfloat16 [1024, 1024], P('tp'), may hold values from -0.1875 to 0.1875
- output_gain: float32 [1024], replicated, may hold values from 0.5 to 1.5
Outputs:
- layer_out: bfloat16 [16384, 1024], P(('sp', 'tp'))
The draws below stay inside these ranges and needn't reach their ends.
Inputs may be any that keep to these rules, and one draw needn't show every extreme that they name: activations are noise of about unit size plus a mean vector of about unit size shared by each aligned block of 512 rows and different between runs; each row as a whole may also be scaled by a factor between 0.25 and 2; the result is clipped to the range. `stop_offset`: each entry equals minus the natural logarithm of 16384, minus 2, plus the natural logarithm of 3, plus a number between 0 and 0.7.
All inputs are finite; a program needn't handle non-finite values.
Results may differ from the reference program's by a relative error of at most 0.015.
Values may be sent and summed in bfloat16 or wider, within the bound.
A program may use at most 128 MiB of HBM per device.

```python
import jax
import jax.numpy as jnp
from jax import lax

D = 1024
HEADS = 16
HEAD_DIM = 64
TOK_DEV = 512
TOKENS = 16384


def draw_activations(key, part):
    noise_key, mean_key, scale_key = jax.random.split(key, 3)
    blocks = TOKENS // TOK_DEV
    noise_part = jax.random.normal(noise_key, (blocks, TOK_DEV, D), jnp.float32)
    block_means = jax.random.normal(mean_key, (blocks, 1, D), jnp.float32)
    combined = noise_part + block_means
    return jnp.clip(combined, -8.0, 8.0).reshape(TOKENS, D).astype(jnp.bfloat16)


def draw_stop_offset(key, part):
    center = -jnp.log(jnp.float32(TOKENS)) - 2.0 + jnp.log(jnp.float32(3.0))
    return center + jax.random.uniform(key, (HEADS,), jnp.float32, 0.0, 0.7)


def steps_of(own_key, dims, cuts, least, top_value):
    loudness, own = 1.0, jax.random.fold_in(own_key, 6)
    for position, parts in cuts:
        draws = jnp.exp(jax.random.uniform(jax.random.fold_in(own, position), (parts,), jnp.float32, least / len(cuts), top_value / len(cuts)))
        loudness = loudness * jnp.repeat(draws, dims[position] // parts).reshape([-1 if axis == position else 1 for axis in range(len(dims))])
    return loudness


def centred(rng, dims, width, most, cuts=(), kind=jnp.bfloat16):
    level = steps_of(rng, dims, cuts, -0.22, 0.18) if cuts else 1.0
    drawn = jax.random.normal(rng, dims, jnp.float32) * width * level
    return jnp.minimum(jnp.maximum(drawn, -most), most).astype(kind)


def setup_inputs(seed: int = 0) -> dict:
    arg_keys = jax.random.split(jax.random.key(seed), 9)
    return {
        "activations": draw_activations(jax.random.fold_in(arg_keys[8], 71), 0),
        "input_gain": jnp.clip(1.0 + 0.1 * jax.random.normal(arg_keys[1], (D,), jnp.float32), 0.5, 1.5),
        "query_weight": centred(arg_keys[2], (D, HEADS * HEAD_DIM), D ** -0.5, 0.1875, ((1, 8),)),
        "key_weight": centred(arg_keys[3], (D, HEADS * HEAD_DIM), (D // 4) ** -0.5, 0.375, ((1, 8),)),
        "value_weight": centred(arg_keys[4], (D, HEADS * HEAD_DIM), D ** -0.5, 0.1875, ((1, 8),)),
        "stop_offset": draw_stop_offset(jax.random.fold_in(arg_keys[8], 71), 0),
        "output_weight": centred(arg_keys[6], (HEADS * HEAD_DIM, D), (HEADS * HEAD_DIM) ** -0.5, 0.1875, ((0, 8),)),
        "output_gain": jnp.clip(1.0 + 0.1 * jax.random.normal(arg_keys[7], (D,), jnp.float32), 0.5, 1.5),
    }


epsilon = 1e-06

def scaled_rows(row_block, row_gain):
    widened = row_block.astype(jnp.float32)
    spread = lax.optimization_barrier(jnp.mean(widened * widened, axis=-1, keepdims=True))
    return (widened * lax.rsqrt(spread + epsilon) * row_gain).astype(jnp.bfloat16)

def reference(activations, input_gain, query_weight, key_weight, value_weight, stop_offset, output_weight, output_gain):
    normed = scaled_rows(activations, input_gain)
    query_rows = jnp.dot(normed, query_weight, preferred_element_type=jnp.float32).astype(jnp.bfloat16)
    key_rows = jnp.dot(normed, key_weight, preferred_element_type=jnp.float32).astype(jnp.bfloat16)
    value_rows = jnp.dot(normed, value_weight, preferred_element_type=jnp.float32).astype(jnp.bfloat16)
    blocks = TOKENS // TOK_DEV
    query_blocks = query_rows.reshape(blocks, TOK_DEV, HEADS, HEAD_DIM)
    key_blocks = key_rows.reshape(blocks, TOK_DEV, HEADS, HEAD_DIM)
    value_blocks = value_rows.reshape(blocks, TOK_DEV, HEADS, HEAD_DIM)
    score_scale = HEAD_DIM ** (-0.5)
    offsets = stop_offset.astype(jnp.float32)

    def attend_block(query_index):
        queries = query_blocks[query_index].astype(jnp.float32)
        first_query = query_index * TOK_DEV

        def per_key(key_index):

            def compute(unused):
                key_here = key_blocks[key_index].astype(jnp.float32)
                value_here = value_blocks[key_index].astype(jnp.float32)
                scores = jnp.einsum('thd,shd->hts', queries, key_here, precision=lax.Precision.HIGHEST)
                scores = scores * score_scale + offsets[:, None, None]
                query_pos = first_query + jnp.arange(TOK_DEV, dtype=jnp.int32)
                key_pos = key_index * TOK_DEV + jnp.arange(TOK_DEV, dtype=jnp.int32)
                earlier = key_pos[None, :] < query_pos[:, None]
                log_keep = jnp.where(earlier[None], jax.nn.log_sigmoid(-scores), 0.0)
                within = lax.cumsum(log_keep, axis=2, reverse=True) - log_keep
                weights = jnp.where(earlier[None], jnp.exp(jax.nn.log_sigmoid(scores) + within), 0.0)
                weights = weights.astype(jnp.bfloat16).astype(jnp.float32)
                shard_part = jnp.einsum('hts,shd->thd', weights, value_here, precision=lax.Precision.HIGHEST)
                return (shard_part, lax.optimization_barrier(jnp.sum(log_keep, axis=2)))

            def skipped(unused):
                return (jnp.zeros((TOK_DEV, HEADS, HEAD_DIM), jnp.float32), jnp.zeros((HEADS, TOK_DEV), jnp.float32))
            return lax.cond(key_index <= query_index, compute, skipped, 0)
        block_parts, totals = lax.map(per_key, jnp.arange(blocks, dtype=jnp.int32))
        prefix_sums = jnp.cumsum(totals, axis=0)
        factors = jnp.exp(prefix_sums[-1:] - prefix_sums)
        combined = jnp.einsum('bht,bthd->thd', factors, block_parts, precision=lax.Precision.HIGHEST)
        return combined.astype(jnp.bfloat16)
    attended = lax.map(attend_block, jnp.arange(blocks, dtype=jnp.int32))
    attended = attended.reshape(TOKENS, HEADS * HEAD_DIM)
    projected = jnp.dot(attended, output_weight, preferred_element_type=jnp.float32)
    return scaled_rows(projected, output_gain)
```

```python
import functools

import jax
import jax.numpy as jnp
from jax import lax
from jax.experimental import pallas as pl
from jax.experimental.pallas import tpu as pltpu
from jax.sharding import PartitionSpec as P

epsilon = 1e-06
log2e = 1.4426950408889634
MESH = pl.DeviceIdType.MESH
f32 = jnp.float32
bf16 = jnp.bfloat16
XS = 4
ZMAX = 63.0


def scaled_rows(widened, row_gain):
    spread = jnp.mean(widened * widened, axis=-1, keepdims=True)
    return (widened * lax.rsqrt(spread + epsilon) * row_gain).astype(bf16)


def layer_kernel(
    S,
    T,
    H,
    dh,
    act,
    gain_in,
    wq_hbm,
    wk_hbm,
    wv_hbm,
    off,
    wo_hbm,
    gain_out,
    out,
    wq,
    wk,
    wv,
    xg,
    wg,
    perm,
    kvb,
    qb,
    kvr,
    qr,
    offt,
    ws,
    acc,
    obuf,
    orecv,
    heads,
    x_send,
    x_recv,
    w_send,
    w_recv,
    kv_send,
    kv_recv,
    q_send,
    q_recv,
    o_send,
    o_recv,
    load,
):
    R = act.shape[0]
    B = R * T
    W = B // 2
    rows = wo_hbm.shape[0]
    Z = S // XS
    half_z = Z // 2
    s = lax.axis_index("sp")
    t = lax.axis_index("tp")
    z, x = s // XS, s % XS
    h = z // half_z
    mz = Z - 1 - z
    kz = jnp.where(h == 0, z, mz)
    y, c = t // 2, t % 2
    partner = y * 2 + 1 - c
    Y = T // 2

    def remote(src, dst, send, recv, dev):
        return pltpu.make_async_remote_copy(
            src_ref=src, dst_ref=dst, send_sem=send, recv_sem=recv, device_id=dev, device_id_type=MESH
        )

    started = []

    def go(copy):
        copy.start()
        started.append(copy)
        return copy

    def xrow(index):
        return xg.at[pl.ds(pl.multiple_of(index * R, R), R)]

    def wrow(index):
        return wg.at[pl.ds(pl.multiple_of(index * rows, rows), rows)]

    def x_copy(index, slot, dev):
        return remote(xrow(index), xrow(index), x_send.at[slot], x_recv.at[index], (s, dev))

    def w_copy(src, index, slot, dev):
        return remote(src, wrow(index), w_send.at[slot], w_recv.at[index], (s, dev))

    barrier = pltpu.get_barrier_semaphore()
    for d in range(1, S * T):
        other = (s * T + t + d) % (S * T)
        pl.semaphore_signal(barrier, inc=1, device_id=(other // T, other % T), device_id_type=MESH)
    loads = [
        pltpu.make_async_copy(wk_hbm, wk, load.at[0]),
        pltpu.make_async_copy(wv_hbm, wv, load.at[1]),
        pltpu.make_async_copy(wq_hbm, wq, load.at[2]),
        pltpu.make_async_copy(wo_hbm, wrow(t), load.at[3]),
    ]
    for copy in loads:
        copy.start()

    xg[pl.ds(pl.multiple_of(t * R, R), R)] = scaled_rows(act[...].astype(f32), gain_in[...])
    pl.semaphore_wait(barrier, S * T - 1)
    for e in range(1, Y):
        go(x_copy(t, e, ((y + e) % Y) * 2 + c))
    go(x_copy(t, 0, partner))

    token = lax.broadcasted_iota(jnp.int32, (B, B), 0)
    place = lax.broadcasted_iota(jnp.int32, (B, B), 1)
    perm[...] = (token == (place & (T - 1)) * R + (place >> (T.bit_length() - 1))).astype(f32).astype(bf16)
    whole = jnp.broadcast_to(off[h] * log2e, (16, B)).astype(f32)
    high = whole.astype(bf16).astype(f32)
    middle = (whole - high).astype(bf16).astype(f32)
    low = whole - high - middle
    part_row = lax.broadcasted_iota(jnp.int32, (16, B), 0)
    offt[...] = jnp.where(
        part_row == 0, high, jnp.where(part_row == 1, middle, jnp.where(part_row == 2, low, 0.0))
    ).astype(bf16)

    for e in range(1, Y):
        came = ((y + e) % Y) * 2 + c
        x_copy(came, 0, partner).wait_recv()
        go(x_copy(came, Y + e - 1, partner))
    for copy in loads:
        copy.wait()
    for e in range(1, Y):
        go(w_copy(wrow(t), t, e, ((y + e) % Y) * 2 + c))
    x_copy(partner, 0, partner).wait_recv()
    for e in range(1, Y):
        x_copy(((y + e) % Y) * 2 + 1 - c, 0, partner).wait_recv()

    rows_all = xg[...]
    keys = jnp.dot(rows_all, wk[...], preferred_element_type=f32).astype(bf16).astype(f32)
    values = jnp.dot(rows_all, wv[...], preferred_element_type=f32).astype(bf16).astype(f32)
    turned = jnp.concatenate([keys.T, values.T], axis=0).astype(bf16)
    placed = jnp.dot(turned, perm[...], preferred_element_type=f32)
    keys_placed = placed[: H * dh].T
    for i in range(H):
        cols = slice(i * dh, (i + 1) * dh)
        kvb[i, :W] = jnp.concatenate([keys_placed[:W, cols], keys_placed[W:, cols]], axis=1).astype(bf16)
        for part in range(4):
            piece = placed[(H + i) * dh : (H + i + 1) * dh, part * 128 : (part + 1) * 128]
            kvb[i, W + part * dh : W + (part + 1) * dh] = piece.astype(bf16)

    def kv_copy(src, row, col, slot, dev):
        return remote(src, kvr.at[row, col], kv_send.at[slot], kv_recv.at[row * XS + col], (dev, t))

    go(kv_copy(kvb.at[1 - h], h, x, 0, mz * XS + x))
    for e in (1, 3, 2):
        go(kv_copy(kvb.at[h], h, x, e, z * XS + (x + e) % XS))
    kvr[h, x] = kvb[h]

    queries = jnp.dot(rows_all, wq[...], preferred_element_type=f32) * (dh ** (-0.5) * log2e)
    q_turned = queries.T.astype(bf16)
    for i in range(H):
        qb[i] = q_turned[i * dh : (i + 1) * dh]
    qr[z] = qb[h]

    def q_copy(i, depth):
        dev = depth if i == 0 else Z - 1 - depth
        return dev, remote(qb.at[i], qr.at[z], q_send.at[i * half_z + depth], q_recv.at[z], (dev * XS + x, t))

    def q_extra(i):
        dev = mz if i == 0 else z
        return remote(qb.at[i], qr.at[Z], q_send.at[H * half_z + i], q_recv.at[Z], (dev * XS + XS - 1 - x, t))

    def each_q(act_on):
        @pl.when(h == 1)
        def _():
            for i in range(H):
                act_on(q_extra(i))

        for depth in range(half_z - 1, -1, -1):
            for i in range(H):
                dev, copy = q_copy(i, depth)

                @pl.when(jnp.logical_and(depth <= z, dev != z))
                def _():
                    act_on(copy)

    each_q(lambda copy: copy.start())

    def kv_wait(row, col):
        @pl.when(jnp.logical_or(row != h, col != x))
        def _():
            remote(kvb.at[0], kvr.at[row, col], kv_send.at[0], kv_recv.at[row * XS + col], (s, t)).wait_recv()

    def q_wait(slot):
        @pl.when(slot != z)
        def _():
            remote(qb.at[0], qr.at[slot], q_send.at[0], q_recv.at[slot], (s, t)).wait_recv()

    lane = lax.broadcasted_iota(jnp.int32, (16, 128), 1)
    ones = (lane < 3).astype(f32).astype(bf16)
    zeros = jnp.zeros((dh, W), bf16)
    pad = jnp.zeros((112, W), bf16)

    def weigh(row, col, slot, j, masked):
        sl = slice(j * W, (j + 1) * W)
        run = jnp.ones((8, W), f32)
        if masked:
            ahead = (
                lax.broadcasted_iota(jnp.int32, (8, W), 1)
                + j * W
                - R * lax.broadcasted_iota(jnp.int32, (8, W), 0)
            )
        lhs = jnp.concatenate([kvr[row, col, :W], jnp.tile(ones, (W // 16, 1))], axis=1)
        for part in (1, 0):
            q = qr[slot, :, sl]
            stack = [q, zeros] if part == 0 else [zeros, q]
            rhs = jnp.concatenate(stack + [offt[:, sl], pad], axis=0)
            score = jnp.minimum(jnp.dot(lhs, rhs, preferred_element_type=f32), ZMAX)
            for v in range(W // 8 - 2, -1, -2):
                e0 = jnp.exp2(score[8 * v : 8 * v + 8])
                e1 = jnp.exp2(score[8 * v + 8 : 8 * v + 16])
                if masked:
                    place_v = part * (W // 8) + v
                    e0 = jnp.where(ahead > place_v, e0, 0.0)
                    e1 = jnp.where(ahead > place_v + 1, e1, 0.0)
                u0, u1 = 1.0 + e0, 1.0 + e1
                left = run * (1.0 / (u0 * u1))
                first = e0 * left
                second = e1 * (u0 * left)
                run = left
                base = part * W + 8 * v
                ws[j, base : base + 16] = jnp.concatenate([first, second], axis=0).astype(bf16)
        later = [None] * 8
        total = jnp.ones((1, W), f32)
        for i in range(7, -1, -1):
            later[i] = total
            total = total * run[i : i + 1]
        return jnp.concatenate(later + later, axis=0).astype(bf16), total

    def gather(row, col, j, later, total, first):
        sl = slice(j * W, (j + 1) * W)
        weight = (ws[j].reshape(B // 16, 16, W) * later[None]).reshape(B, W)
        vt = jnp.concatenate([kvr[row, col, W + p * dh : W + (p + 1) * dh] for p in range(4)], axis=1)
        part = jnp.dot(vt, weight, preferred_element_type=f32)
        acc[:, sl] = part if first else acc[:, sl] * total + part

    def unit_of(turn):
        j = jnp.where(h == 0, turn, Z - 2 - turn)
        is_low = j < Z - 1 - kz
        zq = jnp.where(is_low, kz + 1 + j, j + 1)
        return jnp.where(is_low, 0, 1), zq

    def send_out(u, row, block, kept):
        lanes = lax.broadcasted_iota(jnp.int32, (dh // 2, 128), 1) < dh
        lanes_t = lax.broadcasted_iota(jnp.int32, (16, 128), 1) < dh
        top = lax.broadcasted_iota(jnp.int32, (16, 128), 0) == 0
        for g in range(T // 2):
            cols = slice(g * 128, (g + 1) * 128)
            a, b = acc[: dh // 2, cols], acc[dh // 2 :, cols]
            ar, br = pltpu.roll(a, dh, 1), pltpu.roll(b, dh, 1)
            j, inner = g * 128 // W, g * 128 % W
            tt = jnp.broadcast_to(kept[j][:, inner : inner + 128], (16, 128))
            tr = pltpu.roll(tt, dh, 1)
            for odd in range(2):
                body = jnp.where(lanes, ar, b) if odd else jnp.where(lanes, a, br)
                fac = jnp.where(lanes_t, tr, tt) if odd else jnp.where(lanes_t, tt, tr)
                fac_high = fac.astype(bf16).astype(f32)
                tail = jnp.where(top, fac_high, fac - fac_high)
                obuf[u, 2 * g + odd] = jnp.concatenate([body, tail], axis=0).astype(bf16)
        dst = row * T * H + t * H + h
        for e in range(1, T):
            r = (t + e) % T
            remote(obuf.at[u, r], orecv.at[dst], o_send.at[u * T + e], o_recv.at[dst], (block, r)).start()

        @pl.when(block != s)
        def _():
            remote(obuf.at[u, t], orecv.at[dst], o_send.at[u * T], o_recv.at[dst], (block, t)).start()

        @pl.when(block == s)
        def _():
            orecv[dst] = obuf[u, t]

    def key_row(row):
        return jnp.where(row == 0, kz, Z - 1 - kz)

    def self_unit(u, row, fresh):
        n = jnp.where(row == 0, x, XS - 1 - x)
        slot = jnp.where(row == 0, kz, Z)
        q_wait(slot)
        for j in range(2):
            acc[:, j * W : (j + 1) * W] = jnp.zeros((dh, W), f32)

        def step(col, kept):
            if fresh:
                kv_wait(row, col)
            nxt = []
            found = []
            for j in range(2):
                found.append(weigh(row, col, slot, j, False))
            for j in range(2):
                gather(row, col, j, *found[j], False)
                nxt.append(kept[j] * found[j][1])
            return tuple(nxt)

        one = jnp.ones((1, W), f32)
        kept = lax.fori_loop(0, n, step, (one, one))
        if fresh:
            kv_wait(row, n)
        found = [weigh(row, n, slot, j, True) for j in range(2)]
        for j in range(2):
            gather(row, n, j, *found[j], False)
        send_out(u, key_row(row), key_row(row) * XS + n, [kept[j] * found[j][1] for j in range(2)])
        return n

    n = self_unit(0, h, True)
    for col in range(XS):

        @pl.when(col > n)
        def _():
            kv_wait(h, col)

    kv_wait(1 - h, x)
    for e in (1, 3, 2):
        go(kv_copy(kvr.at[1 - h, x], 1 - h, x, 3 + e, z * XS + (x + e) % XS))

    turn_over = jnp.where(h == 0, Z - 1 - kz, kz)

    def mirrored():
        for e in range(1, XS):
            kv_wait(1 - h, (x + e) % XS)

    def full(turn, unused):
        row, zq = unit_of(turn)

        @pl.when(turn == turn_over)
        def _():
            mirrored()

        later_use = jnp.logical_and(row != h, zq > Z - 1 - kz)

        @pl.when(jnp.logical_not(later_use))
        def _():
            q_wait(zq)

        kept = [None, None]
        waiting = None
        for col in range(XS):
            for j in range(2):
                later, total = weigh(row, col, zq, j, False)
                if waiting is not None:
                    gather(*waiting)
                waiting = (row, col, j, later, total, col == 0)
                kept[j] = total if col == 0 else kept[j] * total
        gather(*waiting)
        send_out(turn + 1, key_row(row), zq * XS + x, kept)
        return unused

    lax.fori_loop(0, 3, full, 0)
    go(w_copy(wrow(t), t, 0, partner))
    for e in range(1, Y):
        came = ((y + e) % Y) * 2 + c
        w_copy(wrow(t), came, 0, partner).wait_recv()
        go(w_copy(wrow(came), came, Y + e - 1, partner))
    lax.fori_loop(3, Z - 1, full, 0)

    @pl.when(turn_over == Z - 1)
    def _():
        mirrored()

    self_unit(Z, 1 - h, False)

    w_copy(wrow(t), partner, 0, partner).wait_recv()
    for e in range(1, Y):
        w_copy(wrow(t), ((y + e) % Y) * 2 + 1 - c, 0, partner).wait_recv()

    for hh in range(T * H):
        heads[hh] = jnp.zeros((dh // 2, 128), f32)

    def combine(r, unused):
        for hh in range(T * H):

            @pl.when(jnp.logical_or(r != kz, hh != t * H + h))
            def _():
                e = r * T * H + hh
                remote(obuf.at[0, 0], orecv.at[e], o_send.at[0], o_recv.at[e], (s, t)).wait_recv()

        for hh in range(T * H):
            got = orecv[r * T * H + hh].astype(f32)
            fac = got[dh // 2 : dh // 2 + 1] + got[dh // 2 + 1 : dh // 2 + 2]
            heads[hh] = heads[hh] * fac + got[: dh // 2]
        return unused

    lax.fori_loop(0, z + 1, combine, 0)

    lhs, rhs = [], []
    for q in range(T * H // 4):
        both = jnp.concatenate([heads[4 * q + a] for a in range(4)], axis=0).T
        for e in range(2):
            lhs.append(both[e * dh : (e + 1) * dh].astype(bf16))
            for a in range(4):
                base = (4 * q + a) * dh + e * (dh // 2)
                rhs.append(wg[base : base + dh // 2])
    projected = jnp.dot(
        jnp.concatenate(lhs, axis=1), jnp.concatenate(rhs, axis=0), preferred_element_type=f32
    )
    out[...] = scaled_rows(projected, gain_out[...])

    for copy in started:
        copy.wait_send()
    each_q(lambda copy: copy.wait_send())

    def sent(u, block):
        for e in range(1, T):
            remote(obuf.at[u, 0], orecv.at[0], o_send.at[u * T + e], o_recv.at[0], (s, t)).wait_send()

        @pl.when(block != s)
        def _():
            remote(obuf.at[u, 0], orecv.at[0], o_send.at[u * T], o_recv.at[0], (s, t)).wait_send()

    def self_block(row):
        return key_row(row) * XS + jnp.where(row == 0, x, XS - 1 - x)

    sent(0, self_block(h))
    sent(Z, self_block(1 - h))

    def sent_full(turn, unused):
        sent(turn + 1, unit_of(turn)[1] * XS + x)
        return unused

    lax.fori_loop(0, Z - 1, sent_full, 0)


def solution(mesh):
    S, T = mesh.shape["sp"], mesh.shape["tp"]

    def local(act, gain_in, wq, wk, wv, off, wo, gain_out):
        R, D = act.shape
        H = off.shape[0]
        dh = wq.shape[1] // H
        B = R * T
        Z = S // XS
        vmem = pl.BlockSpec(memory_space=pltpu.VMEM)
        hbm = pl.BlockSpec(memory_space=pl.ANY)
        smem = pl.BlockSpec(memory_space=pltpu.SMEM)
        dma = pltpu.SemaphoreType.DMA
        return pl.pallas_call(
            functools.partial(layer_kernel, S, T, H, dh),
            out_shape=jax.ShapeDtypeStruct((R, D), bf16),
            in_specs=[vmem, vmem, hbm, hbm, hbm, smem, hbm, vmem],
            out_specs=vmem,
            scratch_shapes=[
                pltpu.VMEM(wq.shape, bf16),
                pltpu.VMEM(wk.shape, bf16),
                pltpu.VMEM(wv.shape, bf16),
                pltpu.VMEM((B, D), bf16),
                pltpu.VMEM((wo.shape[0] * T, D), bf16),
                pltpu.VMEM((B, B), bf16),
                pltpu.VMEM((H, B, 128), bf16),
                pltpu.VMEM((H, dh, B), bf16),
                pltpu.VMEM((2, XS, B, 128), bf16),
                pltpu.VMEM((Z + 1, dh, B), bf16),
                pltpu.VMEM((16, B), bf16),
                pltpu.VMEM((2, B, B // 2), bf16),
                pltpu.VMEM((dh, B), f32),
                pltpu.VMEM((Z + 1, T, dh // 2 + 16, 128), bf16),
                pltpu.VMEM((Z * T * H, dh // 2 + 16, 128), bf16),
                pltpu.VMEM((T * H, dh // 2, 128), f32),
                dma((T,)),
                dma((T,)),
                dma((T,)),
                dma((T,)),
                dma((8,)),
                dma((2 * XS,)),
                dma((H * Z // 2 + H,)),
                dma((Z + 1,)),
                dma(((Z + 1) * T,)),
                dma((Z * T * H,)),
                dma((4,)),
            ],
            compiler_params=pltpu.CompilerParams(collective_id=0, has_side_effects=True, vmem_limit_bytes=50 * 2**20),
        )(act, gain_in.reshape(1, D), wq, wk, wv, off, wo, gain_out.reshape(1, D))

    in_specs = (
        P(("sp", "tp"), None),
        P(),
        P(None, "tp"),
        P(None, "tp"),
        P(None, "tp"),
        P("tp"),
        P("tp", None),
        P(),
    )
    out_specs = P(("sp", "tp"), None)
    return jax.shard_map(local, mesh=mesh, in_specs=in_specs, out_specs=out_specs, check_vma=False)
```

```python
import functools

import jax
import jax.numpy as jnp
from jax import lax
from jax.experimental import pallas as pl
from jax.experimental.pallas import tpu as pltpu
from jax.sharding import PartitionSpec as P

epsilon = 1e-06
log2e = 1.4426950408889634
MESH = pl.DeviceIdType.MESH
f32 = jnp.float32
bf16 = jnp.bfloat16
XS = 4
ZMAX = 63.0


def scaled_rows(widened, row_gain):
    spread = jnp.mean(widened * widened, axis=-1, keepdims=True)
    return (widened * lax.rsqrt(spread + epsilon) * row_gain).astype(bf16)


def layer_kernel(
    S,
    T,
    H,
    dh,
    act_hbm,
    gain_in_hbm,
    wq_hbm,
    wk_hbm,
    wv_hbm,
    off,
    wo_hbm,
    gain_out_hbm,
    out,
    act,
    gain_in,
    gain_out,
    wq,
    wk,
    wv,
    xg,
    wg,
    perm,
    kvb,
    qb,
    kvr,
    qr,
    offt,
    ws,
    acc,
    obuf,
    orecv,
    tbuf,
    trecv,
    heads,
    x_send,
    x_recv,
    w_send,
    w_recv,
    kv_send,
    kv_recv,
    q_send,
    q_recv,
    o_send,
    o_recv,
    t_send,
    t_recv,
    load,
):
    R = act.shape[0]
    B = R * T
    W = B // 2
    rows = wo_hbm.shape[0]
    Z = S // XS
    half_z = Z // 2
    s = lax.axis_index("sp")
    t = lax.axis_index("tp")
    z, x = s // XS, s % XS
    h = z // half_z
    mz = Z - 1 - z
    kz = jnp.where(h == 0, z, mz)
    y, c = t // 2, t % 2
    partner = y * 2 + 1 - c
    Y = T // 2

    def remote(src, dst, send, recv, dev):
        return pltpu.make_async_remote_copy(
            src_ref=src, dst_ref=dst, send_sem=send, recv_sem=recv, device_id=dev, device_id_type=MESH
        )

    started = []

    def go(copy):
        copy.start()
        started.append(copy)
        return copy

    def xrow(index):
        return xg.at[pl.ds(pl.multiple_of(index * R, R), R)]

    def wrow(index):
        return wg.at[pl.ds(pl.multiple_of(index * rows, rows), rows)]

    def x_copy(index, slot, dev):
        return remote(xrow(index), xrow(index), x_send.at[slot], x_recv.at[index], (s, dev))

    def w_copy(src, index, slot, dev):
        return remote(src, wrow(index), w_send.at[slot], w_recv.at[index], (s, dev))

    early = [
        pltpu.make_async_copy(act_hbm, act, load.at[4]),
        pltpu.make_async_copy(gain_in_hbm, gain_in, load.at[5]),
    ]
    for copy in early:
        copy.start()
    loads = [
        pltpu.make_async_copy(wk_hbm, wk, load.at[0]),
        pltpu.make_async_copy(wv_hbm, wv, load.at[1]),
        pltpu.make_async_copy(wq_hbm, wq, load.at[2]),
        pltpu.make_async_copy(wo_hbm, wrow(t), load.at[3]),
        pltpu.make_async_copy(gain_out_hbm, gain_out, load.at[6]),
    ]
    for copy in loads:
        copy.start()
    barrier = pltpu.get_barrier_semaphore()
    partners = [(s, (t + d) % T) for d in range(1, T)]
    partners += [((z + d) % Z * XS + x, t) for d in range(1, Z)]
    partners += [(z * XS + (x + d) % XS, t) for d in range(1, XS)]
    partners += [(mz * XS + XS - 1 - x, t)]
    for other in partners:
        pl.semaphore_signal(barrier, inc=1, device_id=other, device_id_type=MESH)
    for copy in early:
        copy.wait()
    xg[pl.ds(pl.multiple_of(t * R, R), R)] = scaled_rows(act[...].astype(f32), gain_in[...])
    pl.semaphore_wait(barrier, len(partners))
    onward = (y + 1 + (Y - 2) * c) % Y
    behind = (y + Y - 1 - (Y - 2) * c) % Y
    across = (y + 2) % Y
    go(x_copy(t, 1, onward * 2 + c))
    go(x_copy(t, 2, behind * 2 + c))
    go(x_copy(t, 0, partner))

    token = lax.broadcasted_iota(jnp.int32, (B, B), 0)
    place = lax.broadcasted_iota(jnp.int32, (B, B), 1)
    perm[...] = (token == (place & (T - 1)) * R + (place >> (T.bit_length() - 1))).astype(f32).astype(bf16)
    whole = jnp.broadcast_to(off[h] * log2e, (16, B)).astype(f32)
    high = whole.astype(bf16).astype(f32)
    middle = (whole - high).astype(bf16).astype(f32)
    low = whole - high - middle
    part_row = lax.broadcasted_iota(jnp.int32, (16, B), 0)
    offt[...] = jnp.where(
        part_row == 0, high, jnp.where(part_row == 1, middle, jnp.where(part_row == 2, low, 0.0))
    ).astype(bf16)

    x_copy(behind * 2 + c, 0, partner).wait_recv()
    go(x_copy(behind * 2 + c, 3, onward * 2 + c))
    go(x_copy(behind * 2 + c, 4, partner))
    x_copy(onward * 2 + c, 0, partner).wait_recv()
    go(x_copy(onward * 2 + c, 5, partner))
    x_copy(across * 2 + c, 0, partner).wait_recv()
    go(x_copy(across * 2 + c, 6, partner))
    for copy in loads:
        copy.wait()
    for e in range(1, Y):
        go(w_copy(wrow(t), t, e, ((y + e) % Y) * 2 + c))
    x_copy(partner, 0, partner).wait_recv()
    for e in range(1, Y):
        x_copy(((y + e) % Y) * 2 + 1 - c, 0, partner).wait_recv()

    rows_all = xg[...]
    keys = jnp.dot(rows_all, wk[...], preferred_element_type=f32).astype(bf16).astype(f32)
    values = jnp.dot(rows_all, wv[...], preferred_element_type=f32).astype(bf16).astype(f32)
    turned = jnp.concatenate([keys.T, values.T], axis=0).astype(bf16)
    placed = jnp.dot(turned, perm[...], preferred_element_type=f32)
    keys_placed = placed[: H * dh].T
    for i in range(H):
        cols = slice(i * dh, (i + 1) * dh)
        kvb[i, :W] = jnp.concatenate([keys_placed[:W, cols], keys_placed[W:, cols]], axis=1).astype(bf16)
        for part in range(4):
            piece = placed[(H + i) * dh : (H + i + 1) * dh, part * 128 : (part + 1) * 128]
            kvb[i, W + part * dh : W + (part + 1) * dh] = piece.astype(bf16)

    def kv_copy(src, row, col, slot, dev):
        return remote(src, kvr.at[row, col], kv_send.at[slot], kv_recv.at[row * XS + col], (dev, t))

    go(kv_copy(kvb.at[1 - h], h, x, 0, mz * XS + x))
    for e in (1, 3, 2):
        go(kv_copy(kvb.at[h], h, x, e, z * XS + (x + e) % XS))
    kvr[h, x] = kvb[h]

    queries = jnp.dot(rows_all, wq[...], preferred_element_type=f32) * (dh ** (-0.5) * log2e)
    q_turned = queries.T.astype(bf16)
    for i in range(H):
        qb[i] = q_turned[i * dh : (i + 1) * dh]
    qr[z] = qb[h]

    def q_copy(i, depth):
        dev = depth if i == 0 else Z - 1 - depth
        return dev, remote(qb.at[i], qr.at[z], q_send.at[i * half_z + depth], q_recv.at[z], (dev * XS + x, t))

    def q_extra(i):
        dev = mz if i == 0 else z
        return remote(qb.at[i], qr.at[Z], q_send.at[H * half_z + i], q_recv.at[Z], (dev * XS + XS - 1 - x, t))

    def each_q(act_on):
        @pl.when(h == 1)
        def _():
            for i in range(H):
                act_on(q_extra(i))

        for depth in range(half_z - 1, -1, -1):
            for i in range(H):
                dev, copy = q_copy(i, depth)

                @pl.when(jnp.logical_and(depth <= z, dev != z))
                def _():
                    act_on(copy)

    each_q(lambda copy: copy.start())

    def kv_wait(row, col):
        @pl.when(jnp.logical_or(row != h, col != x))
        def _():
            remote(kvb.at[0], kvr.at[row, col], kv_send.at[0], kv_recv.at[row * XS + col], (s, t)).wait_recv()

    def q_wait(slot):
        @pl.when(slot != z)
        def _():
            remote(qb.at[0], qr.at[slot], q_send.at[0], q_recv.at[slot], (s, t)).wait_recv()

    lane = lax.broadcasted_iota(jnp.int32, (16, 128), 1)
    ones = (lane < 3).astype(f32).astype(bf16)
    zeros = jnp.zeros((dh, W), bf16)
    pad = jnp.zeros((112, W), bf16)

    def weigh(row, col, slot, j, masked):
        sl = slice(j * W, (j + 1) * W)
        run = jnp.ones((8, W), f32)
        if masked:
            ahead = (
                lax.broadcasted_iota(jnp.int32, (8, W), 1)
                + j * W
                - R * lax.broadcasted_iota(jnp.int32, (8, W), 0)
            )
        lhs = jnp.concatenate([kvr[row, col, :W], jnp.tile(ones, (W // 16, 1))], axis=1)
        for part in (1, 0):
            q = qr[slot, :, sl]
            stack = [q, zeros] if part == 0 else [zeros, q]
            rhs = jnp.concatenate(stack + [offt[:, sl], pad], axis=0)
            score = jnp.minimum(jnp.dot(lhs, rhs, preferred_element_type=f32), ZMAX)
            for v in range(W // 8 - 2, -1, -2):
                e0 = jnp.exp2(score[8 * v : 8 * v + 8])
                e1 = jnp.exp2(score[8 * v + 8 : 8 * v + 16])
                if masked:
                    place_v = part * (W // 8) + v
                    e0 = jnp.where(ahead > place_v, e0, 0.0)
                    e1 = jnp.where(ahead > place_v + 1, e1, 0.0)
                u0, u1 = 1.0 + e0, 1.0 + e1
                left = run * (1.0 / (u0 * u1))
                first = e0 * left
                second = e1 * (u0 * left)
                run = left
                base = part * W + 8 * v
                ws[j, base : base + 16] = jnp.concatenate([first, second], axis=0).astype(bf16)
        later = [None] * 8
        total = jnp.ones((1, W), f32)
        for i in range(7, -1, -1):
            later[i] = total
            total = total * run[i : i + 1]
        return jnp.concatenate(later + later, axis=0).astype(bf16), total

    def gather(row, col, j, later, total, first):
        sl = slice(j * W, (j + 1) * W)
        weight = (ws[j].reshape(B // 16, 16, W) * later[None]).reshape(B, W)
        vt = jnp.concatenate([kvr[row, col, W + p * dh : W + (p + 1) * dh] for p in range(4)], axis=1)
        part = jnp.dot(vt, weight, preferred_element_type=f32)
        acc[:, sl] = part if first else acc[:, sl] * total + part

    def unit_of(turn):
        j = jnp.where(h == 0, turn, Z - 2 - turn)
        is_low = j < Z - 1 - kz
        zq = jnp.where(is_low, kz + 1 + j, j + 1)
        return jnp.where(is_low, 0, 1), zq

    def o_copies(u, r, e, dst, dev):
        return (
            remote(obuf.at[u, r], orecv.at[dst], o_send.at[u * T + e], o_recv.at[dst], dev),
            remote(tbuf.at[u, r], trecv.at[dst], t_send.at[u * T + e], t_recv.at[dst], dev),
        )

    def send_out(u, row, block, kept):
        lanes = lax.broadcasted_iota(jnp.int32, (dh // 2, 128), 1) < dh
        lanes_t = lax.broadcasted_iota(jnp.int32, (8, 128), 1) < dh
        for g in range(T // 2):
            cols = slice(g * 128, (g + 1) * 128)
            a, b = acc[: dh // 2, cols], acc[dh // 2 :, cols]
            ar, br = pltpu.roll(a, dh, 1), pltpu.roll(b, dh, 1)
            j, inner = g * 128 // W, g * 128 % W
            tt = jnp.broadcast_to(kept[j][:, inner : inner + 128], (8, 128))
            tr = pltpu.roll(tt, dh, 1)
            for odd in range(2):
                body = jnp.where(lanes, ar, b) if odd else jnp.where(lanes, a, br)
                fac = jnp.where(lanes_t, tr, tt) if odd else jnp.where(lanes_t, tt, tr)
                obuf[u, 2 * g + odd] = body.astype(bf16)
                tbuf[u, 2 * g + odd] = fac[:1]
        dst = row * T * H + t * H + h
        for e in range(1, T):
            r = (t + e) % T
            for copy in o_copies(u, r, e, dst, (block, r)):
                copy.start()

        @pl.when(block != s)
        def _():
            for copy in o_copies(u, t, 0, dst, (block, t)):
                copy.start()

        @pl.when(block == s)
        def _():
            orecv[dst] = obuf[u, t]
            trecv[dst] = tbuf[u, t]

    def key_row(row):
        return jnp.where(row == 0, kz, Z - 1 - kz)

    def self_unit(u, row, fresh):
        n = jnp.where(row == 0, x, XS - 1 - x)
        slot = jnp.where(row == 0, kz, Z)
        q_wait(slot)
        for j in range(2):
            acc[:, j * W : (j + 1) * W] = jnp.zeros((dh, W), f32)

        def step(col, kept):
            if fresh:
                kv_wait(row, col)
            nxt = []
            found = []
            for j in range(2):
                found.append(weigh(row, col, slot, j, False))
            for j in range(2):
                gather(row, col, j, *found[j], False)
                nxt.append(kept[j] * found[j][1])
            return tuple(nxt)

        one = jnp.ones((1, W), f32)
        kept = lax.fori_loop(0, n, step, (one, one))
        if fresh:
            kv_wait(row, n)
        found = [weigh(row, n, slot, j, True) for j in range(2)]
        for j in range(2):
            gather(row, n, j, *found[j], False)
        send_out(u, key_row(row), key_row(row) * XS + n, [kept[j] * found[j][1] for j in range(2)])
        return n

    n = self_unit(0, h, True)
    for col in range(XS):

        @pl.when(col > n)
        def _():
            kv_wait(h, col)

    kv_wait(1 - h, x)
    for e in (1, 3, 2):
        go(kv_copy(kvr.at[1 - h, x], 1 - h, x, 3 + e, z * XS + (x + e) % XS))

    turn_over = jnp.where(h == 0, Z - 1 - kz, kz)

    def mirrored():
        for e in range(1, XS):
            kv_wait(1 - h, (x + e) % XS)

    def full(turn, unused):
        row, zq = unit_of(turn)

        @pl.when(turn == turn_over)
        def _():
            mirrored()

        later_use = jnp.logical_and(row != h, zq > Z - 1 - kz)

        @pl.when(jnp.logical_not(later_use))
        def _():
            q_wait(zq)

        kept = [None, None]
        waiting = None
        for col in range(XS):
            for j in range(2):
                later, total = weigh(row, col, zq, j, False)
                if waiting is not None:
                    gather(*waiting)
                waiting = (row, col, j, later, total, col == 0)
                kept[j] = total if col == 0 else kept[j] * total
        gather(*waiting)
        send_out(turn + 1, key_row(row), zq * XS + x, kept)
        return unused

    lax.fori_loop(0, 3, full, 0)
    go(w_copy(wrow(t), t, 0, partner))
    for e in range(1, Y):
        came = ((y + e) % Y) * 2 + c
        w_copy(wrow(t), came, 0, partner).wait_recv()
        go(w_copy(wrow(came), came, Y + e - 1, partner))
    lax.fori_loop(3, Z - 1, full, 0)

    @pl.when(turn_over == Z - 1)
    def _():
        mirrored()

    self_unit(Z, 1 - h, False)

    w_copy(wrow(t), partner, 0, partner).wait_recv()
    for e in range(1, Y):
        w_copy(wrow(t), ((y + e) % Y) * 2 + 1 - c, 0, partner).wait_recv()

    for hh in range(T * H):
        heads[hh] = jnp.zeros((dh // 2, 128), f32)

    def combine(r, unused):
        for hh in range(T * H):

            @pl.when(jnp.logical_or(r != kz, hh != t * H + h))
            def _():
                e = r * T * H + hh
                for copy in o_copies(0, 0, 0, e, (s, t)):
                    copy.wait_recv()

        for hh in range(T * H):
            heads[hh] = heads[hh] * trecv[r * T * H + hh] + orecv[r * T * H + hh].astype(f32)
        return unused

    lax.fori_loop(0, z + 1, combine, 0)

    lhs, rhs = [], []
    for q in range(T * H // 4):
        both = jnp.concatenate([heads[4 * q + a] for a in range(4)], axis=0).T
        for e in range(2):
            lhs.append(both[e * dh : (e + 1) * dh].astype(bf16))
            for a in range(4):
                base = (4 * q + a) * dh + e * (dh // 2)
                rhs.append(wg[base : base + dh // 2])
    projected = jnp.dot(
        jnp.concatenate(lhs, axis=1), jnp.concatenate(rhs, axis=0), preferred_element_type=f32
    )
    out[...] = scaled_rows(projected, gain_out[...])

    for copy in started:
        copy.wait_send()
    each_q(lambda copy: copy.wait_send())

    def sent(u, block):
        for e in range(1, T):
            for copy in o_copies(u, 0, e, 0, (s, t)):
                copy.wait_send()

        @pl.when(block != s)
        def _():
            for copy in o_copies(u, 0, 0, 0, (s, t)):
                copy.wait_send()

    def self_block(row):
        return key_row(row) * XS + jnp.where(row == 0, x, XS - 1 - x)

    sent(0, self_block(h))
    sent(Z, self_block(1 - h))

    def sent_full(turn, unused):
        sent(turn + 1, unit_of(turn)[1] * XS + x)
        return unused

    lax.fori_loop(0, Z - 1, sent_full, 0)


def solution(mesh):
    S, T = mesh.shape["sp"], mesh.shape["tp"]

    def local(act, gain_in, wq, wk, wv, off, wo, gain_out):
        R, D = act.shape
        H = off.shape[0]
        dh = wq.shape[1] // H
        B = R * T
        Z = S // XS
        vmem = pl.BlockSpec(memory_space=pltpu.VMEM)
        hbm = pl.BlockSpec(memory_space=pl.ANY)
        smem = pl.BlockSpec(memory_space=pltpu.SMEM)
        dma = pltpu.SemaphoreType.DMA
        return pl.pallas_call(
            functools.partial(layer_kernel, S, T, H, dh),
            out_shape=jax.ShapeDtypeStruct((R, D), bf16),
            in_specs=[hbm, hbm, hbm, hbm, hbm, smem, hbm, hbm],
            out_specs=vmem,
            scratch_shapes=[
                pltpu.VMEM((R, D), bf16),
                pltpu.VMEM((1, D), f32),
                pltpu.VMEM((1, D), f32),
                pltpu.VMEM(wq.shape, bf16),
                pltpu.VMEM(wk.shape, bf16),
                pltpu.VMEM(wv.shape, bf16),
                pltpu.VMEM((B, D), bf16),
                pltpu.VMEM((wo.shape[0] * T, D), bf16),
                pltpu.VMEM((B, B), bf16),
                pltpu.VMEM((H, B, 128), bf16),
                pltpu.VMEM((H, dh, B), bf16),
                pltpu.VMEM((2, XS, B, 128), bf16),
                pltpu.VMEM((Z + 1, dh, B), bf16),
                pltpu.VMEM((16, B), bf16),
                pltpu.VMEM((2, B, B // 2), bf16),
                pltpu.VMEM((dh, B), f32),
                pltpu.VMEM((Z + 1, T, dh // 2, 128), bf16),
                pltpu.VMEM((Z * T * H, dh // 2, 128), bf16),
                pltpu.VMEM((Z + 1, T, 1, 128), f32),
                pltpu.VMEM((Z * T * H, 1, 128), f32),
                pltpu.VMEM((T * H, dh // 2, 128), f32),
                dma((T,)),
                dma((T,)),
                dma((T,)),
                dma((T,)),
                dma((8,)),
                dma((2 * XS,)),
                dma((H * Z // 2 + H,)),
                dma((Z + 1,)),
                dma(((Z + 1) * T,)),
                dma((Z * T * H,)),
                dma(((Z + 1) * T,)),
                dma((Z * T * H,)),
                dma((7,)),
            ],
            compiler_params=pltpu.CompilerParams(collective_id=0, has_side_effects=True, vmem_limit_bytes=67043328),
        )(act, gain_in.reshape(1, D), wq, wk, wv, off, wo, gain_out.reshape(1, D))

    in_specs = (
        P(("sp", "tp"), None),
        P(),
        P(None, "tp"),
        P(None, "tp"),
        P(None, "tp"),
        P("tp"),
        P("tp", None),
        P(),
    )
    out_specs = P(("sp", "tp"), None)
    return jax.shard_map(local, mesh=mesh, in_specs=in_specs, out_specs=out_specs, check_vma=False)
```

```python
import functools

import jax
import jax.numpy as jnp
from jax import lax
from jax.experimental import pallas as pl
from jax.experimental.pallas import tpu as pltpu
from jax.sharding import PartitionSpec as P

epsilon = 1e-06
log2e = 1.4426950408889634
MESH = pl.DeviceIdType.MESH
f32 = jnp.float32
bf16 = jnp.bfloat16
XS = 4
ZMAX = 63.0
LAST = 11


def scaled_rows(widened, row_gain):
    spread = jnp.mean(widened * widened, axis=-1, keepdims=True)
    return (widened * lax.rsqrt(spread + epsilon) * row_gain).astype(bf16)


def layer_kernel(
    S,
    T,
    H,
    dh,
    act_hbm,
    gain_in_hbm,
    wq_hbm,
    wk_hbm,
    wv_hbm,
    off,
    wo_hbm,
    gain_out_hbm,
    out,
    act,
    gain_in,
    gain_out,
    wq,
    wk,
    wv,
    xg,
    wg,
    perm,
    kvb,
    qb,
    kvr,
    qr,
    offt,
    ws,
    acc,
    factors,
    mbuf,
    offs,
    obuf,
    orecv,
    tbuf,
    trecv,
    heads,
    x_send,
    x_recv,
    w_send,
    w_recv,
    kv_send,
    kv_recv,
    q_send,
    q_recv,
    f_send,
    m_send,
    m_recv,
    off_send,
    off_recv,
    o_send,
    o_recv,
    t_send,
    t_recv,
    load,
):
    R = act.shape[0]
    B = R * T
    W = B // 2
    rows = wo_hbm.shape[0]
    Z = S // XS
    s = lax.axis_index("sp")
    t = lax.axis_index("tp")
    z, x = s // XS, s % XS
    y, c = t // 2, t % 2
    partner = y * 2 + 1 - c
    place_z = (z + 2) % Z
    g, hl = place_z // 4, place_z % 4
    kz = 2 * g + c
    head = 2 * H * y + hl
    home = hl // H == c

    def spot(group, local):
        return (4 * group + local + Z - 2) % Z

    Y = T // 2

    def remote(src, dst, send, recv, dev):
        return pltpu.make_async_remote_copy(
            src_ref=src, dst_ref=dst, send_sem=send, recv_sem=recv, device_id=dev, device_id_type=MESH
        )

    started = []

    def go(copy):
        copy.start()
        started.append(copy)
        return copy

    def xrow(index):
        return xg.at[pl.ds(pl.multiple_of(index * R, R), R)]

    def wrow(index):
        return wg.at[pl.ds(pl.multiple_of(index * rows, rows), rows)]

    def x_copy(index, slot, dev):
        return remote(xrow(index), xrow(index), x_send.at[slot], x_recv.at[index], (s, dev))

    def w_copy(src, index, slot, dev):
        return remote(src, wrow(index), w_send.at[slot], w_recv.at[index], (s, dev))

    early = [
        pltpu.make_async_copy(act_hbm, act, load.at[4]),
        pltpu.make_async_copy(gain_in_hbm, gain_in, load.at[5]),
    ]
    for copy in early:
        copy.start()
    loads = [
        pltpu.make_async_copy(wk_hbm, wk, load.at[0]),
        pltpu.make_async_copy(wv_hbm, wv, load.at[1]),
        pltpu.make_async_copy(wq_hbm, wq, load.at[2]),
        pltpu.make_async_copy(wo_hbm, wrow(t), load.at[3]),
        pltpu.make_async_copy(gain_out_hbm, gain_out, load.at[6]),
    ]
    for copy in loads:
        copy.start()
    barrier = pltpu.get_barrier_semaphore()
    partners = [(s, (t + d) % T) for d in range(1, T)]
    for d in range(Z):
        for core in range(2):
            if d:
                partners.append(((z + d) % Z * XS + x, 2 * y + core))
            partners.append(((z + d) % Z * XS + XS - 1 - x, 2 * y + core))
    partners += [(z * XS + (x + 2) % XS, t), (z * XS + (XS - 1 - x + 2) % XS, t)]
    for other in partners:
        pl.semaphore_signal(barrier, inc=1, device_id=other, device_id_type=MESH)
    for copy in early:
        copy.wait()
    xg[pl.ds(pl.multiple_of(t * R, R), R)] = scaled_rows(act[...].astype(f32), gain_in[...])
    pl.semaphore_wait(barrier, len(partners))
    onward = (y + 1 + (Y - 2) * c) % Y
    behind = (y + Y - 1 - (Y - 2) * c) % Y
    across = (y + 2) % Y
    go(x_copy(t, 1, onward * 2 + c))
    go(x_copy(t, 2, behind * 2 + c))
    go(x_copy(t, 0, partner))

    token = lax.broadcasted_iota(jnp.int32, (B, B), 0)
    place = lax.broadcasted_iota(jnp.int32, (B, B), 1)
    perm[...] = (token == (place & (T - 1)) * R + (place >> (T.bit_length() - 1))).astype(f32).astype(bf16)
    for i in range(H):
        offs[H * c + i] = jnp.broadcast_to(off[i] * log2e, (1, 128)).astype(f32)
    mine = offs.at[pl.ds(H * c, H)]
    go(remote(mine, mine, off_send.at[0], off_recv.at[0], (s, partner)))
    x_copy(behind * 2 + c, 0, partner).wait_recv()
    go(x_copy(behind * 2 + c, 3, onward * 2 + c))
    go(x_copy(behind * 2 + c, 4, partner))
    x_copy(onward * 2 + c, 0, partner).wait_recv()
    go(x_copy(onward * 2 + c, 5, partner))
    x_copy(across * 2 + c, 0, partner).wait_recv()
    go(x_copy(across * 2 + c, 6, partner))
    for copy in loads:
        copy.wait()
    for e in range(1, Y):
        go(w_copy(wrow(t), t, e, ((y + e) % Y) * 2 + c))
    x_copy(partner, 0, partner).wait_recv()
    for e in range(1, Y):
        x_copy(((y + e) % Y) * 2 + 1 - c, 0, partner).wait_recv()

    rows_all = xg[...]
    keys = jnp.dot(rows_all, wk[...], preferred_element_type=f32).astype(bf16).astype(f32)
    values = jnp.dot(rows_all, wv[...], preferred_element_type=f32).astype(bf16).astype(f32)
    turned = jnp.concatenate([keys.T, values.T], axis=0).astype(bf16)
    placed = jnp.dot(turned, perm[...], preferred_element_type=f32)
    keys_placed = placed[: H * dh].T
    for i in range(H):
        cols = slice(i * dh, (i + 1) * dh)
        kvb[i, :W] = jnp.concatenate([keys_placed[:W, cols], keys_placed[W:, cols]], axis=1).astype(bf16)
        for part in range(4):
            piece = placed[(H + i) * dh : (H + i + 1) * dh, part * 128 : (part + 1) * 128]
            kvb[i, W + part * dh : W + (part + 1) * dh] = piece.astype(bf16)

    outer = jnp.minimum(z, Z - 1 - z)

    def kv_copy(src, row, col, slot, dev):
        return remote(src, kvr.at[row, col], kv_send.at[slot], kv_recv.at[row * XS + col], dev)

    def kv_first(i):
        zd = spot(outer // 2, H * c + i)
        stays = jnp.logical_and(zd == z, outer % 2 == c)
        return stays, kv_copy(kvb.at[i], z // (Z // 2), x, i, (zd * XS + x, 2 * y + outer % 2))

    for i in range(H):
        stays, copy = kv_first(i)

        @pl.when(stays)
        def _():
            kvr[z // (Z // 2), x] = kvb[i]

        @pl.when(jnp.logical_not(stays))
        def _():
            copy.start()

    queries = jnp.dot(rows_all, wq[...], preferred_element_type=f32) * (dh ** (-0.5) * log2e)
    q_turned = queries.T.astype(bf16)
    for i in range(H):
        qb[i] = q_turned[i * dh : (i + 1) * dh]

    def q_first(i, group):
        zd = spot(group, H * c + i)
        stays = jnp.logical_and(zd == z, c == 0)
        copy = remote(qb.at[i], qr.at[z], q_send.at[i * 2 + group], q_recv.at[z], (zd * XS + x, 2 * y))
        return stays, z >= 2 * group, copy

    def q_extra(i):
        depth = Z - 1 - z
        zd = spot(depth // 2, H * c + i)
        dev = (zd * XS + XS - 1 - x, 2 * y + depth % 2)
        return remote(qb.at[i], qr.at[Z], q_send.at[2 * H + i], q_recv.at[Z], dev)

    def each_q(act_on):
        for group in (0, 1):
            for i in range(H):
                stays, wanted, copy = q_first(i, group)

                @pl.when(jnp.logical_and(wanted, jnp.logical_not(stays)))
                def _():
                    act_on(copy)

        @pl.when(z >= Z // 2)
        def _():
            for i in range(H):
                act_on(q_extra(i))

    for i in range(H):
        for group in (0, 1):
            stays, wanted, _ = q_first(i, group)

            @pl.when(jnp.logical_and(wanted, stays))
            def _():
                qr[z] = qb[i]

    each_q(lambda copy: copy.start())

    def kv_wait(row, col):
        remote(kvb.at[0], kvr.at[row, col], kv_send.at[0], kv_recv.at[row * XS + col], (s, t)).wait_recv()

    def q_forward(slot):
        return remote(qr.at[slot], qr.at[slot], f_send.at[slot], q_recv.at[slot], (s, partner))

    def q_wait(slot):
        local = jnp.logical_and(jnp.logical_and(slot == z, c == 0), hl // H == 0)

        @pl.when(jnp.logical_not(local))
        def _():
            q_forward(slot).wait_recv()

    x_on = (x + 1 + (XS - 2) * c) % XS
    x_back = (x + XS - 1 - (XS - 2) * c) % XS
    x_far = (x + 2) % XS

    def kv_spread(row):
        base = H + row * 3
        return (
            kv_copy(kvr.at[row, x], row, x, base, (z * XS + x_on, t)),
            kv_copy(kvr.at[row, x], row, x, base + 1, (z * XS + x_back, t)),
            kv_copy(kvr.at[row, x_back], row, x_back, base + 2, (z * XS + x_on, t)),
        )

    for row in range(2):
        local = jnp.logical_and(z == (kz if row == 0 else Z - 1 - kz), home)

        @pl.when(jnp.logical_not(local))
        def _():
            kv_wait(row, x)

        for copy in kv_spread(row)[:2]:
            copy.start()

    kv_wait(0, x_back)
    kv_spread(0)[2].start()

    theirs = offs.at[pl.ds(H * (1 - c), H)]
    remote(theirs, theirs, off_send.at[0], off_recv.at[0], (s, partner)).wait_recv()
    whole = jnp.concatenate([jnp.broadcast_to(offs[hl], (16, 128))] * (B // 128), axis=1)
    high = whole.astype(bf16).astype(f32)
    middle = (whole - high).astype(bf16).astype(f32)
    low = whole - high - middle
    part_row = lax.broadcasted_iota(jnp.int32, (16, B), 0)
    offt[...] = jnp.where(
        part_row == 0, high, jnp.where(part_row == 1, middle, jnp.where(part_row == 2, low, 0.0))
    ).astype(bf16)

    lane = lax.broadcasted_iota(jnp.int32, (16, 128), 1)
    ones = (lane < 3).astype(f32).astype(bf16)
    zeros = jnp.zeros((dh, W), bf16)
    pad = jnp.zeros((112, W), bf16)

    def weigh(row, col, slot, j, masked):
        sl = slice(j * W, (j + 1) * W)
        run = jnp.ones((8, W), f32)
        if masked:
            ahead = (
                lax.broadcasted_iota(jnp.int32, (8, W), 1)
                + j * W
                - R * lax.broadcasted_iota(jnp.int32, (8, W), 0)
            )
        lhs = jnp.concatenate([kvr[row, col, :W], jnp.tile(ones, (W // 16, 1))], axis=1)
        for part in (1, 0):
            q = qr[slot, :, sl]
            stack = [q, zeros] if part == 0 else [zeros, q]
            rhs = jnp.concatenate(stack + [offt[:, sl], pad], axis=0)
            score = jnp.minimum(jnp.dot(lhs, rhs, preferred_element_type=f32), ZMAX)
            for v in range(W // 8 - 2, -1, -2):
                e0 = jnp.exp2(score[8 * v : 8 * v + 8])
                e1 = jnp.exp2(score[8 * v + 8 : 8 * v + 16])
                if masked:
                    place_v = part * (W // 8) + v
                    e0 = jnp.where(ahead > place_v, e0, 0.0)
                    e1 = jnp.where(ahead > place_v + 1, e1, 0.0)
                u0, u1 = 1.0 + e0, 1.0 + e1
                left = run * (1.0 / (u0 * u1))
                first = e0 * left
                second = e1 * (u0 * left)
                run = left
                base = part * W + 8 * v
                ws[j, base : base + 16] = jnp.concatenate([first, second], axis=0).astype(bf16)
        later = [None] * 8
        total = jnp.ones((1, W), f32)
        for i in range(7, -1, -1):
            later[i] = total
            total = total * run[i : i + 1]
        return jnp.concatenate(later + later, axis=0).astype(bf16), total

    def gather(row, col, j, later, total, first):
        sl = slice(j * W, (j + 1) * W)
        weight = (ws[j].reshape(B // 16, 16, W) * later[None]).reshape(B, W)
        vt = jnp.concatenate([kvr[row, col, W + p * dh : W + (p + 1) * dh] for p in range(4)], axis=1)
        part = jnp.dot(vt, weight, preferred_element_type=f32)
        acc[:, sl] = part if first else acc[:, sl] * total + part

    def o_copies(u, r, e, dst, dev):
        return (
            remote(obuf.at[u, r], orecv.at[dst], o_send.at[u * T + e], o_recv.at[dst], dev),
            remote(tbuf.at[u, r], trecv.at[dst], t_send.at[u * T + e], t_recv.at[dst], dev),
        )

    def send_out(u, slot, block, kept):
        lanes = lax.broadcasted_iota(jnp.int32, (dh // 2, 128), 1) < dh
        lanes_t = lax.broadcasted_iota(jnp.int32, (8, 128), 1) < dh
        for g in range(T // 2):
            cols = slice(g * 128, (g + 1) * 128)
            a, b = acc[: dh // 2, cols], acc[dh // 2 :, cols]
            ar, br = pltpu.roll(a, dh, 1), pltpu.roll(b, dh, 1)
            j, inner = g * 128 // W, g * 128 % W
            tt = jnp.broadcast_to(kept[j][:, inner : inner + 128], (8, 128))
            tr = pltpu.roll(tt, dh, 1)
            for odd in range(2):
                body = jnp.where(lanes, ar, b) if odd else jnp.where(lanes, a, br)
                fac = jnp.where(lanes_t, tr, tt) if odd else jnp.where(lanes_t, tt, tr)
                obuf[u, 2 * g + odd] = body.astype(bf16)
                tbuf[u, 2 * g + odd] = fac[:1]
        dst = slot * T * H + head
        for e in range(1, T):
            r = (t + e) % T
            for copy in o_copies(u, r, e, dst, (block, r)):
                copy.start()

        @pl.when(block != s)
        def _():
            for copy in o_copies(u, t, 0, dst, (block, t)):
                copy.start()

        @pl.when(block == s)
        def _():
            orecv[dst] = obuf[u, t]
            trecv[dst] = tbuf[u, t]

    def merge(slot, kept):
        remote(mbuf.at[slot], mbuf.at[slot], m_send.at[slot], m_recv.at[slot], (s, t)).wait_recv()
        out_kept = []
        for j in range(2):
            sl = slice(j * W, (j + 1) * W)
            acc[:, sl] = mbuf[slot, :dh, sl] * kept[j] + acc[:, sl]
            out_kept.append(mbuf[slot, dh : dh + 1, sl] * kept[j])
        return out_kept

    def self_unit(row):
        n = x if row == 0 else XS - 1 - x
        zq = kz if row == 0 else Z - 1 - kz
        slot = kz if row == 0 else Z
        q_wait(slot)
        for j in range(2):
            acc[:, j * W : (j + 1) * W] = jnp.zeros((dh, W), f32)

        def step(col, kept):
            found = [weigh(row, col, slot, j, False) for j in range(2)]
            for j in range(2):
                gather(row, col, j, *found[j], False)
            return tuple(kept[j] * found[j][1] for j in range(2))

        one = jnp.ones((1, W), f32)
        kept = lax.fori_loop(0, n, step, (one, one))
        found = [weigh(row, n, slot, j, True) for j in range(2)]
        for j in range(2):
            gather(row, n, j, *found[j], False)
        kept = [kept[j] * found[j][1] for j in range(2)]
        if row == 0:

            @pl.when(c == 0)
            def _():
                send_out(kz, g, zq * XS + n, kept)

            @pl.when(c == 1)
            def _():
                send_out(kz, g, zq * XS + n, merge(kz, kept))
        else:
            send_out(LAST, Z - 3 - kz, zq * XS + n, kept)

    def full(turn, unused):
        low_row = turn < Z
        hop = (turn + 1) // 2
        near = jnp.where(turn % 2 == 1, z + hop, z + Z - hop) % Z
        zq = jnp.where(low_row, near, turn - Z)
        row = jnp.where(low_row, 0, 1)
        valid = jnp.where(low_row, zq - kz > 0, zq + kz >= Z)

        @pl.when(turn == 2)
        def _():
            kv_wait(1, x_back)
            kv_spread(1)[2].start()

        @pl.when(turn == Z)
        def _():
            kv_wait(1, x_on)
            kv_wait(1, x_far)

        @pl.when(valid)
        def _():
            @pl.when(low_row)
            def _():
                q_wait(zq)

                @pl.when(c == 0)
                def _():
                    q_forward(zq).start()

            kept = [None, None]
            waiting = None
            for col in range(XS):
                for j in range(2):
                    later, total = weigh(row, col, zq, j, False)
                    if waiting is not None:
                        gather(*waiting)
                    waiting = (row, col, j, later, total, col == 0)
                    kept[j] = total if col == 0 else kept[j] * total
            gather(*waiting)
            for j in range(2):
                factors[:, j * W : (j + 1) * W] = jnp.broadcast_to(kept[j], (8, W))

            handed = jnp.logical_and(low_row, c == 0)

            @pl.when(handed)
            def _():
                mbuf[zq, :dh] = acc[...]
                mbuf[zq, dh:] = factors[...]
                remote(mbuf.at[zq], mbuf.at[zq], m_send.at[zq], m_recv.at[zq], (s, partner)).start()

            @pl.when(jnp.logical_and(low_row, c == 1))
            def _():
                for j, both in enumerate(merge(zq, kept)):
                    factors[:, j * W : (j + 1) * W] = jnp.broadcast_to(both, (8, W))

            @pl.when(jnp.logical_not(handed))
            def _():
                u = jnp.where(low_row, zq, zq + 3)
                slot = jnp.where(low_row, g, Z - 3 - kz)
                send_out(u, slot, zq * XS + x, [factors[:1, j * W : (j + 1) * W] for j in range(2)])

        return unused

    go(w_copy(wrow(t), t, 0, partner))
    for e in range(1, Y):
        came = ((y + e) % Y) * 2 + c
        w_copy(wrow(t), came, 0, partner).wait_recv()
        go(w_copy(wrow(came), came, Y + e - 1, partner))
    kv_wait(0, x_on)
    kv_wait(0, x_far)
    lax.fori_loop(0, 2 * Z, full, 0)
    self_unit(0)
    self_unit(1)

    w_copy(wrow(t), partner, 0, partner).wait_recv()
    for e in range(1, Y):
        w_copy(wrow(t), ((y + e) % Y) * 2 + 1 - c, 0, partner).wait_recv()

    for hh in range(T * H):
        heads[hh] = jnp.zeros((dh // 2, 128), f32)

    def made_here(slot):
        low_made = jnp.where(c == 1, z >= kz, z == kz)
        high_made = jnp.logical_and(slot == Z - 3 - kz, z + kz >= Z)
        return jnp.logical_or(jnp.logical_and(slot == g, low_made), high_made)

    def combine(r, unused):
        for hh in range(T * H):

            @pl.when(jnp.logical_not(jnp.logical_and(hh == head, made_here(r))))
            def _():
                e = r * T * H + hh
                for copy in o_copies(0, 0, 0, e, (s, t)):
                    copy.wait_recv()

        for hh in range(T * H):
            heads[hh] = heads[hh] * trecv[r * T * H + hh] + orecv[r * T * H + hh].astype(f32)
        return unused

    slots = jnp.where(z < 2, 1, jnp.where(z < 4, 2, z - 1))
    lax.fori_loop(0, slots, combine, 0)

    lhs, rhs = [], []
    for q in range(T * H // 4):
        both = jnp.concatenate([heads[4 * q + a] for a in range(4)], axis=0).T
        for e in range(2):
            lhs.append(both[e * dh : (e + 1) * dh].astype(bf16))
            for a in range(4):
                base = (4 * q + a) * dh + e * (dh // 2)
                rhs.append(wg[base : base + dh // 2])
    projected = jnp.dot(
        jnp.concatenate(lhs, axis=1), jnp.concatenate(rhs, axis=0), preferred_element_type=f32
    )
    out[...] = scaled_rows(projected, gain_out[...])

    for copy in started:
        copy.wait_send()
    each_q(lambda copy: copy.wait_send())

    for i in range(H):
        stays, copy = kv_first(i)

        @pl.when(jnp.logical_not(stays))
        def _():
            copy.wait_send()

    for row in range(2):
        for copy in kv_spread(row):
            copy.wait_send()

    def sent(u, valid, block):
        @pl.when(valid)
        def _():
            for e in range(1, T):
                for copy in o_copies(u, 0, e, 0, (s, t)):
                    copy.wait_send()

            @pl.when(block != s)
            def _():
                for copy in o_copies(u, 0, 0, 0, (s, t)):
                    copy.wait_send()

    def sent_low(zq, unused):
        sent(zq, jnp.logical_or(zq == kz, jnp.logical_and(zq > kz, c == 1)), zq * XS + x)

        @pl.when(jnp.logical_and(zq > kz, c == 0))
        def _():
            q_forward(zq).wait_send()
            remote(mbuf.at[zq], mbuf.at[zq], m_send.at[zq], m_recv.at[zq], (s, partner)).wait_send()

        return unused

    def sent_high(zq, unused):
        sent(zq + 3, zq + kz >= Z, zq * XS + x)
        return unused

    lax.fori_loop(0, Z, sent_low, 0)
    lax.fori_loop(5, Z, sent_high, 0)
    sent(LAST, z >= 0, (Z - 1 - kz) * XS + XS - 1 - x)


def solution(mesh):
    S, T = mesh.shape["sp"], mesh.shape["tp"]

    def local(act, gain_in, wq, wk, wv, off, wo, gain_out):
        R, D = act.shape
        H = off.shape[0]
        dh = wq.shape[1] // H
        B = R * T
        Z = S // XS
        vmem = pl.BlockSpec(memory_space=pltpu.VMEM)
        hbm = pl.BlockSpec(memory_space=pl.ANY)
        smem = pl.BlockSpec(memory_space=pltpu.SMEM)
        dma = pltpu.SemaphoreType.DMA
        return pl.pallas_call(
            functools.partial(layer_kernel, S, T, H, dh),
            out_shape=jax.ShapeDtypeStruct((R, D), bf16),
            in_specs=[hbm, hbm, hbm, hbm, hbm, smem, hbm, hbm],
            out_specs=vmem,
            scratch_shapes=[
                pltpu.VMEM((R, D), bf16),
                pltpu.VMEM((1, D), f32),
                pltpu.VMEM((1, D), f32),
                pltpu.VMEM(wq.shape, bf16),
                pltpu.VMEM(wk.shape, bf16),
                pltpu.VMEM(wv.shape, bf16),
                pltpu.VMEM((B, D), bf16),
                pltpu.VMEM((wo.shape[0] * T, D), bf16),
                pltpu.VMEM((B, B), bf16),
                pltpu.VMEM((H, B, 128), bf16),
                pltpu.VMEM((H, dh, B), bf16),
                pltpu.VMEM((2, XS, B, 128), bf16),
                pltpu.VMEM((Z + 1, dh, B), bf16),
                pltpu.VMEM((16, B), bf16),
                pltpu.VMEM((2, B, B // 2), bf16),
                pltpu.VMEM((dh, B), f32),
                pltpu.VMEM((8, B), f32),
                pltpu.VMEM((Z, dh + 8, B), f32),
                pltpu.VMEM((2 * H, 1, 128), f32),
                pltpu.VMEM((LAST + 1, T, dh // 2, 128), bf16),
                pltpu.VMEM((6 * T * H, dh // 2, 128), bf16),
                pltpu.VMEM((LAST + 1, T, 1, 128), f32),
                pltpu.VMEM((6 * T * H, 1, 128), f32),
                pltpu.VMEM((T * H, dh // 2, 128), f32),
                dma((T,)),
                dma((T,)),
                dma((T,)),
                dma((T,)),
                dma((8,)),
                dma((2 * XS,)),
                dma((3 * H,)),
                dma((Z + 1,)),
                dma((Z + 1,)),
                dma((Z,)),
                dma((Z,)),
                dma((1,)),
                dma((1,)),
                dma(((LAST + 1) * T,)),
                dma((6 * T * H,)),
                dma(((LAST + 1) * T,)),
                dma((6 * T * H,)),
                dma((7,)),
            ],
            compiler_params=pltpu.CompilerParams(collective_id=0, has_side_effects=True, vmem_limit_bytes=67043328),
        )(act, gain_in.reshape(1, D), wq, wk, wv, off, wo, gain_out.reshape(1, D))

    in_specs = (
        P(("sp", "tp"), None),
        P(),
        P(None, "tp"),
        P(None, "tp"),
        P(None, "tp"),
        P("tp"),
        P("tp", None),
        P(),
    )
    out_specs = P(("sp", "tp"), None)
    return jax.shard_map(local, mesh=mesh, in_specs=in_specs, out_specs=out_specs, check_vma=False)
```

```python
import functools

import jax
import jax.numpy as jnp
from jax import lax
from jax.experimental import pallas as pl
from jax.experimental.pallas import tpu as pltpu
from jax.sharding import PartitionSpec as P

epsilon = 1e-06
log2e = 1.4426950408889634
MESH = pl.DeviceIdType.MESH
f32 = jnp.float32
bf16 = jnp.bfloat16
XS = 4
ZMAX = 63.0
LAST = 11


def scaled_rows(widened, row_gain):
    spread = jnp.mean(widened * widened, axis=-1, keepdims=True)
    return (widened * lax.rsqrt(spread + epsilon) * row_gain).astype(bf16)


def layer_kernel(
    S,
    T,
    H,
    dh,
    act_hbm,
    gain_in_hbm,
    wq_hbm,
    wk_hbm,
    wv_hbm,
    off,
    wo_hbm,
    gain_out_hbm,
    out,
    act,
    gain_in,
    gain_out,
    wq,
    wk,
    wv,
    xg,
    wg,
    perm,
    kvb,
    qb,
    kvr,
    qr,
    offt,
    ws,
    acc,
    factors,
    mbuf,
    offs,
    obuf,
    orecv,
    tbuf,
    trecv,
    heads,
    x_send,
    x_recv,
    w_send,
    w_recv,
    kv_send,
    kv_recv,
    q_send,
    q_recv,
    f_send,
    m_send,
    m_recv,
    off_send,
    off_recv,
    o_send,
    o_recv,
    t_send,
    t_recv,
    load,
):
    R = act.shape[0]
    B = R * T
    W = B // 2
    rows = wo_hbm.shape[0]
    Z = S // XS
    s = lax.axis_index("sp")
    t = lax.axis_index("tp")
    z, x = s // XS, s % XS
    y, c = t // 2, t % 2
    partner = y * 2 + 1 - c
    place_z = (z + 2) % Z
    g, hl = place_z // 4, place_z % 4
    kz = 2 * g + c
    head = 2 * H * y + hl
    home = hl // H == c

    def spot(group, local):
        return (4 * group + local + Z - 2) % Z

    Y = T // 2

    def remote(src, dst, send, recv, dev):
        return pltpu.make_async_remote_copy(
            src_ref=src, dst_ref=dst, send_sem=send, recv_sem=recv, device_id=dev, device_id_type=MESH
        )

    started = []

    def go(copy):
        copy.start()
        started.append(copy)
        return copy

    def xrow(index):
        return xg.at[pl.ds(pl.multiple_of(index * R, R), R)]

    def wrow(index):
        return wg.at[pl.ds(pl.multiple_of(index * rows, rows), rows)]

    def x_copy(index, slot, dev):
        return remote(xrow(index), xrow(index), x_send.at[slot], x_recv.at[index], (s, dev))

    def w_copy(src, index, slot, dev):
        return remote(src, wrow(index), w_send.at[slot], w_recv.at[index], (s, dev))

    early = [
        pltpu.make_async_copy(act_hbm, act, load.at[4]),
        pltpu.make_async_copy(gain_in_hbm, gain_in, load.at[5]),
    ]
    for copy in early:
        copy.start()
    loads = [
        pltpu.make_async_copy(wk_hbm, wk, load.at[0]),
        pltpu.make_async_copy(wv_hbm, wv, load.at[1]),
        pltpu.make_async_copy(wq_hbm, wq, load.at[2]),
        pltpu.make_async_copy(wo_hbm, wrow(t), load.at[3]),
        pltpu.make_async_copy(gain_out_hbm, gain_out, load.at[6]),
    ]
    for copy in loads:
        copy.start()
    barrier = pltpu.get_barrier_semaphore()
    partners = [(s, (t + d) % T) for d in range(1, T)]
    for d in range(Z):
        for core in range(2):
            if d:
                partners.append(((z + d) % Z * XS + x, 2 * y + core))
            partners.append(((z + d) % Z * XS + XS - 1 - x, 2 * y + core))
    partners += [(z * XS + (x + 2) % XS, t), (z * XS + (XS - 1 - x + 2) % XS, t)]
    for other in partners:
        pl.semaphore_signal(barrier, inc=1, device_id=other, device_id_type=MESH)
    for copy in early:
        copy.wait()
    xg[pl.ds(pl.multiple_of(t * R, R), R)] = scaled_rows(act[...].astype(f32), gain_in[...])
    pl.semaphore_wait(barrier, len(partners))
    onward = (y + 1 + (Y - 2) * c) % Y
    behind = (y + Y - 1 - (Y - 2) * c) % Y
    across = (y + 2) % Y
    go(x_copy(t, 1, onward * 2 + c))
    go(x_copy(t, 2, behind * 2 + c))
    go(x_copy(t, 0, partner))

    token = lax.broadcasted_iota(jnp.int32, (B, B), 0)
    place = lax.broadcasted_iota(jnp.int32, (B, B), 1)
    perm[...] = (token == (place & (T - 1)) * R + R - 1 - (place >> (T.bit_length() - 1))).astype(f32).astype(bf16)
    for i in range(H):
        offs[H * c + i] = jnp.broadcast_to(off[i] * log2e, (1, 128)).astype(f32)
    mine = offs.at[pl.ds(H * c, H)]
    go(remote(mine, mine, off_send.at[0], off_recv.at[0], (s, partner)))
    x_copy(behind * 2 + c, 0, partner).wait_recv()
    go(x_copy(behind * 2 + c, 3, onward * 2 + c))
    go(x_copy(behind * 2 + c, 4, partner))
    x_copy(onward * 2 + c, 0, partner).wait_recv()
    go(x_copy(onward * 2 + c, 5, partner))
    x_copy(across * 2 + c, 0, partner).wait_recv()
    go(x_copy(across * 2 + c, 6, partner))
    for copy in loads:
        copy.wait()
    for e in range(1, Y):
        go(w_copy(wrow(t), t, e, ((y + e) % Y) * 2 + c))
    x_copy(partner, 0, partner).wait_recv()
    for e in range(1, Y):
        x_copy(((y + e) % Y) * 2 + 1 - c, 0, partner).wait_recv()

    rows_all = xg[...]
    keys = jnp.dot(rows_all, wk[...], preferred_element_type=f32).astype(bf16).astype(f32)
    values = jnp.dot(rows_all, wv[...], preferred_element_type=f32).astype(bf16).astype(f32)
    turned = jnp.concatenate([keys.T, values.T], axis=0).astype(bf16)
    placed = jnp.dot(turned, perm[...], preferred_element_type=f32)
    keys_placed = placed[: H * dh].T
    for i in range(H):
        cols = slice(i * dh, (i + 1) * dh)
        kvb[i, :W] = jnp.concatenate([keys_placed[:W, cols], keys_placed[W:, cols]], axis=1).astype(bf16)
        for part in range(4):
            piece = placed[(H + i) * dh : (H + i + 1) * dh, part * 128 : (part + 1) * 128]
            kvb[i, W + part * dh : W + (part + 1) * dh] = piece.astype(bf16)

    outer = jnp.minimum(z, Z - 1 - z)

    class Both:
        def __init__(self, parts):
            self.parts = parts

        def start(self):
            for part in self.parts:
                part.start()

        def wait_send(self):
            for part in self.parts:
                part.wait_send()

    def kv_part(src, row, col, slot, dev, part):
        rows_of = pl.ds(part * W, W)
        return remote(
            src.at[rows_of],
            kvr.at[row, col, rows_of],
            kv_send.at[2 * slot + part],
            kv_recv.at[2 * (row * XS + col) + part],
            dev,
        )

    def kv_copy(src, row, col, slot, dev):
        return Both([kv_part(src, row, col, slot, dev, part) for part in range(2)])

    def kv_first(i):
        zd = spot(outer // 2, H * c + i)
        stays = jnp.logical_and(zd == z, outer % 2 == c)
        return stays, kv_copy(kvb.at[i], z // (Z // 2), x, i, (zd * XS + x, 2 * y + outer % 2))

    for i in range(H):
        stays, copy = kv_first(i)

        @pl.when(stays)
        def _():
            kvr[z // (Z // 2), x] = kvb[i]

        @pl.when(jnp.logical_not(stays))
        def _():
            copy.start()

    queries = jnp.dot(rows_all, wq[...], preferred_element_type=f32) * (dh ** (-0.5) * log2e)
    q_turned = queries.T.astype(bf16)
    for i in range(H):
        qb[i] = q_turned[i * dh : (i + 1) * dh]

    def q_first(i, group):
        zd = spot(group, H * c + i)
        stays = jnp.logical_and(zd == z, c == 0)
        copy = remote(qb.at[i], qr.at[z], q_send.at[i * 2 + group], q_recv.at[z], (zd * XS + x, 2 * y))
        return stays, z >= 2 * group, copy

    def q_extra(i):
        depth = Z - 1 - z
        zd = spot(depth // 2, H * c + i)
        dev = (zd * XS + XS - 1 - x, 2 * y + depth % 2)
        return remote(qb.at[i], qr.at[Z], q_send.at[2 * H + i], q_recv.at[Z], dev)

    def each_q(act_on):
        for group in (0, 1):
            for i in range(H):
                stays, wanted, copy = q_first(i, group)

                @pl.when(jnp.logical_and(wanted, jnp.logical_not(stays)))
                def _():
                    act_on(copy)

        @pl.when(z >= Z // 2)
        def _():
            for i in range(H):
                act_on(q_extra(i))

    for i in range(H):
        for group in (0, 1):
            stays, wanted, _ = q_first(i, group)

            @pl.when(jnp.logical_and(wanted, stays))
            def _():
                qr[z] = qb[i]


    def kv_wait(row, col):
        for part in range(2):
            kv_part(kvb.at[0], row, col, 0, (s, t), part).wait_recv()

    def q_forward(slot):
        return remote(qr.at[slot], qr.at[slot], f_send.at[slot], q_recv.at[slot], (s, partner))

    def q_wait(slot):
        local = jnp.logical_and(jnp.logical_and(slot == z, c == 0), hl // H == 0)

        @pl.when(jnp.logical_not(local))
        def _():
            q_forward(slot).wait_recv()

    x_on = (x + 1 + (XS - 2) * c) % XS
    x_back = (x + XS - 1 - (XS - 2) * c) % XS
    x_far = (x + 2) % XS

    def kv_spread(row):
        base = H + row * 3
        return (
            kv_copy(kvr.at[row, x], row, x, base, (z * XS + x_on, t)),
            kv_copy(kvr.at[row, x], row, x, base + 1, (z * XS + x_back, t)),
            kv_copy(kvr.at[row, x_back], row, x_back, base + 2, (z * XS + x_on, t)),
        )

    for row in range(2):
        local = jnp.logical_and(z == (kz if row == 0 else Z - 1 - kz), home)

        for part in range(2):

            @pl.when(jnp.logical_not(local))
            def _():
                kv_part(kvb.at[0], row, x, 0, (s, t), part).wait_recv()

            for copy in kv_spread(row)[:2]:
                copy.parts[part].start()

    each_q(lambda copy: copy.start())
    for part in range(2):
        kv_part(kvb.at[0], 0, x_back, 0, (s, t), part).wait_recv()
        kv_spread(0)[2].parts[part].start()

    theirs = offs.at[pl.ds(H * (1 - c), H)]
    remote(theirs, theirs, off_send.at[0], off_recv.at[0], (s, partner)).wait_recv()
    whole = jnp.concatenate([jnp.broadcast_to(offs[hl], (16, 128))] * (B // 128), axis=1)
    high = whole.astype(bf16).astype(f32)
    middle = (whole - high).astype(bf16).astype(f32)
    low = whole - high - middle
    part_row = lax.broadcasted_iota(jnp.int32, (16, B), 0)
    offt[...] = jnp.where(
        part_row == 0, high, jnp.where(part_row == 1, middle, jnp.where(part_row == 2, low, 0.0))
    ).astype(bf16)

    lane = lax.broadcasted_iota(jnp.int32, (16, 128), 1)
    ones = (lane < 3).astype(f32).astype(bf16)
    zeros = jnp.zeros((dh, W), bf16)
    pad = jnp.zeros((112, W), bf16)

    def weigh(row, col, slot, j, masked):
        sl = slice(j * W, (j + 1) * W)
        run = jnp.ones((8, W), f32)
        if masked:
            ahead = (
                lax.broadcasted_iota(jnp.int32, (8, W), 1)
                + j * W
                - R * lax.broadcasted_iota(jnp.int32, (8, W), 0)
            )
        lhs = jnp.concatenate([kvr[row, col, :W], jnp.tile(ones, (W // 16, 1))], axis=1)
        for part in (0, 1):
            q = qr[slot, :, sl]
            stack = [q, zeros] if part == 0 else [zeros, q]
            rhs = jnp.concatenate(stack + [offt[:, sl], pad], axis=0)
            for v in range(0, W // 8, 2):
                if v % 8 == 0:
                    chunk = jnp.dot(lhs[8 * v : 8 * v + 64], rhs, preferred_element_type=f32)
                    score = [None] * v + [jnp.minimum(chunk[8 * w : 8 * w + 8], ZMAX) for w in range(8)]
                e0 = jnp.exp2(score[v])
                e1 = jnp.exp2(score[v + 1])
                if masked:
                    place_v = part * (W // 8) + v
                    e0 = jnp.where(ahead > R - 1 - place_v, e0, 0.0)
                    e1 = jnp.where(ahead > R - 2 - place_v, e1, 0.0)
                u0, u1 = 1.0 + e0, 1.0 + e1
                left = run * (1.0 / (u0 * u1))
                first = e0 * (u1 * left)
                second = e1 * left
                run = left
                base = part * W + 8 * v
                ws[j, base : base + 16] = jnp.concatenate([first, second], axis=0).astype(bf16)
        later = [None] * 8
        total = jnp.ones((1, W), f32)
        for i in range(7, -1, -1):
            later[i] = total
            total = total * run[i : i + 1]
        return jnp.concatenate(later + later, axis=0).astype(bf16), total

    def gather(row, col, j, later, total, first):
        sl = slice(j * W, (j + 1) * W)
        weight = (ws[j].reshape(B // 16, 16, W) * later[None]).reshape(B, W)
        vt = jnp.concatenate([kvr[row, col, W + p * dh : W + (p + 1) * dh] for p in range(4)], axis=1)
        part = jnp.dot(vt, weight, preferred_element_type=f32)
        acc[:, sl] = part if first else acc[:, sl] * total + part

    def o_copies(u, r, e, dst, dev):
        return (
            remote(obuf.at[u, r], orecv.at[dst], o_send.at[u * T + e], o_recv.at[dst], dev),
            remote(tbuf.at[u, r], trecv.at[dst], t_send.at[u * T + e], t_recv.at[dst], dev),
        )

    def send_out(u, slot, block, kept):
        lanes = lax.broadcasted_iota(jnp.int32, (dh // 2, 128), 1) < dh
        lanes_t = lax.broadcasted_iota(jnp.int32, (8, 128), 1) < dh
        for g in range(T // 2):
            cols = slice(g * 128, (g + 1) * 128)
            a, b = acc[: dh // 2, cols], acc[dh // 2 :, cols]
            ar, br = pltpu.roll(a, dh, 1), pltpu.roll(b, dh, 1)
            j, inner = g * 128 // W, g * 128 % W
            tt = jnp.broadcast_to(kept[j][:, inner : inner + 128], (8, 128))
            tr = pltpu.roll(tt, dh, 1)
            for odd in range(2):
                body = jnp.where(lanes, ar, b) if odd else jnp.where(lanes, a, br)
                fac = jnp.where(lanes_t, tr, tt) if odd else jnp.where(lanes_t, tt, tr)
                obuf[u, 2 * g + odd] = body.astype(bf16)
                tbuf[u, 2 * g + odd] = fac[:1]
        dst = slot * T * H + head
        for e in range(1, T):
            r = (t + e) % T
            for copy in o_copies(u, r, e, dst, (block, r)):
                copy.start()

        @pl.when(block != s)
        def _():
            for copy in o_copies(u, t, 0, dst, (block, t)):
                copy.start()

        @pl.when(block == s)
        def _():
            orecv[dst] = obuf[u, t]
            trecv[dst] = tbuf[u, t]

    def merge(slot, kept):
        remote(mbuf.at[slot], mbuf.at[slot], m_send.at[slot], m_recv.at[slot], (s, t)).wait_recv()
        out_kept = []
        for j in range(2):
            sl = slice(j * W, (j + 1) * W)
            acc[:, sl] = mbuf[slot, :dh, sl] * kept[j] + acc[:, sl]
            out_kept.append(mbuf[slot, dh : dh + 1, sl] * kept[j])
        return out_kept

    def self_unit(row):
        n = x if row == 0 else XS - 1 - x
        zq = kz if row == 0 else Z - 1 - kz
        slot = kz if row == 0 else Z
        q_wait(slot)
        for j in range(2):
            acc[:, j * W : (j + 1) * W] = jnp.zeros((dh, W), f32)

        def step(col, kept):
            found = [weigh(row, col, slot, j, False) for j in range(2)]
            for j in range(2):
                gather(row, col, j, *found[j], False)
            return tuple(kept[j] * found[j][1] for j in range(2))

        one = jnp.ones((1, W), f32)
        kept = lax.fori_loop(0, n, step, (one, one))
        found = [weigh(row, n, slot, j, True) for j in range(2)]
        for j in range(2):
            gather(row, n, j, *found[j], False)
        kept = [kept[j] * found[j][1] for j in range(2)]
        if row == 0:

            @pl.when(c == 0)
            def _():
                send_out(kz, g, zq * XS + n, kept)

            @pl.when(c == 1)
            def _():
                send_out(kz, g, zq * XS + n, merge(kz, kept))
        else:
            send_out(LAST, Z - 3 - kz, zq * XS + n, kept)

    def full(turn, unused):
        low_row = turn < Z
        far = Z - 1 - turn
        hop = (far + 1) // 2
        near = jnp.where(far % 2 == 1, z + hop, z + 2 * Z - hop) % Z
        zq = jnp.where(low_row, near, turn - Z)
        row = jnp.where(low_row, 0, 1)
        valid = jnp.where(low_row, zq - kz > 0, zq + kz >= Z)

        @pl.when(turn == 2)
        def _():
            kv_wait(1, x_back)
            kv_spread(1)[2].start()

        @pl.when(turn == Z)
        def _():
            kv_wait(1, x_on)
            kv_wait(1, x_far)

        @pl.when(valid)
        def _():
            @pl.when(low_row)
            def _():
                q_wait(zq)

                @pl.when(c == 0)
                def _():
                    q_forward(zq).start()

            kept = [None, None]
            waiting = None
            for col in range(XS):
                for j in range(2):
                    later, total = weigh(row, col, zq, j, False)
                    if waiting is not None:
                        gather(*waiting)
                    waiting = (row, col, j, later, total, col == 0)
                    kept[j] = total if col == 0 else kept[j] * total
            gather(*waiting)
            for j in range(2):
                factors[:, j * W : (j + 1) * W] = jnp.broadcast_to(kept[j], (8, W))

            handed = jnp.logical_and(low_row, c == 0)

            @pl.when(handed)
            def _():
                mbuf[zq, :dh] = acc[...]
                mbuf[zq, dh:] = factors[...]
                remote(mbuf.at[zq], mbuf.at[zq], m_send.at[zq], m_recv.at[zq], (s, partner)).start()

            @pl.when(jnp.logical_and(low_row, c == 1))
            def _():
                for j, both in enumerate(merge(zq, kept)):
                    factors[:, j * W : (j + 1) * W] = jnp.broadcast_to(both, (8, W))

            @pl.when(jnp.logical_not(handed))
            def _():
                u = jnp.where(low_row, zq, zq + 3)
                slot = jnp.where(low_row, g, Z - 3 - kz)
                send_out(u, slot, zq * XS + x, [factors[:1, j * W : (j + 1) * W] for j in range(2)])

        return unused

    go(w_copy(wrow(t), t, 0, partner))
    for e in range(1, Y):
        came = ((y + e) % Y) * 2 + c
        w_copy(wrow(t), came, 0, partner).wait_recv()
        go(w_copy(wrow(came), came, Y + e - 1, partner))
    kv_wait(0, x_on)
    kv_wait(0, x_far)
    lax.fori_loop(0, 2 * Z, full, 0)
    self_unit(0)
    self_unit(1)

    w_copy(wrow(t), partner, 0, partner).wait_recv()
    for e in range(1, Y):
        w_copy(wrow(t), ((y + e) % Y) * 2 + 1 - c, 0, partner).wait_recv()

    for hh in range(T * H):
        heads[hh] = jnp.zeros((dh // 2, 128), f32)

    def made_here(slot):
        low_made = jnp.where(c == 1, z >= kz, z == kz)
        high_made = jnp.logical_and(slot == Z - 3 - kz, z + kz >= Z)
        return jnp.logical_or(jnp.logical_and(slot == g, low_made), high_made)

    def combine(r, unused):
        for hh in range(T * H):

            @pl.when(jnp.logical_not(jnp.logical_and(hh == head, made_here(r))))
            def _():
                e = r * T * H + hh
                for copy in o_copies(0, 0, 0, e, (s, t)):
                    copy.wait_recv()

        for hh in range(T * H):
            heads[hh] = heads[hh] * trecv[r * T * H + hh] + orecv[r * T * H + hh].astype(f32)
        return unused

    slots = jnp.where(z < 2, 1, jnp.where(z < 4, 2, z - 1))
    lax.fori_loop(0, slots, combine, 0)

    lhs, rhs = [], []
    for q in range(T * H // 4):
        both = jnp.concatenate([heads[4 * q + a] for a in range(4)], axis=0).T
        for e in range(2):
            lhs.append(both[e * dh : (e + 1) * dh].astype(bf16))
            for a in range(4):
                base = (4 * q + a) * dh + e * (dh // 2)
                rhs.append(wg[base : base + dh // 2])
    projected = jnp.dot(
        jnp.concatenate(lhs, axis=1), jnp.concatenate(rhs, axis=0), preferred_element_type=f32
    )
    out[...] = scaled_rows(projected, gain_out[...])

    for copy in started:
        copy.wait_send()
    each_q(lambda copy: copy.wait_send())

    for i in range(H):
        stays, copy = kv_first(i)

        @pl.when(jnp.logical_not(stays))
        def _():
            copy.wait_send()

    for row in range(2):
        for copy in kv_spread(row):
            copy.wait_send()

    def sent(u, valid, block):
        @pl.when(valid)
        def _():
            for e in range(1, T):
                for copy in o_copies(u, 0, e, 0, (s, t)):
                    copy.wait_send()

            @pl.when(block != s)
            def _():
                for copy in o_copies(u, 0, 0, 0, (s, t)):
                    copy.wait_send()

    def sent_low(zq, unused):
        sent(zq, jnp.logical_or(zq == kz, jnp.logical_and(zq > kz, c == 1)), zq * XS + x)

        @pl.when(jnp.logical_and(zq > kz, c == 0))
        def _():
            q_forward(zq).wait_send()
            remote(mbuf.at[zq], mbuf.at[zq], m_send.at[zq], m_recv.at[zq], (s, partner)).wait_send()

        return unused

    def sent_high(zq, unused):
        sent(zq + 3, zq + kz >= Z, zq * XS + x)
        return unused

    lax.fori_loop(0, Z, sent_low, 0)
    lax.fori_loop(5, Z, sent_high, 0)
    sent(LAST, z >= 0, (Z - 1 - kz) * XS + XS - 1 - x)


def solution(mesh):
    S, T = mesh.shape["sp"], mesh.shape["tp"]

    def local(act, gain_in, wq, wk, wv, off, wo, gain_out):
        R, D = act.shape
        H = off.shape[0]
        dh = wq.shape[1] // H
        B = R * T
        Z = S // XS
        vmem = pl.BlockSpec(memory_space=pltpu.VMEM)
        hbm = pl.BlockSpec(memory_space=pl.ANY)
        smem = pl.BlockSpec(memory_space=pltpu.SMEM)
        dma = pltpu.SemaphoreType.DMA
        return pl.pallas_call(
            functools.partial(layer_kernel, S, T, H, dh),
            out_shape=jax.ShapeDtypeStruct((R, D), bf16),
            in_specs=[hbm, hbm, hbm, hbm, hbm, smem, hbm, hbm],
            out_specs=vmem,
            scratch_shapes=[
                pltpu.VMEM((R, D), bf16),
                pltpu.VMEM((1, D), f32),
                pltpu.VMEM((1, D), f32),
                pltpu.VMEM(wq.shape, bf16),
                pltpu.VMEM(wk.shape, bf16),
                pltpu.VMEM(wv.shape, bf16),
                pltpu.VMEM((B, D), bf16),
                pltpu.VMEM((wo.shape[0] * T, D), bf16),
                pltpu.VMEM((B, B), bf16),
                pltpu.VMEM((H, B, 128), bf16),
                pltpu.VMEM((H, dh, B), bf16),
                pltpu.VMEM((2, XS, B, 128), bf16),
                pltpu.VMEM((Z + 1, dh, B), bf16),
                pltpu.VMEM((16, B), bf16),
                pltpu.VMEM((2, B, B // 2), bf16),
                pltpu.VMEM((dh, B), f32),
                pltpu.VMEM((8, B), f32),
                pltpu.VMEM((Z, dh + 8, B), f32),
                pltpu.VMEM((2 * H, 1, 128), f32),
                pltpu.VMEM((LAST + 1, T, dh // 2, 128), bf16),
                pltpu.VMEM((6 * T * H, dh // 2, 128), bf16),
                pltpu.VMEM((LAST + 1, T, 1, 128), f32),
                pltpu.VMEM((6 * T * H, 1, 128), f32),
                pltpu.VMEM((T * H, dh // 2, 128), f32),
                dma((T,)),
                dma((T,)),
                dma((T,)),
                dma((T,)),
                dma((16,)),
                dma((4 * XS,)),
                dma((3 * H,)),
                dma((Z + 1,)),
                dma((Z + 1,)),
                dma((Z,)),
                dma((Z,)),
                dma((1,)),
                dma((1,)),
                dma(((LAST + 1) * T,)),
                dma((6 * T * H,)),
                dma(((LAST + 1) * T,)),
                dma((6 * T * H,)),
                dma((7,)),
            ],
            compiler_params=pltpu.CompilerParams(collective_id=0, has_side_effects=True, vmem_limit_bytes=67043328),
        )(act, gain_in.reshape(1, D), wq, wk, wv, off, wo, gain_out.reshape(1, D))

    in_specs = (
        P(("sp", "tp"), None),
        P(),
        P(None, "tp"),
        P(None, "tp"),
        P(None, "tp"),
        P("tp"),
        P("tp", None),
        P(),
    )
    out_specs = P(("sp", "tp"), None)
    return jax.shard_map(local, mesh=mesh, in_specs=in_specs, out_specs=out_specs, check_vma=False)
```

```python
import functools

import jax
import jax.numpy as jnp
from jax import lax
from jax.experimental import pallas as pl
from jax.experimental.pallas import tpu as pltpu
from jax.sharding import PartitionSpec as P

epsilon = 1e-06
log2e = 1.4426950408889634
MESH = pl.DeviceIdType.MESH
f32 = jnp.float32
bf16 = jnp.bfloat16
XS = 4
ZMAX = 63.0
LAST = 11
FIRST = 5
SELF_TURN = 9


def scaled_rows(widened, row_gain):
    spread = jnp.mean(widened * widened, axis=-1, keepdims=True)
    return (widened * lax.rsqrt(spread + epsilon) * row_gain).astype(bf16)


def layer_kernel(
    S,
    T,
    H,
    dh,
    act_hbm,
    gain_in_hbm,
    wq_hbm,
    wk_hbm,
    wv_hbm,
    off,
    wo_hbm,
    gain_out_hbm,
    out,
    act,
    gain_in,
    gain_out,
    wq,
    wk,
    wv,
    xg,
    wg,
    perm,
    kvb,
    qb,
    kvr,
    qr,
    offt,
    ws,
    acc,
    duo,
    factors,
    mbuf,
    offs,
    obuf,
    orecv,
    heads,
    x_send,
    x_recv,
    w_send,
    w_recv,
    kv_send,
    kv_recv,
    q_send,
    q_recv,
    f_send,
    m_send,
    m_recv,
    off_send,
    off_recv,
    o_send,
    o_recv,
    load,
):
    R = act.shape[0]
    B = R * T
    W = B // 2
    rows = wo_hbm.shape[0]
    Z = S // XS
    s = lax.axis_index("sp")
    t = lax.axis_index("tp")
    z, x = s // XS, s % XS
    y, c = t // 2, t % 2
    partner = y * 2 + 1 - c
    place_z = (z + 2) % Z
    g, hl = place_z // 4, place_z % 4
    kz = 2 * g + c
    head = 2 * H * y + hl
    home = hl // H == c

    def spot(group, local):
        return (4 * group + local + Z - 2) % Z

    Y = T // 2

    def remote(src, dst, send, recv, dev):
        return pltpu.make_async_remote_copy(
            src_ref=src, dst_ref=dst, send_sem=send, recv_sem=recv, device_id=dev, device_id_type=MESH
        )

    started = []

    def go(copy):
        copy.start()
        started.append(copy)
        return copy

    def xrow(index):
        return xg.at[pl.ds(pl.multiple_of(index * R, R), R)]

    def wrow(index):
        return wg.at[pl.ds(pl.multiple_of(index * rows, rows), rows)]

    def x_copy(index, slot, dev):
        return remote(xrow(index), xrow(index), x_send.at[slot], x_recv.at[index], (s, dev))

    def w_copy(src, index, slot, dev):
        return remote(src, wrow(index), w_send.at[slot], w_recv.at[index], (s, dev))

    early = [
        pltpu.make_async_copy(act_hbm, act, load.at[4]),
        pltpu.make_async_copy(gain_in_hbm, gain_in, load.at[5]),
    ]
    for copy in early:
        copy.start()
    loads = [
        pltpu.make_async_copy(wk_hbm, wk, load.at[0]),
        pltpu.make_async_copy(wv_hbm, wv, load.at[1]),
        pltpu.make_async_copy(wq_hbm, wq, load.at[2]),
        pltpu.make_async_copy(wo_hbm, wrow(t), load.at[3]),
        pltpu.make_async_copy(gain_out_hbm, gain_out, load.at[6]),
    ]
    for copy in loads:
        copy.start()
    barrier = pltpu.get_barrier_semaphore()
    partners = [(s, (t + d) % T) for d in range(1, T)]
    for d in range(Z):
        for core in range(2):
            if d:
                partners.append(((z + d) % Z * XS + x, 2 * y + core))
            partners.append(((z + d) % Z * XS + XS - 1 - x, 2 * y + core))
    partners += [(z * XS + (x + 2) % XS, t), (z * XS + (XS - 1 - x + 2) % XS, t)]
    for other in partners:
        pl.semaphore_signal(barrier, inc=1, device_id=other, device_id_type=MESH)
    for copy in early:
        copy.wait()
    xg[pl.ds(pl.multiple_of(t * R, R), R)] = scaled_rows(act[...].astype(f32), gain_in[...])
    pl.semaphore_wait(barrier, len(partners))
    onward = (y + 1 + (Y - 2) * c) % Y
    behind = (y + Y - 1 - (Y - 2) * c) % Y
    across = (y + 2) % Y
    go(x_copy(t, 1, onward * 2 + c))
    go(x_copy(t, 2, behind * 2 + c))
    go(x_copy(t, 0, partner))

    token = lax.broadcasted_iota(jnp.int32, (B, B), 0)
    place = lax.broadcasted_iota(jnp.int32, (B, B), 1)
    perm[...] = (token == (place & (T - 1)) * R + R - 1 - (place >> (T.bit_length() - 1))).astype(f32).astype(bf16)
    for i in range(H):
        offs[H * c + i] = jnp.broadcast_to(off[i] * log2e, (1, 128)).astype(f32)
    mine = offs.at[pl.ds(H * c, H)]
    go(remote(mine, mine, off_send.at[0], off_recv.at[0], (s, partner)))
    x_copy(behind * 2 + c, 0, partner).wait_recv()
    go(x_copy(behind * 2 + c, 3, onward * 2 + c))
    go(x_copy(behind * 2 + c, 4, partner))
    x_copy(onward * 2 + c, 0, partner).wait_recv()
    go(x_copy(onward * 2 + c, 5, partner))
    x_copy(across * 2 + c, 0, partner).wait_recv()
    go(x_copy(across * 2 + c, 6, partner))
    for copy in loads:
        copy.wait()
    for e in range(1, Y):
        go(w_copy(wrow(t), t, e, ((y + e) % Y) * 2 + c))
    x_copy(partner, 0, partner).wait_recv()
    for e in range(1, Y):
        x_copy(((y + e) % Y) * 2 + 1 - c, 0, partner).wait_recv()

    rows_all = xg[...]
    keys = jnp.dot(rows_all, wk[...], preferred_element_type=f32).astype(bf16).astype(f32)
    values = jnp.dot(rows_all, wv[...], preferred_element_type=f32).astype(bf16).astype(f32)
    turned = jnp.concatenate([keys.T, values.T], axis=0).astype(bf16)
    placed = jnp.dot(turned, perm[...], preferred_element_type=f32)
    keys_placed = placed[: H * dh].T
    for i in range(H):
        cols = slice(i * dh, (i + 1) * dh)
        kvb[i, :W] = jnp.concatenate([keys_placed[:W, cols], keys_placed[W:, cols]], axis=1).astype(bf16)
        for part in range(4):
            piece = placed[(H + i) * dh : (H + i + 1) * dh, part * 128 : (part + 1) * 128]
            kvb[i, W + part * dh : W + (part + 1) * dh] = piece.astype(bf16)

    outer = jnp.minimum(z, Z - 1 - z)

    class Both:
        def __init__(self, parts):
            self.parts = parts

        def start(self):
            for part in self.parts:
                part.start()

        def wait_send(self):
            for part in self.parts:
                part.wait_send()

    def kv_part(src, row, col, slot, dev, part):
        rows_of = pl.ds(part * W, W)
        return remote(
            src.at[rows_of],
            kvr.at[row, col, rows_of],
            kv_send.at[2 * slot + part],
            kv_recv.at[2 * (row * XS + col) + part],
            dev,
        )

    def kv_copy(src, row, col, slot, dev):
        return Both([kv_part(src, row, col, slot, dev, part) for part in range(2)])

    def kv_first(i):
        zd = spot(outer // 2, H * c + i)
        stays = jnp.logical_and(zd == z, outer % 2 == c)
        return stays, kv_copy(kvb.at[i], z // (Z // 2), x, i, (zd * XS + x, 2 * y + outer % 2))

    for i in range(H):
        stays, copy = kv_first(i)

        @pl.when(stays)
        def _():
            kvr[z // (Z // 2), x] = kvb[i]

        @pl.when(jnp.logical_not(stays))
        def _():
            copy.start()

    queries = jnp.dot(rows_all, wq[...], preferred_element_type=f32) * (dh ** (-0.5) * log2e)
    q_turned = queries.T.astype(bf16)
    for i in range(H):
        qb[i] = q_turned[i * dh : (i + 1) * dh]

    def q_first(i, group):
        zd = spot(group, H * c + i)
        stays = jnp.logical_and(zd == z, c == 0)
        copy = remote(qb.at[i], qr.at[z], q_send.at[i * 2 + group], q_recv.at[z], (zd * XS + x, 2 * y))
        return stays, z >= 2 * group, copy

    def q_extra(i):
        depth = Z - 1 - z
        zd = spot(depth // 2, H * c + i)
        dev = (zd * XS + XS - 1 - x, 2 * y + depth % 2)
        return remote(qb.at[i], qr.at[Z], q_send.at[2 * H + i], q_recv.at[Z], dev)

    def each_q(act_on):
        for group in (0, 1):
            for i in range(H):
                stays, wanted, copy = q_first(i, group)

                @pl.when(jnp.logical_and(wanted, jnp.logical_not(stays)))
                def _():
                    act_on(copy)

        @pl.when(z >= Z // 2)
        def _():
            for i in range(H):
                act_on(q_extra(i))

    for i in range(H):
        for group in (0, 1):
            stays, wanted, _ = q_first(i, group)

            @pl.when(jnp.logical_and(wanted, stays))
            def _():
                qr[z] = qb[i]


    def kv_wait(row, col):
        for part in range(2):
            kv_part(kvb.at[0], row, col, 0, (s, t), part).wait_recv()

    def q_forward(slot):
        return remote(qr.at[slot], qr.at[slot], f_send.at[slot], q_recv.at[slot], (s, partner))

    def q_wait(slot):
        local = jnp.logical_and(jnp.logical_and(slot == z, c == 0), hl // H == 0)

        @pl.when(jnp.logical_not(local))
        def _():
            q_forward(slot).wait_recv()

    def q_get(slot):
        q_wait(slot)

        @pl.when(c == 0)
        def _():
            q_forward(slot).start()

    x_on = (x + 1 + (XS - 2) * c) % XS
    x_back = (x + XS - 1 - (XS - 2) * c) % XS
    x_far = (x + 2) % XS

    def kv_spread(row):
        base = H + row * 3
        return (
            kv_copy(kvr.at[row, x], row, x, base, (z * XS + x_on, t)),
            kv_copy(kvr.at[row, x], row, x, base + 1, (z * XS + x_back, t)),
            kv_copy(kvr.at[row, x_back], row, x_back, base + 2, (z * XS + x_on, t)),
        )

    def kv_relay(row):
        local = jnp.logical_and(z == (kz if row == 0 else Z - 1 - kz), home)
        for part in range(2):

            @pl.when(jnp.logical_not(local))
            def _():
                kv_part(kvb.at[0], row, x, 0, (s, t), part).wait_recv()

            for copy in kv_spread(row)[:2]:
                copy.parts[part].start()

    kv_relay(0)
    each_q(lambda copy: copy.start())
    for part in range(2):
        kv_part(kvb.at[0], 0, x_back, 0, (s, t), part).wait_recv()
        kv_spread(0)[2].parts[part].start()
    kv_relay(1)

    theirs = offs.at[pl.ds(H * (1 - c), H)]
    remote(theirs, theirs, off_send.at[0], off_recv.at[0], (s, partner)).wait_recv()
    whole = jnp.concatenate([jnp.broadcast_to(offs[hl], (16, 128))] * (B // 128), axis=1)
    high = whole.astype(bf16).astype(f32)
    middle = (whole - high).astype(bf16).astype(f32)
    low = whole - high - middle
    part_row = lax.broadcasted_iota(jnp.int32, (16, B), 0)
    offt[...] = jnp.where(
        part_row == 0, high, jnp.where(part_row == 1, middle, jnp.where(part_row == 2, low, 0.0))
    ).astype(bf16)

    lane = lax.broadcasted_iota(jnp.int32, (16, 128), 1)
    ones = (lane < 3).astype(f32).astype(bf16)
    zeros = jnp.zeros((dh, W), bf16)
    pad = jnp.zeros((112, W), bf16)

    def weigh(row, col, slot, j, masked):
        sl = slice(j * W, (j + 1) * W)
        run = jnp.ones((8, W), f32)
        if masked:
            ahead = (
                lax.broadcasted_iota(jnp.int32, (8, W), 1)
                + j * W
                - R * lax.broadcasted_iota(jnp.int32, (8, W), 0)
            )
        lhs = jnp.concatenate([kvr[row, col, :W], jnp.tile(ones, (W // 16, 1))], axis=1)
        for part in (0, 1):
            q = qr[slot, :, sl]
            stack = [q, zeros] if part == 0 else [zeros, q]
            rhs = jnp.concatenate(stack + [offt[:, sl], pad], axis=0)
            for v in range(0, W // 8, 2):
                if v % 8 == 0:
                    chunk = jnp.dot(lhs[8 * v : 8 * v + 64], rhs, preferred_element_type=f32)
                    score = [None] * v + [jnp.minimum(chunk[8 * w : 8 * w + 8], ZMAX) for w in range(8)]
                e0 = jnp.exp2(score[v])
                e1 = jnp.exp2(score[v + 1])
                if masked:
                    place_v = part * (W // 8) + v
                    e0 = jnp.where(ahead > R - 1 - place_v, e0, 0.0)
                    e1 = jnp.where(ahead > R - 2 - place_v, e1, 0.0)
                u0, u1 = 1.0 + e0, 1.0 + e1
                left = run * (1.0 / (u0 * u1))
                first = e0 * (u1 * left)
                second = e1 * left
                run = left
                base = part * W + 8 * v
                ws[j, base : base + 16] = jnp.concatenate([first, second], axis=0).astype(bf16)
        later = [None] * 8
        total = jnp.ones((1, W), f32)
        for i in range(7, -1, -1):
            later[i] = total
            total = total * run[i : i + 1]
        return jnp.concatenate(later + later, axis=0).astype(bf16), total

    def gather(row, col, j, later, total, first):
        sl = slice(j * W, (j + 1) * W)
        weight = (ws[j].reshape(B // 16, 16, W) * later[None]).reshape(B, W)
        vt = jnp.concatenate([kvr[row, col, W + p * dh : W + (p + 1) * dh] for p in range(4)], axis=1)
        part = jnp.dot(vt, weight, preferred_element_type=f32)
        if first is None:
            duo[row, :, sl] = duo[row, :, sl] * total + part
        else:
            acc[:, sl] = part if first else acc[:, sl] * total + part

    def o_copies(u, r, e, dst, dev):
        return (
            remote(obuf.at[u, r], orecv.at[dst], o_send.at[u * T + e], o_recv.at[dst], dev),
        )

    def send_out(u, slot, block, kept):
        lanes = lax.broadcasted_iota(jnp.int32, (dh // 2, 128), 1) < dh
        top = lax.broadcasted_iota(jnp.int32, (8, 128), 0) == 0
        lanes_t = lax.broadcasted_iota(jnp.int32, (8, 128), 1) < dh
        for g in range(T // 2):
            cols = slice(g * 128, (g + 1) * 128)
            a, b = acc[: dh // 2, cols], acc[dh // 2 :, cols]
            ar, br = pltpu.roll(a, dh, 1), pltpu.roll(b, dh, 1)
            j, inner = g * 128 // W, g * 128 % W
            tt = jnp.broadcast_to(kept[j][:, inner : inner + 128], (8, 128))
            tr = pltpu.roll(tt, dh, 1)
            for odd in range(2):
                body = jnp.where(lanes, ar, b) if odd else jnp.where(lanes, a, br)
                fac = jnp.where(lanes_t, tr, tt) if odd else jnp.where(lanes_t, tt, tr)
                fac_high = fac.astype(bf16).astype(f32)
                tail = jnp.where(top, fac_high, fac - fac_high)
                obuf[u, 2 * g + odd] = jnp.concatenate([body, tail], axis=0).astype(bf16)
        dst = slot * T * H + head
        for e in range(1, T):
            r = (t + e) % T
            for copy in o_copies(u, r, e, dst, (block, r)):
                copy.start()

        @pl.when(block != s)
        def _():
            for copy in o_copies(u, t, 0, dst, (block, t)):
                copy.start()

        @pl.when(block == s)
        def _():
            orecv[dst] = obuf[u, t]

    def merge(slot, kept):
        remote(mbuf.at[slot], mbuf.at[slot], m_send.at[slot], m_recv.at[slot], (s, t)).wait_recv()
        out_kept = []
        for j in range(2):
            sl = slice(j * W, (j + 1) * W)
            acc[:, sl] = mbuf[slot, :dh, sl] * kept[j] + acc[:, sl]
            out_kept.append(mbuf[slot, dh : dh + 1, sl] * kept[j])
        return out_kept

    def self_units():
        slots = (kz, Z)
        q_wait(slots[0])
        q_wait(slots[1])
        ends = (x, XS - 1 - x)
        duo[...] = jnp.zeros((2, dh, B), f32)
        one = jnp.ones((1, W), f32)
        kept = [[one, one], [one, one]]
        waiting = None
        for p in range(XS + 1):
            if p < XS - 1:
                row = jnp.where(p < x, 0, 1)
                col = jnp.where(p < x, p, p - x)
                slot = jnp.where(p < x, kz, Z)
            else:
                row = p - XS + 1
                col, slot = ends[row], slots[row]
            for j in range(2):
                later, total = weigh(row, col, slot, j, p >= XS - 1)
                if waiting is not None:
                    gather(*waiting)
                waiting = (row, col, j, later, total, None)
                for k in range(2):
                    kept[k][j] = kept[k][j] * (jnp.where(row == k, total, 1.0) if p < XS - 1 else total if row == k else one)
        gather(*waiting)

        acc[...] = duo[0]

        @pl.when(c == 0)
        def _():
            send_out(kz, g, kz * XS + x, kept[0])

        @pl.when(c == 1)
        def _():
            send_out(kz, g, kz * XS + x, merge(kz, kept[0]))

        acc[...] = duo[1]
        send_out(LAST, Z - 3 - kz, (Z - 1 - kz) * XS + XS - 1 - x, kept[1])

    def full(turn, unused):
        low_row = jnp.logical_or(turn <= FIRST, turn > FIRST + 3)
        far = jnp.where(turn < FIRST, Z - 1 - turn, Z + 3 - turn)
        hop = (far + 1) // 2
        near = jnp.where(far % 2 == 1, z + hop, z + 2 * Z - hop) % Z
        shared = 2 * g + 1
        zq = jnp.where(turn == FIRST, shared, jnp.where(low_row, near, Z + FIRST - turn))
        row = jnp.where(low_row, 0, 1)
        low_valid = jnp.where(turn == FIRST, c == 0, zq > shared)
        valid = jnp.where(low_row, low_valid, zq + kz >= Z)

        @pl.when(turn == 1)
        def _():
            kv_wait(1, x_back)
            kv_spread(1)[2].start()

        @pl.when(turn == FIRST)
        def _():
            for step in (0, 1, Z - 1):
                close = (z + step) % Z

                @pl.when(close >= Z - 1 - 2 * g)
                def _():
                    q_get(close)

        @pl.when(turn == FIRST + 1)
        def _():
            kv_wait(1, x_on)
            kv_wait(1, x_far)

        @pl.when(turn == SELF_TURN)
        def _():
            self_units()

        @pl.when(valid)
        def _():
            @pl.when(jnp.logical_and(low_row, jnp.logical_or(turn <= FIRST, zq < Z - 1 - 2 * g)))
            def _():
                q_get(zq)

            kept = [None, None]
            waiting = None
            for col in range(XS):
                for j in range(2):
                    later, total = weigh(row, col, zq, j, False)
                    if waiting is not None:
                        gather(*waiting)
                    waiting = (row, col, j, later, total, col == 0)
                    kept[j] = total if col == 0 else kept[j] * total
            gather(*waiting)
            for j in range(2):
                factors[:, j * W : (j + 1) * W] = jnp.broadcast_to(kept[j], (8, W))

            handed = jnp.logical_and(low_row, c == 0)

            @pl.when(handed)
            def _():
                mbuf[zq, :dh] = acc[...]
                mbuf[zq, dh:] = factors[...]
                remote(mbuf.at[zq], mbuf.at[zq], m_send.at[zq], m_recv.at[zq], (s, partner)).start()

            @pl.when(jnp.logical_and(low_row, c == 1))
            def _():
                for j, both in enumerate(merge(zq, kept)):
                    factors[:, j * W : (j + 1) * W] = jnp.broadcast_to(both, (8, W))

            @pl.when(jnp.logical_not(handed))
            def _():
                u = jnp.where(low_row, zq, zq + 3)
                slot = jnp.where(low_row, g, Z - 3 - kz)
                send_out(u, slot, zq * XS + x, [factors[:1, j * W : (j + 1) * W] for j in range(2)])

        return unused

    go(w_copy(wrow(t), t, 0, partner))
    for e in range(1, Y):
        came = ((y + e) % Y) * 2 + c
        w_copy(wrow(t), came, 0, partner).wait_recv()
        go(w_copy(wrow(came), came, Y + e - 1, partner))
    kv_wait(0, x_on)
    kv_wait(0, x_far)
    lax.fori_loop(0, Z + 4, full, 0)
    w_copy(wrow(t), partner, 0, partner).wait_recv()
    for e in range(1, Y):
        w_copy(wrow(t), ((y + e) % Y) * 2 + 1 - c, 0, partner).wait_recv()

    for hh in range(T * H):
        heads[hh] = jnp.zeros((dh // 2, 128), f32)

    def made_here(slot):
        low_made = jnp.where(c == 1, z >= kz, z == kz)
        high_made = jnp.logical_and(slot == Z - 3 - kz, z + kz >= Z)
        return jnp.logical_or(jnp.logical_and(slot == g, low_made), high_made)

    def combine(r, unused):
        for hh in range(T * H):

            @pl.when(jnp.logical_not(jnp.logical_and(hh == head, made_here(r))))
            def _():
                e = r * T * H + hh
                for copy in o_copies(0, 0, 0, e, (s, t)):
                    copy.wait_recv()

        for hh in range(T * H):
            got = orecv[r * T * H + hh].astype(f32)
            fac = got[dh // 2 : dh // 2 + 1] + got[dh // 2 + 1 : dh // 2 + 2]
            heads[hh] = heads[hh] * fac + got[: dh // 2]
        return unused

    slots = jnp.where(z < 2, 1, jnp.where(z < 4, 2, z - 1))
    lax.fori_loop(0, slots, combine, 0)

    lhs, rhs = [], []
    for q in range(T * H // 4):
        both = jnp.concatenate([heads[4 * q + a] for a in range(4)], axis=0).T
        for e in range(2):
            lhs.append(both[e * dh : (e + 1) * dh].astype(bf16))
            for a in range(4):
                base = (4 * q + a) * dh + e * (dh // 2)
                rhs.append(wg[base : base + dh // 2])
    projected = jnp.dot(
        jnp.concatenate(lhs, axis=1), jnp.concatenate(rhs, axis=0), preferred_element_type=f32
    )
    out[...] = scaled_rows(projected, gain_out[...])

    for copy in started:
        copy.wait_send()
    each_q(lambda copy: copy.wait_send())

    for i in range(H):
        stays, copy = kv_first(i)

        @pl.when(jnp.logical_not(stays))
        def _():
            copy.wait_send()

    for row in range(2):
        for copy in kv_spread(row):
            copy.wait_send()

    def sent(u, valid, block):
        @pl.when(valid)
        def _():
            for e in range(1, T):
                for copy in o_copies(u, 0, e, 0, (s, t)):
                    copy.wait_send()

            @pl.when(block != s)
            def _():
                for copy in o_copies(u, 0, 0, 0, (s, t)):
                    copy.wait_send()

    def sent_low(zq, unused):
        sent(zq, jnp.logical_or(zq == kz, jnp.logical_and(zq > kz, c == 1)), zq * XS + x)

        @pl.when(jnp.logical_and(zq > kz, c == 0))
        def _():
            q_forward(zq).wait_send()
            remote(mbuf.at[zq], mbuf.at[zq], m_send.at[zq], m_recv.at[zq], (s, partner)).wait_send()

        return unused

    def sent_high(zq, unused):
        sent(zq + 3, zq + kz >= Z, zq * XS + x)
        return unused

    lax.fori_loop(0, Z, sent_low, 0)
    lax.fori_loop(5, Z, sent_high, 0)
    sent(LAST, z >= 0, (Z - 1 - kz) * XS + XS - 1 - x)


def solution(mesh):
    S, T = mesh.shape["sp"], mesh.shape["tp"]

    def local(act, gain_in, wq, wk, wv, off, wo, gain_out):
        R, D = act.shape
        H = off.shape[0]
        dh = wq.shape[1] // H
        B = R * T
        Z = S // XS
        vmem = pl.BlockSpec(memory_space=pltpu.VMEM)
        hbm = pl.BlockSpec(memory_space=pl.ANY)
        smem = pl.BlockSpec(memory_space=pltpu.SMEM)
        dma = pltpu.SemaphoreType.DMA
        return pl.pallas_call(
            functools.partial(layer_kernel, S, T, H, dh),
            out_shape=jax.ShapeDtypeStruct((R, D), bf16),
            in_specs=[hbm, hbm, hbm, hbm, hbm, smem, hbm, hbm],
            out_specs=vmem,
            scratch_shapes=[
                pltpu.VMEM((R, D), bf16),
                pltpu.VMEM((1, D), f32),
                pltpu.VMEM((1, D), f32),
                pltpu.VMEM(wq.shape, bf16),
                pltpu.VMEM(wk.shape, bf16),
                pltpu.VMEM(wv.shape, bf16),
                pltpu.VMEM((B, D), bf16),
                pltpu.VMEM((wo.shape[0] * T, D), bf16),
                pltpu.VMEM((B, B), bf16),
                pltpu.VMEM((H, B, 128), bf16),
                pltpu.VMEM((H, dh, B), bf16),
                pltpu.VMEM((2, XS, B, 128), bf16),
                pltpu.VMEM((Z + 1, dh, B), bf16),
                pltpu.VMEM((16, B), bf16),
                pltpu.VMEM((2, B, B // 2), bf16),
                pltpu.VMEM((dh, B), f32),
                pltpu.VMEM((2, dh, B), f32),
                pltpu.VMEM((8, B), f32),
                pltpu.VMEM((Z, dh + 8, B), f32),
                pltpu.VMEM((2 * H, 1, 128), f32),
                pltpu.VMEM((LAST + 1, T, dh // 2 + 8, 128), bf16),
                pltpu.VMEM((6 * T * H, dh // 2 + 8, 128), bf16),
                pltpu.VMEM((T * H, dh // 2, 128), f32),
                dma((T,)),
                dma((T,)),
                dma((T,)),
                dma((T,)),
                dma((16,)),
                dma((4 * XS,)),
                dma((3 * H,)),
                dma((Z + 1,)),
                dma((Z + 1,)),
                dma((Z,)),
                dma((Z,)),
                dma((1,)),
                dma((1,)),
                dma(((LAST + 1) * T,)),
                dma((6 * T * H,)),
                dma((7,)),
            ],
            compiler_params=pltpu.CompilerParams(collective_id=0, has_side_effects=True, vmem_limit_bytes=67043328),
        )(act, gain_in.reshape(1, D), wq, wk, wv, off, wo, gain_out.reshape(1, D))

    in_specs = (
        P(("sp", "tp"), None),
        P(),
        P(None, "tp"),
        P(None, "tp"),
        P(None, "tp"),
        P("tp"),
        P("tp", None),
        P(),
    )
    out_specs = P(("sp", "tp"), None)
    return jax.shard_map(local, mesh=mesh, in_specs=in_specs, out_specs=out_specs, check_vma=False)
```

```python
import functools

import jax
import jax.numpy as jnp
from jax import lax
from jax.experimental import pallas as pl
from jax.experimental.pallas import tpu as pltpu
from jax.sharding import PartitionSpec as P

epsilon = 1e-06
log2e = 1.4426950408889634
MESH = pl.DeviceIdType.MESH
f32 = jnp.float32
bf16 = jnp.bfloat16
XS = 4
ZMAX = 63.0
LAST = 11
FIRST = 5
SELF_TURN = 9


def scaled_rows(widened, row_gain):
    spread = jnp.mean(widened * widened, axis=-1, keepdims=True)
    return (widened * lax.rsqrt(spread + epsilon) * row_gain).astype(bf16)


def layer_kernel(
    S,
    T,
    H,
    dh,
    act_hbm,
    gain_in_hbm,
    wq_hbm,
    wk_hbm,
    wv_hbm,
    off,
    wo_hbm,
    gain_out_hbm,
    out,
    act,
    gain_in,
    gain_out,
    weights,
    rows_q,
    xg,
    wg,
    perm,
    kvb,
    qb,
    kvr,
    qr,
    offt,
    ws,
    acc,
    duo,
    factors,
    mbuf,
    offs,
    obuf,
    orecv,
    heads,
    x_send,
    x_recv,
    w_send,
    w_recv,
    kv_send,
    kv_recv,
    q_send,
    q_recv,
    f_send,
    m_send,
    m_recv,
    off_send,
    off_recv,
    o_send,
    o_recv,
    load,
):
    R = act.shape[0]
    B = R * T
    W = B // 2
    rows = wo_hbm.shape[0]
    Z = S // XS
    s = lax.axis_index("sp")
    t = lax.axis_index("tp")
    z, x = s // XS, s % XS
    y, c = t // 2, t % 2
    partner = y * 2 + 1 - c
    place_z = (z + 2) % Z
    g, hl = place_z // 4, place_z % 4
    kz = 2 * g + c
    head = 2 * H * y + hl
    home = hl // H == c

    def spot(group, local):
        return (4 * group + local + Z - 2) % Z

    Y = T // 2

    def remote(src, dst, send, recv, dev):
        return pltpu.make_async_remote_copy(
            src_ref=src, dst_ref=dst, send_sem=send, recv_sem=recv, device_id=dev, device_id_type=MESH
        )

    started = []

    def go(copy):
        copy.start()
        started.append(copy)
        return copy

    def xrow(index):
        return xg.at[pl.ds(pl.multiple_of(index * R, R), R)]

    def wrow(index):
        return wg.at[pl.ds(pl.multiple_of(index * rows, rows), rows)]

    def x_copy(index, slot, dev):
        return remote(xrow(index), xrow(index), x_send.at[slot], x_recv.at[index], (s, dev))

    def w_copy(src, index, slot, dev):
        return remote(src, wrow(index), w_send.at[slot], w_recv.at[index], (s, dev))

    early = [
        pltpu.make_async_copy(act_hbm, act, load.at[4]),
        pltpu.make_async_copy(gain_in_hbm, gain_in, load.at[5]),
    ]
    for copy in early:
        copy.start()
    loads = [
        pltpu.make_async_copy(wk_hbm, weights.at[:, : H * dh], load.at[0]),
        pltpu.make_async_copy(wv_hbm, weights.at[:, H * dh : 2 * H * dh], load.at[1]),
        pltpu.make_async_copy(wq_hbm, weights.at[:, 2 * H * dh :], load.at[2]),
        pltpu.make_async_copy(wo_hbm, wrow(t), load.at[3]),
        pltpu.make_async_copy(gain_out_hbm, gain_out, load.at[6]),
    ]
    for copy in loads:
        copy.start()
    barrier = pltpu.get_barrier_semaphore()
    partners = [(s, (t + d) % T) for d in range(1, T)]
    for d in range(Z):
        for core in range(2):
            if d:
                partners.append(((z + d) % Z * XS + x, 2 * y + core))
            partners.append(((z + d) % Z * XS + XS - 1 - x, 2 * y + core))
    partners += [(z * XS + (x + 2) % XS, t), (z * XS + (XS - 1 - x + 2) % XS, t)]
    for other in partners:
        pl.semaphore_signal(barrier, inc=1, device_id=other, device_id_type=MESH)
    for copy in early:
        copy.wait()
    xg[pl.ds(pl.multiple_of(t * R, R), R)] = scaled_rows(act[...].astype(f32), gain_in[...])
    pl.semaphore_wait(barrier, len(partners))
    onward = (y + 1 + (Y - 2) * c) % Y
    behind = (y + Y - 1 - (Y - 2) * c) % Y
    across = (y + 2) % Y
    go(x_copy(t, 1, onward * 2 + c))
    go(x_copy(t, 2, behind * 2 + c))
    go(x_copy(t, 0, partner))

    token = lax.broadcasted_iota(jnp.int32, (B, B), 0)
    place = lax.broadcasted_iota(jnp.int32, (B, B), 1)
    perm[...] = (token == (place & (T - 1)) * R + R - 1 - (place >> (T.bit_length() - 1))).astype(f32).astype(bf16)
    for i in range(H):
        offs[H * c + i] = jnp.broadcast_to(off[i] * log2e, (1, 128)).astype(f32)
    mine = offs.at[pl.ds(H * c, H)]
    go(remote(mine, mine, off_send.at[0], off_recv.at[0], (s, partner)))
    def project(chip):
        rows_of = pl.ds(pl.multiple_of(chip * 2 * R, 2 * R), 2 * R)
        rows_q[rows_of] = jnp.dot(xg[rows_of], weights[...], preferred_element_type=f32)

    for copy in loads:
        copy.wait()
    x_copy(partner, 0, partner).wait_recv()
    project(y)
    x_copy(behind * 2 + c, 0, partner).wait_recv()
    go(x_copy(behind * 2 + c, 3, onward * 2 + c))
    go(x_copy(behind * 2 + c, 4, partner))
    x_copy(onward * 2 + c, 0, partner).wait_recv()
    go(x_copy(onward * 2 + c, 5, partner))
    for chip in (behind, onward):
        x_copy(chip * 2 + 1 - c, 0, partner).wait_recv()
        project(chip)
    x_copy(across * 2 + c, 0, partner).wait_recv()
    go(x_copy(across * 2 + c, 6, partner))
    for e in range(1, Y):
        go(w_copy(wrow(t), t, e, ((y + e) % Y) * 2 + c))
    x_copy(across * 2 + 1 - c, 0, partner).wait_recv()
    project(across)
    keys = rows_q[:, : H * dh].astype(bf16).astype(f32)
    values = rows_q[:, H * dh : 2 * H * dh].astype(bf16).astype(f32)
    turned = jnp.concatenate([keys.T, values.T], axis=0).astype(bf16)
    placed = jnp.dot(turned, perm[...], preferred_element_type=f32)
    keys_placed = placed[: H * dh].T
    for i in range(H):
        cols = slice(i * dh, (i + 1) * dh)
        kvb[i, :W] = jnp.concatenate([keys_placed[:W, cols], keys_placed[W:, cols]], axis=1).astype(bf16)
        for part in range(4):
            piece = placed[(H + i) * dh : (H + i + 1) * dh, part * 128 : (part + 1) * 128]
            kvb[i, W + part * dh : W + (part + 1) * dh] = piece.astype(bf16)

    outer = jnp.minimum(z, Z - 1 - z)

    class Both:
        def __init__(self, parts):
            self.parts = parts

        def start(self):
            for part in self.parts:
                part.start()

        def wait_send(self):
            for part in self.parts:
                part.wait_send()

    def kv_part(src, row, col, slot, dev, part):
        rows_of = pl.ds(part * W, W)
        return remote(
            src.at[rows_of],
            kvr.at[row, col, rows_of],
            kv_send.at[2 * slot + part],
            kv_recv.at[2 * (row * XS + col) + part],
            dev,
        )

    def kv_copy(src, row, col, slot, dev):
        return Both([kv_part(src, row, col, slot, dev, part) for part in range(2)])

    def kv_first(i):
        zd = spot(outer // 2, H * c + i)
        stays = jnp.logical_and(zd == z, outer % 2 == c)
        return stays, kv_copy(kvb.at[i], z // (Z // 2), x, i, (zd * XS + x, 2 * y + outer % 2))

    for i in range(H):
        stays, copy = kv_first(i)

        @pl.when(stays)
        def _():
            kvr[z // (Z // 2), x] = kvb[i]

        @pl.when(jnp.logical_not(stays))
        def _():
            copy.start()

    queries = rows_q[:, 2 * H * dh :] * (dh ** (-0.5) * log2e)
    q_turned = queries.T.astype(bf16)
    for i in range(H):
        qb[i] = q_turned[i * dh : (i + 1) * dh]

    def q_first(i, group):
        zd = spot(group, H * c + i)
        stays = jnp.logical_and(zd == z, c == 0)
        copy = remote(qb.at[i], qr.at[z], q_send.at[i * 2 + group], q_recv.at[z], (zd * XS + x, 2 * y))
        return stays, z >= 2 * group, copy

    def q_extra(i):
        depth = Z - 1 - z
        zd = spot(depth // 2, H * c + i)
        dev = (zd * XS + XS - 1 - x, 2 * y + depth % 2)
        return remote(qb.at[i], qr.at[Z], q_send.at[2 * H + i], q_recv.at[Z], dev)

    def each_q(act_on):
        for group in (0, 1):
            for i in range(H):
                stays, wanted, copy = q_first(i, group)

                @pl.when(jnp.logical_and(wanted, jnp.logical_not(stays)))
                def _():
                    act_on(copy)

        @pl.when(z >= Z // 2)
        def _():
            for i in range(H):
                act_on(q_extra(i))

    for i in range(H):
        for group in (0, 1):
            stays, wanted, _ = q_first(i, group)

            @pl.when(jnp.logical_and(wanted, stays))
            def _():
                qr[z] = qb[i]


    def kv_wait(row, col):
        for part in range(2):
            kv_part(kvb.at[0], row, col, 0, (s, t), part).wait_recv()

    def q_forward(slot):
        return remote(qr.at[slot], qr.at[slot], f_send.at[slot], q_recv.at[slot], (s, partner))

    def q_wait(slot):
        local = jnp.logical_and(jnp.logical_and(slot == z, c == 0), hl // H == 0)

        @pl.when(jnp.logical_not(local))
        def _():
            q_forward(slot).wait_recv()

    def q_get(slot):
        q_wait(slot)

        @pl.when(c == 0)
        def _():
            q_forward(slot).start()

    x_on = (x + 1 + (XS - 2) * c) % XS
    x_back = (x + XS - 1 - (XS - 2) * c) % XS
    x_far = (x + 2) % XS

    def kv_spread(row):
        base = H + row * 3
        return (
            kv_copy(kvr.at[row, x], row, x, base, (z * XS + x_on, t)),
            kv_copy(kvr.at[row, x], row, x, base + 1, (z * XS + x_back, t)),
            kv_copy(kvr.at[row, x_back], row, x_back, base + 2, (z * XS + x_on, t)),
        )

    def kv_relay(row):
        local = jnp.logical_and(z == (kz if row == 0 else Z - 1 - kz), home)
        for part in range(2):

            @pl.when(jnp.logical_not(local))
            def _():
                kv_part(kvb.at[0], row, x, 0, (s, t), part).wait_recv()

            for copy in kv_spread(row)[:2]:
                copy.parts[part].start()

    kv_relay(0)
    each_q(lambda copy: copy.start())
    for part in range(2):
        kv_part(kvb.at[0], 0, x_back, 0, (s, t), part).wait_recv()
        kv_spread(0)[2].parts[part].start()
    kv_relay(1)

    theirs = offs.at[pl.ds(H * (1 - c), H)]
    remote(theirs, theirs, off_send.at[0], off_recv.at[0], (s, partner)).wait_recv()
    whole = jnp.concatenate([jnp.broadcast_to(offs[hl], (16, 128))] * (B // 128), axis=1)
    high = whole.astype(bf16).astype(f32)
    middle = (whole - high).astype(bf16).astype(f32)
    low = whole - high - middle
    part_row = lax.broadcasted_iota(jnp.int32, (16, B), 0)
    offt[...] = jnp.where(
        part_row == 0, high, jnp.where(part_row == 1, middle, jnp.where(part_row == 2, low, 0.0))
    ).astype(bf16)

    lane = lax.broadcasted_iota(jnp.int32, (16, 128), 1)
    ones = (lane < 3).astype(f32).astype(bf16)
    zeros = jnp.zeros((dh, W), bf16)
    pad = jnp.zeros((112, W), bf16)

    def weigh(row, col, slot, j, masked):
        sl = slice(j * W, (j + 1) * W)
        run = jnp.ones((8, W), f32)
        if masked:
            ahead = (
                lax.broadcasted_iota(jnp.int32, (8, W), 1)
                + j * W
                - R * lax.broadcasted_iota(jnp.int32, (8, W), 0)
            )
        lhs = jnp.concatenate([kvr[row, col, :W], jnp.tile(ones, (W // 16, 1))], axis=1)
        for part in (0, 1):
            q = qr[slot, :, sl]
            stack = [q, zeros] if part == 0 else [zeros, q]
            rhs = jnp.concatenate(stack + [offt[:, sl], pad], axis=0)
            for v in range(0, W // 8, 2):
                if v % 8 == 0:
                    chunk = jnp.dot(lhs[8 * v : 8 * v + 64], rhs, preferred_element_type=f32)
                    score = [None] * v + [jnp.minimum(chunk[8 * w : 8 * w + 8], ZMAX) for w in range(8)]
                e0 = jnp.exp2(score[v])
                e1 = jnp.exp2(score[v + 1])
                if masked:
                    place_v = part * (W // 8) + v
                    e0 = jnp.where(ahead > R - 1 - place_v, e0, 0.0)
                    e1 = jnp.where(ahead > R - 2 - place_v, e1, 0.0)
                u0, u1 = 1.0 + e0, 1.0 + e1
                left = run * (1.0 / (u0 * u1))
                first = e0 * (u1 * left)
                second = e1 * left
                run = left
                base = part * W + 8 * v
                ws[j, base : base + 16] = jnp.concatenate([first, second], axis=0).astype(bf16)
        later = [None] * 8
        total = jnp.ones((1, W), f32)
        for i in range(7, -1, -1):
            later[i] = total
            total = total * run[i : i + 1]
        return jnp.concatenate(later + later, axis=0).astype(bf16), total

    def gather(row, col, j, later, total, first):
        sl = slice(j * W, (j + 1) * W)
        weight = (ws[j].reshape(B // 16, 16, W) * later[None]).reshape(B, W)
        vt = jnp.concatenate([kvr[row, col, W + p * dh : W + (p + 1) * dh] for p in range(4)], axis=1)
        part = jnp.dot(vt, weight, preferred_element_type=f32)
        if first is None:
            duo[row, :, sl] = duo[row, :, sl] * total + part
        else:
            acc[:, sl] = part if first else acc[:, sl] * total + part

    def o_copies(u, r, e, dst, dev):
        return (
            remote(obuf.at[u, r], orecv.at[dst], o_send.at[u * T + e], o_recv.at[dst], dev),
        )

    def send_out(u, slot, block, kept):
        lanes = lax.broadcasted_iota(jnp.int32, (dh // 2, 128), 1) < dh
        top = lax.broadcasted_iota(jnp.int32, (8, 128), 0) == 0
        lanes_t = lax.broadcasted_iota(jnp.int32, (8, 128), 1) < dh
        for g in range(T // 2):
            cols = slice(g * 128, (g + 1) * 128)
            a, b = acc[: dh // 2, cols], acc[dh // 2 :, cols]
            ar, br = pltpu.roll(a, dh, 1), pltpu.roll(b, dh, 1)
            j, inner = g * 128 // W, g * 128 % W
            tt = jnp.broadcast_to(kept[j][:, inner : inner + 128], (8, 128))
            tr = pltpu.roll(tt, dh, 1)
            for odd in range(2):
                body = jnp.where(lanes, ar, b) if odd else jnp.where(lanes, a, br)
                fac = jnp.where(lanes_t, tr, tt) if odd else jnp.where(lanes_t, tt, tr)
                fac_high = fac.astype(bf16).astype(f32)
                tail = jnp.where(top, fac_high, fac - fac_high)
                obuf[u, 2 * g + odd] = jnp.concatenate([body, tail], axis=0).astype(bf16)
        dst = slot * T * H + head
        for e in range(1, T):
            r = (t + e) % T
            for copy in o_copies(u, r, e, dst, (block, r)):
                copy.start()

        @pl.when(block != s)
        def _():
            for copy in o_copies(u, t, 0, dst, (block, t)):
                copy.start()

        @pl.when(block == s)
        def _():
            orecv[dst] = obuf[u, t]

    def merge(slot, kept):
        remote(mbuf.at[slot], mbuf.at[slot], m_send.at[slot], m_recv.at[slot], (s, t)).wait_recv()
        out_kept = []
        for j in range(2):
            sl = slice(j * W, (j + 1) * W)
            acc[:, sl] = mbuf[slot, :dh, sl] * kept[j] + acc[:, sl]
            out_kept.append(mbuf[slot, dh : dh + 1, sl] * kept[j])
        return out_kept

    def self_units():
        slots = (kz, Z)
        q_wait(slots[0])
        q_wait(slots[1])
        ends = (x, XS - 1 - x)
        duo[...] = jnp.zeros((2, dh, B), f32)
        one = jnp.ones((1, W), f32)
        kept = [[one, one], [one, one]]
        waiting = None
        for p in range(XS + 1):
            if p < XS - 1:
                row = jnp.where(p < x, 0, 1)
                col = jnp.where(p < x, p, p - x)
                slot = jnp.where(p < x, kz, Z)
            else:
                row = p - XS + 1
                col, slot = ends[row], slots[row]
            for j in range(2):
                later, total = weigh(row, col, slot, j, p >= XS - 1)
                if waiting is not None:
                    gather(*waiting)
                waiting = (row, col, j, later, total, None)
                for k in range(2):
                    kept[k][j] = kept[k][j] * (jnp.where(row == k, total, 1.0) if p < XS - 1 else total if row == k else one)
        gather(*waiting)

        acc[...] = duo[0]

        @pl.when(c == 0)
        def _():
            send_out(kz, g, kz * XS + x, kept[0])

        @pl.when(c == 1)
        def _():
            send_out(kz, g, kz * XS + x, merge(kz, kept[0]))

        acc[...] = duo[1]
        send_out(LAST, Z - 3 - kz, (Z - 1 - kz) * XS + XS - 1 - x, kept[1])

    def full(turn, unused):
        low_row = jnp.logical_or(turn <= FIRST, turn > FIRST + 3)
        far = jnp.where(turn < FIRST, Z - 1 - turn, Z + 3 - turn)
        hop = (far + 1) // 2
        near = jnp.where(far % 2 == 1, z + hop, z + 2 * Z - hop) % Z
        shared = 2 * g + 1
        zq = jnp.where(turn == FIRST, shared, jnp.where(low_row, near, Z + FIRST - turn))
        row = jnp.where(low_row, 0, 1)
        low_valid = jnp.where(turn == FIRST, c == 0, zq > shared)
        valid = jnp.where(low_row, low_valid, zq + kz >= Z)

        @pl.when(turn == 1)
        def _():
            kv_wait(1, x_back)
            kv_spread(1)[2].start()

        @pl.when(turn == FIRST)
        def _():
            for step in (0, 1, Z - 1):
                close = (z + step) % Z

                @pl.when(close >= Z - 1 - 2 * g)
                def _():
                    q_get(close)

        @pl.when(turn == FIRST + 1)
        def _():
            kv_wait(1, x_on)
            kv_wait(1, x_far)

        @pl.when(turn == SELF_TURN)
        def _():
            self_units()

        @pl.when(valid)
        def _():
            @pl.when(jnp.logical_and(low_row, jnp.logical_or(turn <= FIRST, zq < Z - 1 - 2 * g)))
            def _():
                q_get(zq)

            kept = [None, None]
            waiting = None
            for col in range(XS):
                for j in range(2):
                    later, total = weigh(row, col, zq, j, False)
                    if waiting is not None:
                        gather(*waiting)
                    waiting = (row, col, j, later, total, col == 0)
                    kept[j] = total if col == 0 else kept[j] * total
            gather(*waiting)
            for j in range(2):
                factors[:, j * W : (j + 1) * W] = jnp.broadcast_to(kept[j], (8, W))

            handed = jnp.logical_and(low_row, c == 0)

            @pl.when(handed)
            def _():
                mbuf[zq, :dh] = acc[...]
                mbuf[zq, dh:] = factors[...]
                remote(mbuf.at[zq], mbuf.at[zq], m_send.at[zq], m_recv.at[zq], (s, partner)).start()

            @pl.when(jnp.logical_and(low_row, c == 1))
            def _():
                for j, both in enumerate(merge(zq, kept)):
                    factors[:, j * W : (j + 1) * W] = jnp.broadcast_to(both, (8, W))

            @pl.when(jnp.logical_not(handed))
            def _():
                u = jnp.where(low_row, zq, zq + 3)
                slot = jnp.where(low_row, g, Z - 3 - kz)
                send_out(u, slot, zq * XS + x, [factors[:1, j * W : (j + 1) * W] for j in range(2)])

        return unused

    go(w_copy(wrow(t), t, 0, partner))
    for e in range(1, Y):
        came = ((y + e) % Y) * 2 + c
        w_copy(wrow(t), came, 0, partner).wait_recv()
        go(w_copy(wrow(came), came, Y + e - 1, partner))
    kv_wait(0, x_on)
    kv_wait(0, x_far)
    lax.fori_loop(0, Z + 4, full, 0)
    w_copy(wrow(t), partner, 0, partner).wait_recv()
    for e in range(1, Y):
        w_copy(wrow(t), ((y + e) % Y) * 2 + 1 - c, 0, partner).wait_recv()

    for hh in range(T * H):
        heads[hh] = jnp.zeros((dh // 2, 128), f32)

    def made_here(slot):
        low_made = jnp.where(c == 1, z >= kz, z == kz)
        high_made = jnp.logical_and(slot == Z - 3 - kz, z + kz >= Z)
        return jnp.logical_or(jnp.logical_and(slot == g, low_made), high_made)

    def combine(r, unused):
        for hh in range(T * H):

            @pl.when(jnp.logical_not(jnp.logical_and(hh == head, made_here(r))))
            def _():
                e = r * T * H + hh
                for copy in o_copies(0, 0, 0, e, (s, t)):
                    copy.wait_recv()

        for hh in range(T * H):
            got = orecv[r * T * H + hh].astype(f32)
            fac = got[dh // 2 : dh // 2 + 1] + got[dh // 2 + 1 : dh // 2 + 2]
            heads[hh] = heads[hh] * fac + got[: dh // 2]
        return unused

    slots = jnp.where(z < 2, 1, jnp.where(z < 4, 2, z - 1))
    lax.fori_loop(0, slots, combine, 0)

    lhs, rhs = [], []
    for q in range(T * H // 4):
        both = jnp.concatenate([heads[4 * q + a] for a in range(4)], axis=0).T
        for e in range(2):
            lhs.append(both[e * dh : (e + 1) * dh].astype(bf16))
            for a in range(4):
                base = (4 * q + a) * dh + e * (dh // 2)
                rhs.append(wg[base : base + dh // 2])
    projected = jnp.dot(
        jnp.concatenate(lhs, axis=1), jnp.concatenate(rhs, axis=0), preferred_element_type=f32
    )
    out[...] = scaled_rows(projected, gain_out[...])

    for copy in started:
        copy.wait_send()
    each_q(lambda copy: copy.wait_send())

    for i in range(H):
        stays, copy = kv_first(i)

        @pl.when(jnp.logical_not(stays))
        def _():
            copy.wait_send()

    for row in range(2):
        for copy in kv_spread(row):
            copy.wait_send()

    def sent(u, valid, block):
        @pl.when(valid)
        def _():
            for e in range(1, T):
                for copy in o_copies(u, 0, e, 0, (s, t)):
                    copy.wait_send()

            @pl.when(block != s)
            def _():
                for copy in o_copies(u, 0, 0, 0, (s, t)):
                    copy.wait_send()

    def sent_low(zq, unused):
        sent(zq, jnp.logical_or(zq == kz, jnp.logical_and(zq > kz, c == 1)), zq * XS + x)

        @pl.when(jnp.logical_and(zq > kz, c == 0))
        def _():
            q_forward(zq).wait_send()
            remote(mbuf.at[zq], mbuf.at[zq], m_send.at[zq], m_recv.at[zq], (s, partner)).wait_send()

        return unused

    def sent_high(zq, unused):
        sent(zq + 3, zq + kz >= Z, zq * XS + x)
        return unused

    lax.fori_loop(0, Z, sent_low, 0)
    lax.fori_loop(5, Z, sent_high, 0)
    sent(LAST, z >= 0, (Z - 1 - kz) * XS + XS - 1 - x)


def solution(mesh):
    S, T = mesh.shape["sp"], mesh.shape["tp"]

    def local(act, gain_in, wq, wk, wv, off, wo, gain_out):
        R, D = act.shape
        H = off.shape[0]
        dh = wq.shape[1] // H
        B = R * T
        Z = S // XS
        vmem = pl.BlockSpec(memory_space=pltpu.VMEM)
        hbm = pl.BlockSpec(memory_space=pl.ANY)
        smem = pl.BlockSpec(memory_space=pltpu.SMEM)
        dma = pltpu.SemaphoreType.DMA
        return pl.pallas_call(
            functools.partial(layer_kernel, S, T, H, dh),
            out_shape=jax.ShapeDtypeStruct((R, D), bf16),
            in_specs=[hbm, hbm, hbm, hbm, hbm, smem, hbm, hbm],
            out_specs=vmem,
            scratch_shapes=[
                pltpu.VMEM((R, D), bf16),
                pltpu.VMEM((1, D), f32),
                pltpu.VMEM((1, D), f32),
                pltpu.VMEM((D, 3 * H * dh), bf16),
                pltpu.VMEM((B, 3 * H * dh), f32),
                pltpu.VMEM((B, D), bf16),
                pltpu.VMEM((wo.shape[0] * T, D), bf16),
                pltpu.VMEM((B, B), bf16),
                pltpu.VMEM((H, B, 128), bf16),
                pltpu.VMEM((H, dh, B), bf16),
                pltpu.VMEM((2, XS, B, 128), bf16),
                pltpu.VMEM((Z + 1, dh, B), bf16),
                pltpu.VMEM((16, B), bf16),
                pltpu.VMEM((2, B, B // 2), bf16),
                pltpu.VMEM((dh, B), f32),
                pltpu.VMEM((2, dh, B), f32),
                pltpu.VMEM((8, B), f32),
                pltpu.VMEM((Z, dh + 8, B), f32),
                pltpu.VMEM((2 * H, 1, 128), f32),
                pltpu.VMEM((LAST + 1, T, dh // 2 + 8, 128), bf16),
                pltpu.VMEM((6 * T * H, dh // 2 + 8, 128), bf16),
                pltpu.VMEM((T * H, dh // 2, 128), f32),
                dma((T,)),
                dma((T,)),
                dma((T,)),
                dma((T,)),
                dma((16,)),
                dma((4 * XS,)),
                dma((3 * H,)),
                dma((Z + 1,)),
                dma((Z + 1,)),
                dma((Z,)),
                dma((Z,)),
                dma((1,)),
                dma((1,)),
                dma(((LAST + 1) * T,)),
                dma((6 * T * H,)),
                dma((7,)),
            ],
            compiler_params=pltpu.CompilerParams(collective_id=0, has_side_effects=True, vmem_limit_bytes=67043328),
        )(act, gain_in.reshape(1, D), wq, wk, wv, off, wo, gain_out.reshape(1, D))

    in_specs = (
        P(("sp", "tp"), None),
        P(),
        P(None, "tp"),
        P(None, "tp"),
        P(None, "tp"),
        P("tp"),
        P("tp", None),
        P(),
    )
    out_specs = P(("sp", "tp"), None)
    return jax.shard_map(local, mesh=mesh, in_specs=in_specs, out_specs=out_specs, check_vma=False)
```

```python
import functools

import jax
import jax.numpy as jnp
from jax import lax
from jax.experimental import pallas as pl
from jax.experimental.pallas import tpu as pltpu
from jax.sharding import PartitionSpec as P

epsilon = 1e-06
log2e = 1.4426950408889634
MESH = pl.DeviceIdType.MESH
f32 = jnp.float32
bf16 = jnp.bfloat16
XS = 4
ZMAX = 63.0
LAST = 11
FIRST = 5
SELF_TURN = 9


def scaled_rows(widened, row_gain):
    spread = jnp.mean(widened * widened, axis=-1, keepdims=True)
    return (widened * lax.rsqrt(spread + epsilon) * row_gain).astype(bf16)


def layer_kernel(
    S,
    T,
    H,
    dh,
    act_hbm,
    gain_in_hbm,
    wq_hbm,
    wk_hbm,
    wv_hbm,
    off,
    wo_hbm,
    gain_out_hbm,
    out,
    act,
    gain_in,
    gain_out,
    weights,
    rows_q,
    xg,
    wg,
    perm,
    kvb,
    qb,
    kvr,
    qr,
    offt,
    ws,
    acc,
    duo,
    factors,
    mbuf,
    offs,
    obuf,
    orecv,
    heads,
    x_send,
    x_recv,
    w_send,
    w_recv,
    kv_send,
    kv_recv,
    q_send,
    q_recv,
    f_send,
    m_send,
    m_recv,
    off_send,
    off_recv,
    o_send,
    o_recv,
    load,
):
    R = act.shape[0]
    B = R * T
    W = B // 2
    rows = wo_hbm.shape[0]
    Z = S // XS
    s = lax.axis_index("sp")
    t = lax.axis_index("tp")
    z, x = s // XS, s % XS
    y, c = t // 2, t % 2
    partner = y * 2 + 1 - c
    place_z = (z + 2) % Z
    g, hl = place_z // 4, place_z % 4
    kz = 2 * g + c
    head = 2 * H * y + hl
    home = hl // H == c

    def spot(group, local):
        return (4 * group + local + Z - 2) % Z

    Y = T // 2

    def remote(src, dst, send, recv, dev):
        return pltpu.make_async_remote_copy(
            src_ref=src, dst_ref=dst, send_sem=send, recv_sem=recv, device_id=dev, device_id_type=MESH
        )

    started = []

    def go(copy):
        copy.start()
        started.append(copy)
        return copy

    def xrow(index):
        return xg.at[pl.ds(pl.multiple_of(index * R, R), R)]

    def wrow(index):
        return wg.at[pl.ds(pl.multiple_of(index * rows, rows), rows)]

    def x_part(index, slot, dev, part):
        half = xg.at[pl.ds(pl.multiple_of(index * R + part * (R // 2), R // 2), R // 2)]
        return remote(half, half, x_send.at[2 * slot + part], x_recv.at[2 * index + part], (s, dev))

    def x_sends(index, *targets):
        for part in range(2):
            for slot, dev in targets:
                go(x_part(index, slot, dev, part))

    def x_take(index, *targets):
        for part in range(2):
            x_part(index, 0, partner, part).wait_recv()
            for slot, dev in targets:
                go(x_part(index, slot, dev, part))

    def w_copy(src, index, slot, dev):
        return remote(src, wrow(index), w_send.at[slot], w_recv.at[index], (s, dev))

    early = [
        pltpu.make_async_copy(act_hbm, act, load.at[4]),
        pltpu.make_async_copy(gain_in_hbm, gain_in, load.at[5]),
    ]
    for copy in early:
        copy.start()
    loads = [
        pltpu.make_async_copy(wk_hbm, weights.at[:, : H * dh], load.at[0]),
        pltpu.make_async_copy(wv_hbm, weights.at[:, H * dh : 2 * H * dh], load.at[1]),
        pltpu.make_async_copy(wq_hbm, weights.at[:, 2 * H * dh :], load.at[2]),
        pltpu.make_async_copy(wo_hbm, wrow(t), load.at[3]),
        pltpu.make_async_copy(gain_out_hbm, gain_out, load.at[6]),
    ]
    for copy in loads:
        copy.start()
    barrier = pltpu.get_barrier_semaphore()
    partners = [(s, (t + d) % T) for d in range(1, T)]
    for d in range(Z):
        for core in range(2):
            if d:
                partners.append(((z + d) % Z * XS + x, 2 * y + core))
            partners.append(((z + d) % Z * XS + XS - 1 - x, 2 * y + core))
    partners += [(z * XS + (x + 2) % XS, t), (z * XS + (XS - 1 - x + 2) % XS, t)]
    for other in partners:
        pl.semaphore_signal(barrier, inc=1, device_id=other, device_id_type=MESH)
    for copy in early:
        copy.wait()
    xg[pl.ds(pl.multiple_of(t * R, R), R)] = scaled_rows(act[...].astype(f32), gain_in[...])
    pl.semaphore_wait(barrier, len(partners))
    onward = (y + 1 + (Y - 2) * c) % Y
    behind = (y + Y - 1 - (Y - 2) * c) % Y
    across = (y + 2) % Y
    x_sends(t, (1, onward * 2 + c), (2, behind * 2 + c), (0, partner))

    token = lax.broadcasted_iota(jnp.int32, (B, B), 0)
    place = lax.broadcasted_iota(jnp.int32, (B, B), 1)
    perm[...] = (token == (place & (T - 1)) * R + R - 1 - (place >> (T.bit_length() - 1))).astype(f32).astype(bf16)
    for i in range(H):
        offs[H * c + i] = jnp.broadcast_to(off[i] * log2e, (1, 128)).astype(f32)
    mine = offs.at[pl.ds(H * c, H)]
    go(remote(mine, mine, off_send.at[0], off_recv.at[0], (s, partner)))
    def project(chip):
        rows_of = pl.ds(pl.multiple_of(chip * 2 * R, 2 * R), 2 * R)
        rows_q[rows_of] = jnp.dot(xg[rows_of], weights[...], preferred_element_type=f32)

    for copy in loads:
        copy.wait()
    x_take(partner)
    project(y)
    x_take(behind * 2 + c, (3, onward * 2 + c), (4, partner))
    x_take(onward * 2 + c, (5, partner))
    for chip in (behind, onward):
        x_take(chip * 2 + 1 - c)
        project(chip)
    x_take(across * 2 + c, (6, partner))
    for e in range(1, Y):
        go(w_copy(wrow(t), t, e, ((y + e) % Y) * 2 + c))
    x_take(across * 2 + 1 - c)
    project(across)
    keys = rows_q[:, : H * dh].astype(bf16).astype(f32)
    values = rows_q[:, H * dh : 2 * H * dh].astype(bf16).astype(f32)
    turned = jnp.concatenate([keys.T, values.T], axis=0).astype(bf16)
    placed = jnp.dot(turned, perm[...], preferred_element_type=f32)
    keys_placed = placed[: H * dh].T
    for i in range(H):
        cols = slice(i * dh, (i + 1) * dh)
        kvb[i, :W] = jnp.concatenate([keys_placed[:W, cols], keys_placed[W:, cols]], axis=1).astype(bf16)
        for part in range(4):
            piece = placed[(H + i) * dh : (H + i + 1) * dh, part * 128 : (part + 1) * 128]
            kvb[i, W + part * dh : W + (part + 1) * dh] = piece.astype(bf16)

    outer = jnp.minimum(z, Z - 1 - z)

    class Both:
        def __init__(self, parts):
            self.parts = parts

        def start(self):
            for part in self.parts:
                part.start()

        def wait_send(self):
            for part in self.parts:
                part.wait_send()

    def kv_part(src, row, col, slot, dev, part):
        rows_of = pl.ds(part * W, W)
        return remote(
            src.at[rows_of],
            kvr.at[row, col, rows_of],
            kv_send.at[2 * slot + part],
            kv_recv.at[2 * (row * XS + col) + part],
            dev,
        )

    def kv_copy(src, row, col, slot, dev):
        return Both([kv_part(src, row, col, slot, dev, part) for part in range(2)])

    def kv_first(i):
        zd = spot(outer // 2, H * c + i)
        stays = jnp.logical_and(zd == z, outer % 2 == c)
        return stays, kv_copy(kvb.at[i], z // (Z // 2), x, i, (zd * XS + x, 2 * y + outer % 2))

    for i in range(H):
        stays, copy = kv_first(i)

        @pl.when(stays)
        def _():
            kvr[z // (Z // 2), x] = kvb[i]

        @pl.when(jnp.logical_not(stays))
        def _():
            copy.start()

    queries = rows_q[:, 2 * H * dh :] * (dh ** (-0.5) * log2e)
    q_turned = queries.T.astype(bf16)
    for i in range(H):
        qb[i] = q_turned[i * dh : (i + 1) * dh]

    def q_first(i, group):
        zd = spot(group, H * c + i)
        stays = jnp.logical_and(zd == z, c == 0)
        copy = remote(qb.at[i], qr.at[z], q_send.at[i * 2 + group], q_recv.at[z], (zd * XS + x, 2 * y))
        return stays, z >= 2 * group, copy

    def q_extra(i):
        depth = Z - 1 - z
        zd = spot(depth // 2, H * c + i)
        dev = (zd * XS + XS - 1 - x, 2 * y + depth % 2)
        return remote(qb.at[i], qr.at[Z], q_send.at[2 * H + i], q_recv.at[Z], dev)

    def each_q(act_on):
        for group in (0, 1):
            for i in range(H):
                stays, wanted, copy = q_first(i, group)

                @pl.when(jnp.logical_and(wanted, jnp.logical_not(stays)))
                def _():
                    act_on(copy)

        @pl.when(z >= Z // 2)
        def _():
            for i in range(H):
                act_on(q_extra(i))

    for i in range(H):
        for group in (0, 1):
            stays, wanted, _ = q_first(i, group)

            @pl.when(jnp.logical_and(wanted, stays))
            def _():
                qr[z] = qb[i]


    def kv_wait(row, col):
        for part in range(2):
            kv_part(kvb.at[0], row, col, 0, (s, t), part).wait_recv()

    def q_forward(slot):
        return remote(qr.at[slot], qr.at[slot], f_send.at[slot], q_recv.at[slot], (s, partner))

    def q_wait(slot):
        local = jnp.logical_and(jnp.logical_and(slot == z, c == 0), hl // H == 0)

        @pl.when(jnp.logical_not(local))
        def _():
            q_forward(slot).wait_recv()

    def q_get(slot):
        q_wait(slot)

        @pl.when(c == 0)
        def _():
            q_forward(slot).start()

    x_on = (x + 1 + (XS - 2) * c) % XS
    x_back = (x + XS - 1 - (XS - 2) * c) % XS
    x_far = (x + 2) % XS

    def kv_spread(row):
        base = H + row * 3
        return (
            kv_copy(kvr.at[row, x], row, x, base, (z * XS + x_on, t)),
            kv_copy(kvr.at[row, x], row, x, base + 1, (z * XS + x_back, t)),
            kv_copy(kvr.at[row, x_back], row, x_back, base + 2, (z * XS + x_on, t)),
        )

    def kv_relay(row):
        local = jnp.logical_and(z == (kz if row == 0 else Z - 1 - kz), home)
        for part in range(2):

            @pl.when(jnp.logical_not(local))
            def _():
                kv_part(kvb.at[0], row, x, 0, (s, t), part).wait_recv()

            for copy in kv_spread(row)[:2]:
                copy.parts[part].start()

    kv_relay(0)
    each_q(lambda copy: copy.start())
    for part in range(2):
        kv_part(kvb.at[0], 0, x_back, 0, (s, t), part).wait_recv()
        kv_spread(0)[2].parts[part].start()
    kv_relay(1)

    theirs = offs.at[pl.ds(H * (1 - c), H)]
    remote(theirs, theirs, off_send.at[0], off_recv.at[0], (s, partner)).wait_recv()
    whole = jnp.concatenate([jnp.broadcast_to(offs[hl], (16, 128))] * (B // 128), axis=1)
    high = whole.astype(bf16).astype(f32)
    middle = (whole - high).astype(bf16).astype(f32)
    low = whole - high - middle
    part_row = lax.broadcasted_iota(jnp.int32, (16, B), 0)
    offt[...] = jnp.where(
        part_row == 0, high, jnp.where(part_row == 1, middle, jnp.where(part_row == 2, low, 0.0))
    ).astype(bf16)

    lane = lax.broadcasted_iota(jnp.int32, (16, 128), 1)
    ones = (lane < 3).astype(f32).astype(bf16)
    zeros = jnp.zeros((dh, W), bf16)
    pad = jnp.zeros((112, W), bf16)

    def weigh(row, col, slot, j, masked):
        sl = slice(j * W, (j + 1) * W)
        run = jnp.ones((8, W), f32)
        if masked:
            ahead = (
                lax.broadcasted_iota(jnp.int32, (8, W), 1)
                + j * W
                - R * lax.broadcasted_iota(jnp.int32, (8, W), 0)
            )
        lhs = jnp.concatenate([kvr[row, col, :W], jnp.tile(ones, (W // 16, 1))], axis=1)
        for part in (0, 1):
            q = qr[slot, :, sl]
            stack = [q, zeros] if part == 0 else [zeros, q]
            rhs = jnp.concatenate(stack + [offt[:, sl], pad], axis=0)
            for v in range(0, W // 8, 2):
                if v % 8 == 0:
                    chunk = jnp.dot(lhs[8 * v : 8 * v + 64], rhs, preferred_element_type=f32)
                    score = [None] * v + [jnp.minimum(chunk[8 * w : 8 * w + 8], ZMAX) for w in range(8)]
                e0 = jnp.exp2(score[v])
                e1 = jnp.exp2(score[v + 1])
                if masked:
                    place_v = part * (W // 8) + v
                    e0 = jnp.where(ahead > R - 1 - place_v, e0, 0.0)
                    e1 = jnp.where(ahead > R - 2 - place_v, e1, 0.0)
                u0, u1 = 1.0 + e0, 1.0 + e1
                left = run * (1.0 / (u0 * u1))
                first = e0 * (u1 * left)
                second = e1 * left
                run = left
                base = part * W + 8 * v
                ws[j, base : base + 16] = jnp.concatenate([first, second], axis=0).astype(bf16)
        later = [None] * 8
        total = jnp.ones((1, W), f32)
        for i in range(7, -1, -1):
            later[i] = total
            total = total * run[i : i + 1]
        return jnp.concatenate(later + later, axis=0).astype(bf16), total

    def gather(row, col, j, later, total, first):
        sl = slice(j * W, (j + 1) * W)
        weight = (ws[j].reshape(B // 16, 16, W) * later[None]).reshape(B, W)
        vt = jnp.concatenate([kvr[row, col, W + p * dh : W + (p + 1) * dh] for p in range(4)], axis=1)
        part = jnp.dot(vt, weight, preferred_element_type=f32)
        if first is None:
            duo[row, :, sl] = duo[row, :, sl] * total + part
        else:
            acc[:, sl] = part if first else acc[:, sl] * total + part

    def o_copies(u, r, e, dst, dev):
        return (
            remote(obuf.at[u, r], orecv.at[dst], o_send.at[u * T + e], o_recv.at[dst], dev),
        )

    def send_out(u, slot, block, kept):
        lanes = lax.broadcasted_iota(jnp.int32, (dh // 2, 128), 1) < dh
        top = lax.broadcasted_iota(jnp.int32, (8, 128), 0) == 0
        lanes_t = lax.broadcasted_iota(jnp.int32, (8, 128), 1) < dh
        for g in range(T // 2):
            cols = slice(g * 128, (g + 1) * 128)
            a, b = acc[: dh // 2, cols], acc[dh // 2 :, cols]
            ar, br = pltpu.roll(a, dh, 1), pltpu.roll(b, dh, 1)
            j, inner = g * 128 // W, g * 128 % W
            tt = jnp.broadcast_to(kept[j][:, inner : inner + 128], (8, 128))
            tr = pltpu.roll(tt, dh, 1)
            for odd in range(2):
                body = jnp.where(lanes, ar, b) if odd else jnp.where(lanes, a, br)
                fac = jnp.where(lanes_t, tr, tt) if odd else jnp.where(lanes_t, tt, tr)
                fac_high = fac.astype(bf16).astype(f32)
                tail = jnp.where(top, fac_high, fac - fac_high)
                obuf[u, 2 * g + odd] = jnp.concatenate([body, tail], axis=0).astype(bf16)
        dst = slot * T * H + head
        for e in range(1, T):
            r = (t + e) % T
            for copy in o_copies(u, r, e, dst, (block, r)):
                copy.start()

        @pl.when(block != s)
        def _():
            for copy in o_copies(u, t, 0, dst, (block, t)):
                copy.start()

        @pl.when(block == s)
        def _():
            orecv[dst] = obuf[u, t]

    def merge(slot, kept):
        remote(mbuf.at[slot], mbuf.at[slot], m_send.at[slot], m_recv.at[slot], (s, t)).wait_recv()
        out_kept = []
        for j in range(2):
            sl = slice(j * W, (j + 1) * W)
            acc[:, sl] = mbuf[slot, :dh, sl] * kept[j] + acc[:, sl]
            out_kept.append(mbuf[slot, dh : dh + 1, sl] * kept[j])
        return out_kept

    def self_units():
        slots = (kz, Z)
        q_wait(slots[0])
        q_wait(slots[1])
        ends = (x, XS - 1 - x)
        duo[...] = jnp.zeros((2, dh, B), f32)
        one = jnp.ones((1, W), f32)
        kept = [[one, one], [one, one]]
        waiting = None
        for p in range(XS + 1):
            if p < XS - 1:
                row = jnp.where(p < x, 0, 1)
                col = jnp.where(p < x, p, p - x)
                slot = jnp.where(p < x, kz, Z)
            else:
                row = p - XS + 1
                col, slot = ends[row], slots[row]
            for j in range(2):
                later, total = weigh(row, col, slot, j, p >= XS - 1)
                if waiting is not None:
                    gather(*waiting)
                waiting = (row, col, j, later, total, None)
                for k in range(2):
                    kept[k][j] = kept[k][j] * (jnp.where(row == k, total, 1.0) if p < XS - 1 else total if row == k else one)
        gather(*waiting)

        acc[...] = duo[0]

        @pl.when(c == 0)
        def _():
            send_out(kz, g, kz * XS + x, kept[0])

        @pl.when(c == 1)
        def _():
            send_out(kz, g, kz * XS + x, merge(kz, kept[0]))

        acc[...] = duo[1]
        send_out(LAST, Z - 3 - kz, (Z - 1 - kz) * XS + XS - 1 - x, kept[1])

    def full(turn, unused):
        low_row = jnp.logical_or(turn <= FIRST, turn > FIRST + 3)
        far = jnp.where(turn < FIRST, Z - 1 - turn, Z + 3 - turn)
        hop = (far + 1) // 2
        near = jnp.where(far % 2 == 1, z + hop, z + 2 * Z - hop) % Z
        shared = 2 * g + 1
        zq = jnp.where(turn == FIRST, shared, jnp.where(low_row, near, Z + FIRST - turn))
        row = jnp.where(low_row, 0, 1)
        low_valid = jnp.where(turn == FIRST, c == 0, zq > shared)
        valid = jnp.where(low_row, low_valid, zq + kz >= Z)

        @pl.when(turn == 1)
        def _():
            kv_wait(1, x_back)
            kv_spread(1)[2].start()

        @pl.when(turn == FIRST)
        def _():
            for step in (0, 1, Z - 1):
                close = (z + step) % Z

                @pl.when(close >= Z - 1 - 2 * g)
                def _():
                    q_get(close)

        @pl.when(turn == FIRST + 1)
        def _():
            kv_wait(1, x_on)
            kv_wait(1, x_far)

        @pl.when(turn == SELF_TURN)
        def _():
            self_units()

        @pl.when(valid)
        def _():
            @pl.when(jnp.logical_and(low_row, jnp.logical_or(turn <= FIRST, zq < Z - 1 - 2 * g)))
            def _():
                q_get(zq)

            kept = [None, None]
            waiting = None
            for col in range(XS):
                for j in range(2):
                    later, total = weigh(row, col, zq, j, False)
                    if waiting is not None:
                        gather(*waiting)
                    waiting = (row, col, j, later, total, col == 0)
                    kept[j] = total if col == 0 else kept[j] * total
            gather(*waiting)
            for j in range(2):
                factors[:, j * W : (j + 1) * W] = jnp.broadcast_to(kept[j], (8, W))

            handed = jnp.logical_and(low_row, c == 0)

            @pl.when(handed)
            def _():
                mbuf[zq, :dh] = acc[...]
                mbuf[zq, dh:] = factors[...]
                remote(mbuf.at[zq], mbuf.at[zq], m_send.at[zq], m_recv.at[zq], (s, partner)).start()

            @pl.when(jnp.logical_and(low_row, c == 1))
            def _():
                for j, both in enumerate(merge(zq, kept)):
                    factors[:, j * W : (j + 1) * W] = jnp.broadcast_to(both, (8, W))

            @pl.when(jnp.logical_not(handed))
            def _():
                u = jnp.where(low_row, zq, zq + 3)
                slot = jnp.where(low_row, g, Z - 3 - kz)
                send_out(u, slot, zq * XS + x, [factors[:1, j * W : (j + 1) * W] for j in range(2)])

        return unused

    go(w_copy(wrow(t), t, 0, partner))
    for e in range(1, Y):
        came = ((y + e) % Y) * 2 + c
        w_copy(wrow(t), came, 0, partner).wait_recv()
        go(w_copy(wrow(came), came, Y + e - 1, partner))
    kv_wait(0, x_on)
    kv_wait(0, x_far)
    lax.fori_loop(0, Z + 4, full, 0)
    w_copy(wrow(t), partner, 0, partner).wait_recv()
    for e in range(1, Y):
        w_copy(wrow(t), ((y + e) % Y) * 2 + 1 - c, 0, partner).wait_recv()

    for hh in range(T * H):
        heads[hh] = jnp.zeros((dh // 2, 128), f32)

    def made_here(slot):
        low_made = jnp.where(c == 1, z >= kz, z == kz)
        high_made = jnp.logical_and(slot == Z - 3 - kz, z + kz >= Z)
        return jnp.logical_or(jnp.logical_and(slot == g, low_made), high_made)

    def combine(r, unused):
        for hh in range(T * H):

            @pl.when(jnp.logical_not(jnp.logical_and(hh == head, made_here(r))))
            def _():
                e = r * T * H + hh
                for copy in o_copies(0, 0, 0, e, (s, t)):
                    copy.wait_recv()

        for hh in range(T * H):
            got = orecv[r * T * H + hh].astype(f32)
            fac = got[dh // 2 : dh // 2 + 1] + got[dh // 2 + 1 : dh // 2 + 2]
            heads[hh] = heads[hh] * fac + got[: dh // 2]
        return unused

    slots = jnp.where(z < 2, 1, jnp.where(z < 4, 2, z - 1))
    lax.fori_loop(0, slots, combine, 0)

    lhs, rhs = [], []
    for q in range(T * H // 4):
        both = jnp.concatenate([heads[4 * q + a] for a in range(4)], axis=0).T
        for e in range(2):
            lhs.append(both[e * dh : (e + 1) * dh].astype(bf16))
            for a in range(4):
                base = (4 * q + a) * dh + e * (dh // 2)
                rhs.append(wg[base : base + dh // 2])
    projected = jnp.dot(
        jnp.concatenate(lhs, axis=1), jnp.concatenate(rhs, axis=0), preferred_element_type=f32
    )
    out[...] = scaled_rows(projected, gain_out[...])

    for copy in started:
        copy.wait_send()
    each_q(lambda copy: copy.wait_send())

    for i in range(H):
        stays, copy = kv_first(i)

        @pl.when(jnp.logical_not(stays))
        def _():
            copy.wait_send()

    for row in range(2):
        for copy in kv_spread(row):
            copy.wait_send()

    def sent(u, valid, block):
        @pl.when(valid)
        def _():
            for e in range(1, T):
                for copy in o_copies(u, 0, e, 0, (s, t)):
                    copy.wait_send()

            @pl.when(block != s)
            def _():
                for copy in o_copies(u, 0, 0, 0, (s, t)):
                    copy.wait_send()

    def sent_low(zq, unused):
        sent(zq, jnp.logical_or(zq == kz, jnp.logical_and(zq > kz, c == 1)), zq * XS + x)

        @pl.when(jnp.logical_and(zq > kz, c == 0))
        def _():
            q_forward(zq).wait_send()
            remote(mbuf.at[zq], mbuf.at[zq], m_send.at[zq], m_recv.at[zq], (s, partner)).wait_send()

        return unused

    def sent_high(zq, unused):
        sent(zq + 3, zq + kz >= Z, zq * XS + x)
        return unused

    lax.fori_loop(0, Z, sent_low, 0)
    lax.fori_loop(5, Z, sent_high, 0)
    sent(LAST, z >= 0, (Z - 1 - kz) * XS + XS - 1 - x)


def solution(mesh):
    S, T = mesh.shape["sp"], mesh.shape["tp"]

    def local(act, gain_in, wq, wk, wv, off, wo, gain_out):
        R, D = act.shape
        H = off.shape[0]
        dh = wq.shape[1] // H
        B = R * T
        Z = S // XS
        vmem = pl.BlockSpec(memory_space=pltpu.VMEM)
        hbm = pl.BlockSpec(memory_space=pl.ANY)
        smem = pl.BlockSpec(memory_space=pltpu.SMEM)
        dma = pltpu.SemaphoreType.DMA
        return pl.pallas_call(
            functools.partial(layer_kernel, S, T, H, dh),
            out_shape=jax.ShapeDtypeStruct((R, D), bf16),
            in_specs=[hbm, hbm, hbm, hbm, hbm, smem, hbm, hbm],
            out_specs=vmem,
            scratch_shapes=[
                pltpu.VMEM((R, D), bf16),
                pltpu.VMEM((1, D), f32),
                pltpu.VMEM((1, D), f32),
                pltpu.VMEM((D, 3 * H * dh), bf16),
                pltpu.VMEM((B, 3 * H * dh), f32),
                pltpu.VMEM((B, D), bf16),
                pltpu.VMEM((wo.shape[0] * T, D), bf16),
                pltpu.VMEM((B, B), bf16),
                pltpu.VMEM((H, B, 128), bf16),
                pltpu.VMEM((H, dh, B), bf16),
                pltpu.VMEM((2, XS, B, 128), bf16),
                pltpu.VMEM((Z + 1, dh, B), bf16),
                pltpu.VMEM((16, B), bf16),
                pltpu.VMEM((2, B, B // 2), bf16),
                pltpu.VMEM((dh, B), f32),
                pltpu.VMEM((2, dh, B), f32),
                pltpu.VMEM((8, B), f32),
                pltpu.VMEM((Z, dh + 8, B), f32),
                pltpu.VMEM((2 * H, 1, 128), f32),
                pltpu.VMEM((LAST + 1, T, dh // 2 + 8, 128), bf16),
                pltpu.VMEM((6 * T * H, dh // 2 + 8, 128), bf16),
                pltpu.VMEM((T * H, dh // 2, 128), f32),
                dma((2 * T,)),
                dma((2 * T,)),
                dma((T,)),
                dma((T,)),
                dma((16,)),
                dma((4 * XS,)),
                dma((3 * H,)),
                dma((Z + 1,)),
                dma((Z + 1,)),
                dma((Z,)),
                dma((Z,)),
                dma((1,)),
                dma((1,)),
                dma(((LAST + 1) * T,)),
                dma((6 * T * H,)),
                dma((7,)),
            ],
            compiler_params=pltpu.CompilerParams(collective_id=0, has_side_effects=True, vmem_limit_bytes=67043328),
        )(act, gain_in.reshape(1, D), wq, wk, wv, off, wo, gain_out.reshape(1, D))

    in_specs = (
        P(("sp", "tp"), None),
        P(),
        P(None, "tp"),
        P(None, "tp"),
        P(None, "tp"),
        P("tp"),
        P("tp", None),
        P(),
    )
    out_specs = P(("sp", "tp"), None)
    return jax.shard_map(local, mesh=mesh, in_specs=in_specs, out_specs=out_specs, check_vma=False)
```

```python
import functools

import jax
import jax.numpy as jnp
from jax import lax
from jax.experimental import pallas as pl
from jax.experimental.pallas import tpu as pltpu
from jax.sharding import PartitionSpec as P

epsilon = 1e-06
log2e = 1.4426950408889634
MESH = pl.DeviceIdType.MESH
f32 = jnp.float32
bf16 = jnp.bfloat16
XS = 4
ZMAX = 63.0
LAST = 11
FIRST = 5
SELF_TURN = 7


def scaled_rows(widened, row_gain):
    spread = jnp.mean(widened * widened, axis=-1, keepdims=True)
    return (widened * lax.rsqrt(spread + epsilon) * row_gain).astype(bf16)


def layer_kernel(
    S,
    T,
    H,
    dh,
    act_hbm,
    gain_in_hbm,
    wq_hbm,
    wk_hbm,
    wv_hbm,
    off,
    wo_hbm,
    gain_out_hbm,
    out,
    act,
    gain_in,
    gain_out,
    weights,
    rows_q,
    xg,
    wg,
    perm,
    kvb,
    qb,
    kvr,
    qr,
    offt,
    ws,
    acc,
    duo,
    factors,
    mbuf,
    offs,
    obuf,
    orecv,
    heads,
    x_send,
    x_recv,
    w_send,
    w_recv,
    kv_send,
    kv_recv,
    q_send,
    q_recv,
    f_send,
    m_send,
    m_recv,
    off_send,
    off_recv,
    o_send,
    o_recv,
    load,
):
    R = act.shape[0]
    B = R * T
    W = B // 2
    rows = wo_hbm.shape[0]
    Z = S // XS
    s = lax.axis_index("sp")
    t = lax.axis_index("tp")
    z, x = s // XS, s % XS
    y, c = t // 2, t % 2
    partner = y * 2 + 1 - c
    place_z = (z + 2) % Z
    g, hl = place_z // 4, place_z % 4
    kz = 2 * g + c
    head = 2 * H * y + hl
    home = hl // H == c

    def spot(group, local):
        return (4 * group + local + Z - 2) % Z

    Y = T // 2

    def remote(src, dst, send, recv, dev):
        return pltpu.make_async_remote_copy(
            src_ref=src, dst_ref=dst, send_sem=send, recv_sem=recv, device_id=dev, device_id_type=MESH
        )

    started = []

    def go(copy):
        copy.start()
        started.append(copy)
        return copy

    def xrow(index):
        return xg.at[pl.ds(pl.multiple_of(index * R, R), R)]

    def wrow(index):
        return wg.at[pl.ds(pl.multiple_of(index * rows, rows), rows)]

    def x_part(index, slot, dev, part):
        half = xg.at[pl.ds(pl.multiple_of(index * R + part * (R // 2), R // 2), R // 2)]
        return remote(half, half, x_send.at[2 * slot + part], x_recv.at[2 * index + part], (s, dev))

    def x_sends(index, *targets):
        for part in range(2):
            for slot, dev in targets:
                go(x_part(index, slot, dev, part))

    def x_take(index, *targets):
        for part in range(2):
            x_part(index, 0, partner, part).wait_recv()
            for slot, dev in targets:
                go(x_part(index, slot, dev, part))

    def w_copy(src, index, slot, dev):
        return remote(src, wrow(index), w_send.at[slot], w_recv.at[index], (s, dev))

    early = [
        pltpu.make_async_copy(act_hbm, act, load.at[4]),
        pltpu.make_async_copy(gain_in_hbm, gain_in, load.at[5]),
    ]
    for copy in early:
        copy.start()
    loads = [
        pltpu.make_async_copy(wk_hbm, weights.at[:, : H * dh], load.at[0]),
        pltpu.make_async_copy(wv_hbm, weights.at[:, H * dh : 2 * H * dh], load.at[1]),
        pltpu.make_async_copy(wq_hbm, weights.at[:, 2 * H * dh :], load.at[2]),
        pltpu.make_async_copy(wo_hbm, wrow(t), load.at[3]),
        pltpu.make_async_copy(gain_out_hbm, gain_out, load.at[6]),
    ]
    for copy in loads:
        copy.start()
    barrier = pltpu.get_barrier_semaphore()
    partners = [(s, (t + d) % T) for d in range(1, T)]
    for d in range(Z):
        for core in range(2):
            if d:
                partners.append(((z + d) % Z * XS + x, 2 * y + core))
            partners.append(((z + d) % Z * XS + XS - 1 - x, 2 * y + core))
    partners += [(z * XS + (x + 2) % XS, t), (z * XS + (XS - 1 - x + 2) % XS, t)]
    for other in partners:
        pl.semaphore_signal(barrier, inc=1, device_id=other, device_id_type=MESH)
    for copy in early:
        copy.wait()
    xg[pl.ds(pl.multiple_of(t * R, R), R)] = scaled_rows(act[...].astype(f32), gain_in[...])
    pl.semaphore_wait(barrier, len(partners))
    onward = (y + 1 + (Y - 2) * c) % Y
    behind = (y + Y - 1 - (Y - 2) * c) % Y
    across = (y + 2) % Y
    x_sends(t, (1, onward * 2 + c), (2, behind * 2 + c), (0, partner))

    token = lax.broadcasted_iota(jnp.int32, (B, B), 0)
    place = lax.broadcasted_iota(jnp.int32, (B, B), 1)
    perm[...] = (token == (place & (T - 1)) * R + R - 1 - (place >> (T.bit_length() - 1))).astype(f32).astype(bf16)
    for i in range(H):
        offs[H * c + i] = jnp.broadcast_to(off[i] * log2e, (1, 128)).astype(f32)
    mine = offs.at[pl.ds(H * c, H)]
    go(remote(mine, mine, off_send.at[0], off_recv.at[0], (s, partner)))
    def project(chip):
        rows_of = pl.ds(pl.multiple_of(chip * 2 * R, 2 * R), 2 * R)
        rows_q[rows_of] = jnp.dot(xg[rows_of], weights[...], preferred_element_type=f32)

    for copy in loads:
        copy.wait()
    x_take(partner)
    project(y)
    x_take(behind * 2 + c, (3, onward * 2 + c), (4, partner))
    x_take(onward * 2 + c, (5, partner))
    for chip in (behind, onward):
        x_take(chip * 2 + 1 - c)
        project(chip)
    x_take(across * 2 + c, (6, partner))
    for e in range(1, Y):
        go(w_copy(wrow(t), t, e, ((y + e) % Y) * 2 + c))
    x_take(across * 2 + 1 - c)
    project(across)
    keys = rows_q[:, : H * dh].astype(bf16).astype(f32)
    values = rows_q[:, H * dh : 2 * H * dh].astype(bf16).astype(f32)
    turned = jnp.concatenate([keys.T, values.T], axis=0).astype(bf16)
    placed = jnp.dot(turned, perm[...], preferred_element_type=f32)
    keys_placed = placed[: H * dh].T
    for i in range(H):
        cols = slice(i * dh, (i + 1) * dh)
        kvb[i, :W] = jnp.concatenate([keys_placed[:W, cols], keys_placed[W:, cols]], axis=1).astype(bf16)
        for part in range(4):
            piece = placed[(H + i) * dh : (H + i + 1) * dh, part * 128 : (part + 1) * 128]
            kvb[i, W + part * dh : W + (part + 1) * dh] = piece.astype(bf16)

    outer = jnp.minimum(z, Z - 1 - z)

    class Both:
        def __init__(self, parts):
            self.parts = parts

        def start(self):
            for part in self.parts:
                part.start()

        def wait_send(self):
            for part in self.parts:
                part.wait_send()

    def kv_part(src, row, col, slot, dev, part):
        rows_of = pl.ds(part * W, W)
        return remote(
            src.at[rows_of],
            kvr.at[row, col, rows_of],
            kv_send.at[2 * slot + part],
            kv_recv.at[2 * (row * XS + col) + part],
            dev,
        )

    def kv_copy(src, row, col, slot, dev):
        return Both([kv_part(src, row, col, slot, dev, part) for part in range(2)])

    def kv_first(i):
        zd = spot(outer // 2, H * c + i)
        stays = jnp.logical_and(zd == z, outer % 2 == c)
        return stays, kv_copy(kvb.at[i], z // (Z // 2), x, i, (zd * XS + x, 2 * y + outer % 2))

    for i in range(H):
        stays, copy = kv_first(i)

        @pl.when(stays)
        def _():
            kvr[z // (Z // 2), x] = kvb[i]

        @pl.when(jnp.logical_not(stays))
        def _():
            copy.start()

    queries = rows_q[:, 2 * H * dh :] * (dh ** (-0.5) * log2e)
    q_turned = queries.T.astype(bf16)
    for i in range(H):
        qb[i] = q_turned[i * dh : (i + 1) * dh]

    def q_first(i, group):
        zd = spot(group, H * c + i)
        stays = jnp.logical_and(zd == z, c == 0)
        copy = remote(qb.at[i], qr.at[z], q_send.at[i * 2 + group], q_recv.at[z], (zd * XS + x, 2 * y))
        return stays, z >= 2 * group, copy

    def q_extra(i):
        depth = Z - 1 - z
        zd = spot(depth // 2, H * c + i)
        dev = (zd * XS + XS - 1 - x, 2 * y + depth % 2)
        return remote(qb.at[i], qr.at[Z], q_send.at[2 * H + i], q_recv.at[Z], dev)

    def each_q(act_on):
        for group in (0, 1):
            for i in range(H):
                stays, wanted, copy = q_first(i, group)

                @pl.when(jnp.logical_and(wanted, jnp.logical_not(stays)))
                def _():
                    act_on(copy)

        @pl.when(z >= Z // 2)
        def _():
            for i in range(H):
                act_on(q_extra(i))

    for i in range(H):
        for group in (0, 1):
            stays, wanted, _ = q_first(i, group)

            @pl.when(jnp.logical_and(wanted, stays))
            def _():
                qr[z] = qb[i]


    def kv_wait(row, col):
        for part in range(2):
            kv_part(kvb.at[0], row, col, 0, (s, t), part).wait_recv()

    def q_forward(slot):
        return remote(qr.at[slot], qr.at[slot], f_send.at[slot], q_recv.at[slot], (s, partner))

    def q_wait(slot):
        local = jnp.logical_and(jnp.logical_and(slot == z, c == 0), hl // H == 0)

        @pl.when(jnp.logical_not(local))
        def _():
            q_forward(slot).wait_recv()

    def q_get(slot):
        q_wait(slot)

        @pl.when(c == 0)
        def _():
            q_forward(slot).start()

    x_on = (x + 1 + (XS - 2) * c) % XS
    x_back = (x + XS - 1 - (XS - 2) * c) % XS
    x_far = (x + 2) % XS

    def kv_spread(row):
        base = H + row * 3
        return (
            kv_copy(kvr.at[row, x], row, x, base, (z * XS + x_on, t)),
            kv_copy(kvr.at[row, x], row, x, base + 1, (z * XS + x_back, t)),
            kv_copy(kvr.at[row, x_back], row, x_back, base + 2, (z * XS + x_on, t)),
        )

    def kv_relay(row):
        local = jnp.logical_and(z == (kz if row == 0 else Z - 1 - kz), home)
        for part in range(2):

            @pl.when(jnp.logical_not(local))
            def _():
                kv_part(kvb.at[0], row, x, 0, (s, t), part).wait_recv()

            for copy in kv_spread(row)[:2]:
                copy.parts[part].start()

    kv_relay(0)
    each_q(lambda copy: copy.start())
    for part in range(2):
        kv_part(kvb.at[0], 0, x_back, 0, (s, t), part).wait_recv()
        kv_spread(0)[2].parts[part].start()
    kv_relay(1)

    theirs = offs.at[pl.ds(H * (1 - c), H)]
    remote(theirs, theirs, off_send.at[0], off_recv.at[0], (s, partner)).wait_recv()
    whole = jnp.concatenate([jnp.broadcast_to(offs[hl], (16, 128))] * (B // 128), axis=1)
    high = whole.astype(bf16).astype(f32)
    middle = (whole - high).astype(bf16).astype(f32)
    low = whole - high - middle
    part_row = lax.broadcasted_iota(jnp.int32, (16, B), 0)
    offt[...] = jnp.where(
        part_row == 0, high, jnp.where(part_row == 1, middle, jnp.where(part_row == 2, low, 0.0))
    ).astype(bf16)

    lane = lax.broadcasted_iota(jnp.int32, (16, 128), 1)
    ones = (lane < 3).astype(f32).astype(bf16)
    zeros = jnp.zeros((dh, W), bf16)
    pad = jnp.zeros((112, W), bf16)

    def weigh(row, col, slot, j, masked):
        sl = slice(j * W, (j + 1) * W)
        run = jnp.ones((8, W), f32)
        if masked:
            ahead = (
                lax.broadcasted_iota(jnp.int32, (8, W), 1)
                + j * W
                - R * lax.broadcasted_iota(jnp.int32, (8, W), 0)
            )
        lhs = jnp.concatenate([kvr[row, col, :W], jnp.tile(ones, (W // 16, 1))], axis=1)
        for part in (0, 1):
            q = qr[slot, :, sl]
            stack = [q, zeros] if part == 0 else [zeros, q]
            rhs = jnp.concatenate(stack + [offt[:, sl], pad], axis=0)
            for v in range(0, W // 8, 2):
                if v % 8 == 0:
                    chunk = jnp.dot(lhs[8 * v : 8 * v + 64], rhs, preferred_element_type=f32)
                    score = [None] * v + [jnp.minimum(chunk[8 * w : 8 * w + 8], ZMAX) for w in range(8)]
                e0 = jnp.exp2(score[v])
                e1 = jnp.exp2(score[v + 1])
                if masked:
                    place_v = part * (W // 8) + v
                    e0 = jnp.where(ahead > R - 1 - place_v, e0, 0.0)
                    e1 = jnp.where(ahead > R - 2 - place_v, e1, 0.0)
                u0, u1 = 1.0 + e0, 1.0 + e1
                left = run * (1.0 / (u0 * u1))
                first = e0 * (u1 * left)
                second = e1 * left
                run = left
                base = part * W + 8 * v
                ws[j, base : base + 16] = jnp.concatenate([first, second], axis=0).astype(bf16)
        later = [None] * 8
        total = jnp.ones((1, W), f32)
        for i in range(7, -1, -1):
            later[i] = total
            total = total * run[i : i + 1]
        return jnp.concatenate(later + later, axis=0).astype(bf16), total

    def gather(row, col, j, later, total, first):
        sl = slice(j * W, (j + 1) * W)
        weight = (ws[j].reshape(B // 16, 16, W) * later[None]).reshape(B, W)
        vt = jnp.concatenate([kvr[row, col, W + p * dh : W + (p + 1) * dh] for p in range(4)], axis=1)
        part = jnp.dot(vt, weight, preferred_element_type=f32)
        if first is None:
            duo[row, :, sl] = duo[row, :, sl] * total + part
        else:
            acc[:, sl] = part if first else acc[:, sl] * total + part

    def o_copies(u, r, e, dst, dev):
        return (
            remote(obuf.at[u, r], orecv.at[dst], o_send.at[u * T + e], o_recv.at[dst], dev),
        )

    def send_out(u, slot, block, kept):
        lanes = lax.broadcasted_iota(jnp.int32, (dh // 2, 128), 1) < dh
        top = lax.broadcasted_iota(jnp.int32, (8, 128), 0) == 0
        lanes_t = lax.broadcasted_iota(jnp.int32, (8, 128), 1) < dh
        for g in range(T // 2):
            cols = slice(g * 128, (g + 1) * 128)
            a, b = acc[: dh // 2, cols], acc[dh // 2 :, cols]
            ar, br = pltpu.roll(a, dh, 1), pltpu.roll(b, dh, 1)
            j, inner = g * 128 // W, g * 128 % W
            tt = jnp.broadcast_to(kept[j][:, inner : inner + 128], (8, 128))
            tr = pltpu.roll(tt, dh, 1)
            for odd in range(2):
                body = jnp.where(lanes, ar, b) if odd else jnp.where(lanes, a, br)
                fac = jnp.where(lanes_t, tr, tt) if odd else jnp.where(lanes_t, tt, tr)
                fac_high = fac.astype(bf16).astype(f32)
                tail = jnp.where(top, fac_high, fac - fac_high)
                obuf[u, 2 * g + odd] = jnp.concatenate([body, tail], axis=0).astype(bf16)
        dst = slot * T * H + head
        for e in range(1, T):
            r = (t + e) % T
            for copy in o_copies(u, r, e, dst, (block, r)):
                copy.start()

        @pl.when(block != s)
        def _():
            for copy in o_copies(u, t, 0, dst, (block, t)):
                copy.start()

        @pl.when(block == s)
        def _():
            orecv[dst] = obuf[u, t]

    def merge(slot, kept):
        remote(mbuf.at[slot], mbuf.at[slot], m_send.at[slot], m_recv.at[slot], (s, t)).wait_recv()
        out_kept = []
        for j in range(2):
            sl = slice(j * W, (j + 1) * W)
            acc[:, sl] = mbuf[slot, :dh, sl] * kept[j] + acc[:, sl]
            out_kept.append(mbuf[slot, dh : dh + 1, sl] * kept[j])
        return out_kept

    def self_units():
        slots = (kz, Z)
        q_wait(slots[0])
        q_wait(slots[1])
        ends = (x, XS - 1 - x)
        duo[...] = jnp.zeros((2, dh, B), f32)
        one = jnp.ones((1, W), f32)
        kept = [[one, one], [one, one]]
        waiting = None
        for p in range(XS + 1):
            if p < XS - 1:
                row = jnp.where(p < x, 0, 1)
                col = jnp.where(p < x, p, p - x)
                slot = jnp.where(p < x, kz, Z)
            else:
                row = p - XS + 1
                col, slot = ends[row], slots[row]
            for j in range(2):
                later, total = weigh(row, col, slot, j, p >= XS - 1)
                if waiting is not None:
                    gather(*waiting)
                waiting = (row, col, j, later, total, None)
                for k in range(2):
                    kept[k][j] = kept[k][j] * (jnp.where(row == k, total, 1.0) if p < XS - 1 else total if row == k else one)
        gather(*waiting)

        acc[...] = duo[0]

        @pl.when(c == 0)
        def _():
            send_out(kz, g, kz * XS + x, kept[0])

        @pl.when(c == 1)
        def _():
            send_out(kz, g, kz * XS + x, merge(kz, kept[0]))

        acc[...] = duo[1]
        send_out(LAST, Z - 3 - kz, (Z - 1 - kz) * XS + XS - 1 - x, kept[1])

    def full(turn, unused):
        low_row = jnp.logical_or(turn <= FIRST, turn > FIRST + 3)
        far = jnp.where(turn < FIRST, Z - 1 - turn, Z + 3 - turn)
        hop = (far + 1) // 2
        near = jnp.where(far % 2 == 1, z + hop, z + 2 * Z - hop) % Z
        shared = 2 * g + 1
        zq = jnp.where(turn == FIRST, shared, jnp.where(low_row, near, Z + FIRST - turn))
        row = jnp.where(low_row, 0, 1)
        low_valid = jnp.where(turn == FIRST, c == 0, zq > shared)
        valid = jnp.where(low_row, low_valid, zq + kz >= Z)

        @pl.when(turn == 1)
        def _():
            kv_wait(1, x_back)
            kv_spread(1)[2].start()

        @pl.when(turn == FIRST)
        def _():
            for step in (0, 1, Z - 1):
                close = (z + step) % Z

                @pl.when(close >= Z - 1 - 2 * g)
                def _():
                    q_get(close)

        @pl.when(turn == FIRST + 1)
        def _():
            kv_wait(1, x_on)
            kv_wait(1, x_far)

        @pl.when(turn == SELF_TURN)
        def _():
            self_units()

        @pl.when(valid)
        def _():
            @pl.when(jnp.logical_and(low_row, jnp.logical_or(turn <= FIRST, zq < Z - 1 - 2 * g)))
            def _():
                q_get(zq)

            kept = [None, None]
            waiting = None
            for col in range(XS):
                for j in range(2):
                    later, total = weigh(row, col, zq, j, False)
                    if waiting is not None:
                        gather(*waiting)
                    waiting = (row, col, j, later, total, col == 0)
                    kept[j] = total if col == 0 else kept[j] * total
            gather(*waiting)
            for j in range(2):
                factors[:, j * W : (j + 1) * W] = jnp.broadcast_to(kept[j], (8, W))

            handed = jnp.logical_and(low_row, c == 0)

            @pl.when(handed)
            def _():
                mbuf[zq, :dh] = acc[...]
                mbuf[zq, dh:] = factors[...]
                remote(mbuf.at[zq], mbuf.at[zq], m_send.at[zq], m_recv.at[zq], (s, partner)).start()

            @pl.when(jnp.logical_and(low_row, c == 1))
            def _():
                for j, both in enumerate(merge(zq, kept)):
                    factors[:, j * W : (j + 1) * W] = jnp.broadcast_to(both, (8, W))

            @pl.when(jnp.logical_not(handed))
            def _():
                u = jnp.where(low_row, zq, zq + 3)
                slot = jnp.where(low_row, g, Z - 3 - kz)
                send_out(u, slot, zq * XS + x, [factors[:1, j * W : (j + 1) * W] for j in range(2)])

        return unused

    go(w_copy(wrow(t), t, 0, partner))
    for e in range(1, Y):
        came = ((y + e) % Y) * 2 + c
        w_copy(wrow(t), came, 0, partner).wait_recv()
        go(w_copy(wrow(came), came, Y + e - 1, partner))
    kv_wait(0, x_on)
    kv_wait(0, x_far)
    lax.fori_loop(0, Z + 4, full, 0)
    w_copy(wrow(t), partner, 0, partner).wait_recv()
    for e in range(1, Y):
        w_copy(wrow(t), ((y + e) % Y) * 2 + 1 - c, 0, partner).wait_recv()

    for hh in range(T * H):
        heads[hh] = jnp.zeros((dh // 2, 128), f32)

    def made_here(slot):
        low_made = jnp.where(c == 1, z >= kz, z == kz)
        high_made = jnp.logical_and(slot == Z - 3 - kz, z + kz >= Z)
        return jnp.logical_or(jnp.logical_and(slot == g, low_made), high_made)

    def combine(r, unused):
        for hh in range(T * H):

            @pl.when(jnp.logical_not(jnp.logical_and(hh == head, made_here(r))))
            def _():
                e = r * T * H + hh
                for copy in o_copies(0, 0, 0, e, (s, t)):
                    copy.wait_recv()

        for hh in range(T * H):
            got = orecv[r * T * H + hh].astype(f32)
            fac = got[dh // 2 : dh // 2 + 1] + got[dh // 2 + 1 : dh // 2 + 2]
            heads[hh] = heads[hh] * fac + got[: dh // 2]
        return unused

    slots = jnp.where(z < 2, 1, jnp.where(z < 4, 2, z - 1))
    lax.fori_loop(0, slots, combine, 0)

    lhs, rhs = [], []
    for q in range(T * H // 4):
        both = jnp.concatenate([heads[4 * q + a] for a in range(4)], axis=0).T
        for e in range(2):
            lhs.append(both[e * dh : (e + 1) * dh].astype(bf16))
            for a in range(4):
                base = (4 * q + a) * dh + e * (dh // 2)
                rhs.append(wg[base : base + dh // 2])
    projected = jnp.dot(
        jnp.concatenate(lhs, axis=1), jnp.concatenate(rhs, axis=0), preferred_element_type=f32
    )
    out[...] = scaled_rows(projected, gain_out[...])

    for copy in started:
        copy.wait_send()
    each_q(lambda copy: copy.wait_send())

    for i in range(H):
        stays, copy = kv_first(i)

        @pl.when(jnp.logical_not(stays))
        def _():
            copy.wait_send()

    for row in range(2):
        for copy in kv_spread(row):
            copy.wait_send()

    def sent(u, valid, block):
        @pl.when(valid)
        def _():
            for e in range(1, T):
                for copy in o_copies(u, 0, e, 0, (s, t)):
                    copy.wait_send()

            @pl.when(block != s)
            def _():
                for copy in o_copies(u, 0, 0, 0, (s, t)):
                    copy.wait_send()

    def sent_low(zq, unused):
        sent(zq, jnp.logical_or(zq == kz, jnp.logical_and(zq > kz, c == 1)), zq * XS + x)

        @pl.when(jnp.logical_and(zq > kz, c == 0))
        def _():
            q_forward(zq).wait_send()
            remote(mbuf.at[zq], mbuf.at[zq], m_send.at[zq], m_recv.at[zq], (s, partner)).wait_send()

        return unused

    def sent_high(zq, unused):
        sent(zq + 3, zq + kz >= Z, zq * XS + x)
        return unused

    lax.fori_loop(0, Z, sent_low, 0)
    lax.fori_loop(5, Z, sent_high, 0)
    sent(LAST, z >= 0, (Z - 1 - kz) * XS + XS - 1 - x)


def solution(mesh):
    S, T = mesh.shape["sp"], mesh.shape["tp"]

    def local(act, gain_in, wq, wk, wv, off, wo, gain_out):
        R, D = act.shape
        H = off.shape[0]
        dh = wq.shape[1] // H
        B = R * T
        Z = S // XS
        vmem = pl.BlockSpec(memory_space=pltpu.VMEM)
        hbm = pl.BlockSpec(memory_space=pl.ANY)
        smem = pl.BlockSpec(memory_space=pltpu.SMEM)
        dma = pltpu.SemaphoreType.DMA
        return pl.pallas_call(
            functools.partial(layer_kernel, S, T, H, dh),
            out_shape=jax.ShapeDtypeStruct((R, D), bf16),
            in_specs=[hbm, hbm, hbm, hbm, hbm, smem, hbm, hbm],
            out_specs=vmem,
            scratch_shapes=[
                pltpu.VMEM((R, D), bf16),
                pltpu.VMEM((1, D), f32),
                pltpu.VMEM((1, D), f32),
                pltpu.VMEM((D, 3 * H * dh), bf16),
                pltpu.VMEM((B, 3 * H * dh), f32),
                pltpu.VMEM((B, D), bf16),
                pltpu.VMEM((wo.shape[0] * T, D), bf16),
                pltpu.VMEM((B, B), bf16),
                pltpu.VMEM((H, B, 128), bf16),
                pltpu.VMEM((H, dh, B), bf16),
                pltpu.VMEM((2, XS, B, 128), bf16),
                pltpu.VMEM((Z + 1, dh, B), bf16),
                pltpu.VMEM((16, B), bf16),
                pltpu.VMEM((2, B, B // 2), bf16),
                pltpu.VMEM((dh, B), f32),
                pltpu.VMEM((2, dh, B), f32),
                pltpu.VMEM((8, B), f32),
                pltpu.VMEM((Z, dh + 8, B), f32),
                pltpu.VMEM((2 * H, 1, 128), f32),
                pltpu.VMEM((LAST + 1, T, dh // 2 + 8, 128), bf16),
                pltpu.VMEM((6 * T * H, dh // 2 + 8, 128), bf16),
                pltpu.VMEM((T * H, dh // 2, 128), f32),
                dma((2 * T,)),
                dma((2 * T,)),
                dma((T,)),
                dma((T,)),
                dma((16,)),
                dma((4 * XS,)),
                dma((3 * H,)),
                dma((Z + 1,)),
                dma((Z + 1,)),
                dma((Z,)),
                dma((Z,)),
                dma((1,)),
                dma((1,)),
                dma(((LAST + 1) * T,)),
                dma((6 * T * H,)),
                dma((7,)),
            ],
            compiler_params=pltpu.CompilerParams(collective_id=0, has_side_effects=True, vmem_limit_bytes=67043328),
        )(act, gain_in.reshape(1, D), wq, wk, wv, off, wo, gain_out.reshape(1, D))

    in_specs = (
        P(("sp", "tp"), None),
        P(),
        P(None, "tp"),
        P(None, "tp"),
        P(None, "tp"),
        P("tp"),
        P("tp", None),
        P(),
    )
    out_specs = P(("sp", "tp"), None)
    return jax.shard_map(local, mesh=mesh, in_specs=in_specs, out_specs=out_specs, check_vma=False)
```

```python
import functools

import jax
import jax.numpy as jnp
from jax import lax
from jax.experimental import pallas as pl
from jax.experimental.pallas import tpu as pltpu
from jax.sharding import PartitionSpec as P

epsilon = 1e-06
log2e = 1.4426950408889634
MESH = pl.DeviceIdType.MESH
f32 = jnp.float32
bf16 = jnp.bfloat16
XS = 4
ZMAX = 63.0
LAST = 11
FIRST = 6
SELF_TURN = 8


def scaled_rows(widened, row_gain):
    spread = jnp.mean(widened * widened, axis=-1, keepdims=True)
    return (widened * lax.rsqrt(spread + epsilon) * row_gain).astype(bf16)


def layer_kernel(
    S,
    T,
    H,
    dh,
    act_hbm,
    gain_in_hbm,
    wq_hbm,
    wk_hbm,
    wv_hbm,
    off,
    wo_hbm,
    gain_out_hbm,
    out,
    act,
    gain_in,
    gain_out,
    weights,
    rows_q,
    xg,
    wg,
    perm,
    kvb,
    qb,
    kvr,
    qr,
    offt,
    ws,
    acc,
    duo,
    factors,
    mbuf,
    offs,
    obuf,
    orecv,
    heads,
    x_send,
    x_recv,
    w_send,
    w_recv,
    kv_send,
    kv_recv,
    q_send,
    q_recv,
    f_send,
    m_send,
    m_recv,
    off_send,
    off_recv,
    o_send,
    o_recv,
    load,
):
    R = act.shape[0]
    B = R * T
    W = B // 2
    rows = wo_hbm.shape[0]
    Z = S // XS
    s = lax.axis_index("sp")
    t = lax.axis_index("tp")
    z, x = s // XS, s % XS
    y, c = t // 2, t % 2
    partner = y * 2 + 1 - c
    place_z = (z + 2) % Z
    g, hl = place_z // 4, place_z % 4
    kz = 2 * g + c
    head = 2 * H * y + hl
    home = hl // H == c

    def spot(group, local):
        return (4 * group + local + Z - 2) % Z

    Y = T // 2

    def remote(src, dst, send, recv, dev):
        return pltpu.make_async_remote_copy(
            src_ref=src, dst_ref=dst, send_sem=send, recv_sem=recv, device_id=dev, device_id_type=MESH
        )

    started = []

    def go(copy):
        copy.start()
        started.append(copy)
        return copy

    def xrow(index):
        return xg.at[pl.ds(pl.multiple_of(index * R, R), R)]

    def wrow(index):
        return wg.at[pl.ds(pl.multiple_of(index * rows, rows), rows)]

    def x_part(index, slot, dev, part):
        half = xg.at[pl.ds(pl.multiple_of(index * R + part * (R // 2), R // 2), R // 2)]
        return remote(half, half, x_send.at[2 * slot + part], x_recv.at[2 * index + part], (s, dev))

    def x_sends(index, *targets):
        for part in range(2):
            for slot, dev in targets:
                go(x_part(index, slot, dev, part))

    def x_take(index, *targets):
        for part in range(2):
            x_part(index, 0, partner, part).wait_recv()
            for slot, dev in targets:
                go(x_part(index, slot, dev, part))

    def w_copy(src, index, slot, dev):
        return remote(src, wrow(index), w_send.at[slot], w_recv.at[index], (s, dev))

    early = [
        pltpu.make_async_copy(act_hbm, act, load.at[4]),
        pltpu.make_async_copy(gain_in_hbm, gain_in, load.at[5]),
    ]
    for copy in early:
        copy.start()
    loads = [
        pltpu.make_async_copy(wk_hbm, weights.at[:, : H * dh], load.at[0]),
        pltpu.make_async_copy(wv_hbm, weights.at[:, H * dh : 2 * H * dh], load.at[1]),
        pltpu.make_async_copy(wq_hbm, weights.at[:, 2 * H * dh :], load.at[2]),
        pltpu.make_async_copy(wo_hbm, wrow(t), load.at[3]),
        pltpu.make_async_copy(gain_out_hbm, gain_out, load.at[6]),
    ]
    for copy in loads:
        copy.start()
    barrier = pltpu.get_barrier_semaphore()
    partners = [(s, (t + d) % T) for d in range(1, T)]
    for d in range(Z):
        for core in range(2):
            if d:
                partners.append(((z + d) % Z * XS + x, 2 * y + core))
            partners.append(((z + d) % Z * XS + XS - 1 - x, 2 * y + core))
    partners += [(z * XS + (x + 2) % XS, t), (z * XS + (XS - 1 - x + 2) % XS, t)]
    for other in partners:
        pl.semaphore_signal(barrier, inc=1, device_id=other, device_id_type=MESH)
    for copy in early:
        copy.wait()
    xg[pl.ds(pl.multiple_of(t * R, R), R)] = scaled_rows(act[...].astype(f32), gain_in[...])
    pl.semaphore_wait(barrier, len(partners))
    onward = (y + 1 + (Y - 2) * c) % Y
    behind = (y + Y - 1 - (Y - 2) * c) % Y
    across = (y + 2) % Y
    x_sends(t, (1, onward * 2 + c), (2, behind * 2 + c), (0, partner))

    token = lax.broadcasted_iota(jnp.int32, (B, B), 0)
    place = lax.broadcasted_iota(jnp.int32, (B, B), 1)
    perm[...] = (token == (place & (T - 1)) * R + R - 1 - (place >> (T.bit_length() - 1))).astype(f32).astype(bf16)
    for i in range(H):
        offs[H * c + i] = jnp.broadcast_to(off[i] * log2e, (1, 128)).astype(f32)
    mine = offs.at[pl.ds(H * c, H)]
    go(remote(mine, mine, off_send.at[0], off_recv.at[0], (s, partner)))
    def project(chip):
        rows_of = pl.ds(pl.multiple_of(chip * 2 * R, 2 * R), 2 * R)
        rows_q[rows_of] = jnp.dot(xg[rows_of], weights[...], preferred_element_type=f32)

    for copy in loads:
        copy.wait()
    x_take(partner)
    project(y)
    x_take(behind * 2 + c, (3, onward * 2 + c), (4, partner))
    x_take(onward * 2 + c, (5, partner))
    for chip in (behind, onward):
        x_take(chip * 2 + 1 - c)
        project(chip)
    x_take(across * 2 + c, (6, partner))
    for e in range(1, Y):
        go(w_copy(wrow(t), t, e, ((y + e) % Y) * 2 + c))
    x_take(across * 2 + 1 - c)
    project(across)
    keys = rows_q[:, : H * dh].astype(bf16).astype(f32)
    values = rows_q[:, H * dh : 2 * H * dh].astype(bf16).astype(f32)
    turned = jnp.concatenate([keys.T, values.T], axis=0).astype(bf16)
    placed = jnp.dot(turned, perm[...], preferred_element_type=f32)
    keys_placed = placed[: H * dh].T
    for i in range(H):
        cols = slice(i * dh, (i + 1) * dh)
        kvb[i, :W] = jnp.concatenate([keys_placed[:W, cols], keys_placed[W:, cols]], axis=1).astype(bf16)
        for part in range(4):
            piece = placed[(H + i) * dh : (H + i + 1) * dh, part * 128 : (part + 1) * 128]
            kvb[i, W + part * dh : W + (part + 1) * dh] = piece.astype(bf16)

    outer = jnp.minimum(z, Z - 1 - z)

    class Both:
        def __init__(self, parts):
            self.parts = parts

        def start(self):
            for part in self.parts:
                part.start()

        def wait_send(self):
            for part in self.parts:
                part.wait_send()

    def kv_part(src, row, col, slot, dev, part):
        rows_of = pl.ds(part * W, W)
        return remote(
            src.at[rows_of],
            kvr.at[row, col, rows_of],
            kv_send.at[2 * slot + part],
            kv_recv.at[2 * (row * XS + col) + part],
            dev,
        )

    def kv_copy(src, row, col, slot, dev):
        return Both([kv_part(src, row, col, slot, dev, part) for part in range(2)])

    def kv_first(i):
        zd = spot(outer // 2, H * c + i)
        stays = jnp.logical_and(zd == z, outer % 2 == c)
        return stays, kv_copy(kvb.at[i], z // (Z // 2), x, i, (zd * XS + x, 2 * y + outer % 2))

    for i in range(H):
        stays, copy = kv_first(i)

        @pl.when(stays)
        def _():
            kvr[z // (Z // 2), x] = kvb[i]

        @pl.when(jnp.logical_not(stays))
        def _():
            copy.start()

    queries = rows_q[:, 2 * H * dh :] * (dh ** (-0.5) * log2e)
    q_turned = queries.T.astype(bf16)
    for i in range(H):
        qb[i] = q_turned[i * dh : (i + 1) * dh]

    def q_first(i, group):
        zd = spot(group, H * c + i)
        stays = jnp.logical_and(zd == z, c == 0)
        copy = remote(qb.at[i], qr.at[z], q_send.at[i * 2 + group], q_recv.at[z], (zd * XS + x, 2 * y))
        return stays, z >= 2 * group, copy

    def q_extra(i):
        depth = Z - 1 - z
        zd = spot(depth // 2, H * c + i)
        dev = (zd * XS + XS - 1 - x, 2 * y + depth % 2)
        return remote(qb.at[i], qr.at[Z], q_send.at[2 * H + i], q_recv.at[Z], dev)

    def each_q(act_on):
        for group in (0, 1):
            for i in range(H):
                stays, wanted, copy = q_first(i, group)

                @pl.when(jnp.logical_and(wanted, jnp.logical_not(stays)))
                def _():
                    act_on(copy)

        @pl.when(z >= Z // 2)
        def _():
            for i in range(H):
                act_on(q_extra(i))

    for i in range(H):
        for group in (0, 1):
            stays, wanted, _ = q_first(i, group)

            @pl.when(jnp.logical_and(wanted, stays))
            def _():
                qr[z] = qb[i]


    def kv_wait(row, col):
        for part in range(2):
            kv_part(kvb.at[0], row, col, 0, (s, t), part).wait_recv()

    def q_forward(slot):
        return remote(qr.at[slot], qr.at[slot], f_send.at[slot], q_recv.at[slot], (s, partner))

    def q_wait(slot):
        local = jnp.logical_and(jnp.logical_and(slot == z, c == 0), hl // H == 0)

        @pl.when(jnp.logical_not(local))
        def _():
            q_forward(slot).wait_recv()

    def q_get(slot):
        q_wait(slot)

        @pl.when(c == 0)
        def _():
            q_forward(slot).start()

    x_on = (x + 1 + (XS - 2) * c) % XS
    x_back = (x + XS - 1 - (XS - 2) * c) % XS
    x_far = (x + 2) % XS

    def kv_spread(row):
        base = H + row * 3
        return (
            kv_copy(kvr.at[row, x], row, x, base, (z * XS + x_on, t)),
            kv_copy(kvr.at[row, x], row, x, base + 1, (z * XS + x_back, t)),
            kv_copy(kvr.at[row, x_back], row, x_back, base + 2, (z * XS + x_on, t)),
        )

    def kv_relay(row):
        local = jnp.logical_and(z == (kz if row == 0 else Z - 1 - kz), home)
        for part in range(2):

            @pl.when(jnp.logical_not(local))
            def _():
                kv_part(kvb.at[0], row, x, 0, (s, t), part).wait_recv()

            for copy in kv_spread(row)[:2]:
                copy.parts[part].start()

    kv_relay(0)
    each_q(lambda copy: copy.start())
    for part in range(2):
        kv_part(kvb.at[0], 0, x_back, 0, (s, t), part).wait_recv()
        kv_spread(0)[2].parts[part].start()
    kv_relay(1)

    theirs = offs.at[pl.ds(H * (1 - c), H)]
    remote(theirs, theirs, off_send.at[0], off_recv.at[0], (s, partner)).wait_recv()
    whole = jnp.concatenate([jnp.broadcast_to(offs[hl], (16, 128))] * (B // 128), axis=1)
    high = whole.astype(bf16).astype(f32)
    middle = (whole - high).astype(bf16).astype(f32)
    low = whole - high - middle
    part_row = lax.broadcasted_iota(jnp.int32, (16, B), 0)
    offt[...] = jnp.where(
        part_row == 0, high, jnp.where(part_row == 1, middle, jnp.where(part_row == 2, low, 0.0))
    ).astype(bf16)

    lane = lax.broadcasted_iota(jnp.int32, (16, 128), 1)
    ones = (lane < 3).astype(f32).astype(bf16)
    zeros = jnp.zeros((dh, W), bf16)
    pad = jnp.zeros((112, W), bf16)

    def weigh(row, col, slot, j, masked):
        sl = slice(j * W, (j + 1) * W)
        run = jnp.ones((8, W), f32)
        if masked:
            ahead = (
                lax.broadcasted_iota(jnp.int32, (8, W), 1)
                + j * W
                - R * lax.broadcasted_iota(jnp.int32, (8, W), 0)
            )
        lhs = jnp.concatenate([kvr[row, col, :W], jnp.tile(ones, (W // 16, 1))], axis=1)
        for part in (0, 1):
            q = qr[slot, :, sl]
            stack = [q, zeros] if part == 0 else [zeros, q]
            rhs = jnp.concatenate(stack + [offt[:, sl], pad], axis=0)
            for v in range(0, W // 8, 2):
                if v % 8 == 0:
                    chunk = jnp.dot(lhs[8 * v : 8 * v + 64], rhs, preferred_element_type=f32)
                    score = [None] * v + [jnp.minimum(chunk[8 * w : 8 * w + 8], ZMAX) for w in range(8)]
                e0 = jnp.exp2(score[v])
                e1 = jnp.exp2(score[v + 1])
                if masked:
                    place_v = part * (W // 8) + v
                    e0 = jnp.where(ahead > R - 1 - place_v, e0, 0.0)
                    e1 = jnp.where(ahead > R - 2 - place_v, e1, 0.0)
                u0, u1 = 1.0 + e0, 1.0 + e1
                left = run * (1.0 / (u0 * u1))
                first = e0 * (u1 * left)
                second = e1 * left
                run = left
                base = part * W + 8 * v
                ws[j, base : base + 16] = jnp.concatenate([first, second], axis=0).astype(bf16)
        later = [None] * 8
        total = jnp.ones((1, W), f32)
        for i in range(7, -1, -1):
            later[i] = total
            total = total * run[i : i + 1]
        return jnp.concatenate(later + later, axis=0).astype(bf16), total

    def gather(row, col, j, later, total, first):
        sl = slice(j * W, (j + 1) * W)
        weight = (ws[j].reshape(B // 16, 16, W) * later[None]).reshape(B, W)
        vt = jnp.concatenate([kvr[row, col, W + p * dh : W + (p + 1) * dh] for p in range(4)], axis=1)
        part = jnp.dot(vt, weight, preferred_element_type=f32)
        if first is None:
            duo[row, :, sl] = duo[row, :, sl] * total + part
        else:
            acc[:, sl] = part if first else acc[:, sl] * total + part

    def o_copies(u, r, e, dst, dev):
        return (
            remote(obuf.at[u, r], orecv.at[dst], o_send.at[u * T + e], o_recv.at[dst], dev),
        )

    def send_out(u, slot, block, kept):
        lanes = lax.broadcasted_iota(jnp.int32, (dh // 2, 128), 1) < dh
        top = lax.broadcasted_iota(jnp.int32, (8, 128), 0) == 0
        lanes_t = lax.broadcasted_iota(jnp.int32, (8, 128), 1) < dh
        for g in range(T // 2):
            cols = slice(g * 128, (g + 1) * 128)
            a, b = acc[: dh // 2, cols], acc[dh // 2 :, cols]
            ar, br = pltpu.roll(a, dh, 1), pltpu.roll(b, dh, 1)
            j, inner = g * 128 // W, g * 128 % W
            tt = jnp.broadcast_to(kept[j][:, inner : inner + 128], (8, 128))
            tr = pltpu.roll(tt, dh, 1)
            for odd in range(2):
                body = jnp.where(lanes, ar, b) if odd else jnp.where(lanes, a, br)
                fac = jnp.where(lanes_t, tr, tt) if odd else jnp.where(lanes_t, tt, tr)
                fac_high = fac.astype(bf16).astype(f32)
                tail = jnp.where(top, fac_high, fac - fac_high)
                obuf[u, 2 * g + odd] = jnp.concatenate([body, tail], axis=0).astype(bf16)
        dst = slot * T * H + head
        for e in range(1, T):
            r = (t + e) % T
            for copy in o_copies(u, r, e, dst, (block, r)):
                copy.start()

        @pl.when(block != s)
        def _():
            for copy in o_copies(u, t, 0, dst, (block, t)):
                copy.start()

        @pl.when(block == s)
        def _():
            orecv[dst] = obuf[u, t]

    def merge(slot, kept):
        remote(mbuf.at[slot], mbuf.at[slot], m_send.at[slot], m_recv.at[slot], (s, t)).wait_recv()
        out_kept = []
        for j in range(2):
            sl = slice(j * W, (j + 1) * W)
            acc[:, sl] = mbuf[slot, :dh, sl] * kept[j] + acc[:, sl]
            out_kept.append(mbuf[slot, dh : dh + 1, sl] * kept[j])
        return out_kept

    def self_units():
        slots = (kz, Z)
        q_wait(slots[0])
        q_wait(slots[1])
        ends = (x, XS - 1 - x)
        duo[...] = jnp.zeros((2, dh, B), f32)
        one = jnp.ones((1, W), f32)
        kept = [[one, one], [one, one]]
        waiting = None
        for p in range(XS + 1):
            if p < XS - 1:
                row = jnp.where(p < x, 0, 1)
                col = jnp.where(p < x, p, p - x)
                slot = jnp.where(p < x, kz, Z)
            else:
                row = p - XS + 1
                col, slot = ends[row], slots[row]
            for j in range(2):
                later, total = weigh(row, col, slot, j, p >= XS - 1)
                if waiting is not None:
                    gather(*waiting)
                waiting = (row, col, j, later, total, None)
                for k in range(2):
                    kept[k][j] = kept[k][j] * (jnp.where(row == k, total, 1.0) if p < XS - 1 else total if row == k else one)
        gather(*waiting)

        acc[...] = duo[0]

        @pl.when(c == 0)
        def _():
            send_out(kz, g, kz * XS + x, kept[0])

        @pl.when(c == 1)
        def _():
            send_out(kz, g, kz * XS + x, merge(kz, kept[0]))

        acc[...] = duo[1]
        send_out(LAST, Z - 3 - kz, (Z - 1 - kz) * XS + XS - 1 - x, kept[1])

    def full(turn, unused):
        low_row = jnp.logical_or(turn <= FIRST, turn > FIRST + 3)
        far = jnp.where(turn < FIRST, Z - 1 - turn, Z + 3 - turn)
        hop = (far + 1) // 2
        near = jnp.where(far % 2 == 1, z + hop, z + 2 * Z - hop) % Z
        shared = 2 * g + 1
        zq = jnp.where(turn == FIRST, shared, jnp.where(low_row, near, Z + FIRST - turn))
        row = jnp.where(low_row, 0, 1)
        low_valid = jnp.where(turn == FIRST, c == 0, zq > shared)
        valid = jnp.where(low_row, low_valid, zq + kz >= Z)

        @pl.when(turn == 1)
        def _():
            kv_wait(1, x_back)
            kv_spread(1)[2].start()

        @pl.when(turn == FIRST)
        def _():
            for step in (0, 1):
                close = (z + step) % Z

                @pl.when(close >= Z - 1 - 2 * g)
                def _():
                    q_get(close)

        @pl.when(turn == FIRST + 1)
        def _():
            kv_wait(1, x_on)
            kv_wait(1, x_far)

        @pl.when(turn == SELF_TURN)
        def _():
            self_units()

        @pl.when(valid)
        def _():
            @pl.when(jnp.logical_and(low_row, jnp.logical_or(turn <= FIRST, zq < Z - 1 - 2 * g)))
            def _():
                q_get(zq)

            kept = [None, None]
            waiting = None
            for col in range(XS):
                for j in range(2):
                    later, total = weigh(row, col, zq, j, False)
                    if waiting is not None:
                        gather(*waiting)
                    waiting = (row, col, j, later, total, col == 0)
                    kept[j] = total if col == 0 else kept[j] * total
            gather(*waiting)
            for j in range(2):
                factors[:, j * W : (j + 1) * W] = jnp.broadcast_to(kept[j], (8, W))

            handed = jnp.logical_and(low_row, c == 0)

            @pl.when(handed)
            def _():
                mbuf[zq, :dh] = acc[...]
                mbuf[zq, dh:] = factors[...]
                remote(mbuf.at[zq], mbuf.at[zq], m_send.at[zq], m_recv.at[zq], (s, partner)).start()

            @pl.when(jnp.logical_and(low_row, c == 1))
            def _():
                for j, both in enumerate(merge(zq, kept)):
                    factors[:, j * W : (j + 1) * W] = jnp.broadcast_to(both, (8, W))

            @pl.when(jnp.logical_not(handed))
            def _():
                u = jnp.where(low_row, zq, zq + 3)
                slot = jnp.where(low_row, g, Z - 3 - kz)
                send_out(u, slot, zq * XS + x, [factors[:1, j * W : (j + 1) * W] for j in range(2)])

        return unused

    go(w_copy(wrow(t), t, 0, partner))
    for e in range(1, Y):
        came = ((y + e) % Y) * 2 + c
        w_copy(wrow(t), came, 0, partner).wait_recv()
        go(w_copy(wrow(came), came, Y + e - 1, partner))
    kv_wait(0, x_on)
    kv_wait(0, x_far)
    lax.fori_loop(0, Z + 4, full, 0)
    w_copy(wrow(t), partner, 0, partner).wait_recv()
    for e in range(1, Y):
        w_copy(wrow(t), ((y + e) % Y) * 2 + 1 - c, 0, partner).wait_recv()

    for hh in range(T * H):
        heads[hh] = jnp.zeros((dh // 2, 128), f32)

    def made_here(slot):
        low_made = jnp.where(c == 1, z >= kz, z == kz)
        high_made = jnp.logical_and(slot == Z - 3 - kz, z + kz >= Z)
        return jnp.logical_or(jnp.logical_and(slot == g, low_made), high_made)

    def combine(r, unused):
        for hh in range(T * H):

            @pl.when(jnp.logical_not(jnp.logical_and(hh == head, made_here(r))))
            def _():
                e = r * T * H + hh
                for copy in o_copies(0, 0, 0, e, (s, t)):
                    copy.wait_recv()

        for hh in range(T * H):
            got = orecv[r * T * H + hh].astype(f32)
            fac = got[dh // 2 : dh // 2 + 1] + got[dh // 2 + 1 : dh // 2 + 2]
            heads[hh] = heads[hh] * fac + got[: dh // 2]
        return unused

    slots = jnp.where(z < 2, 1, jnp.where(z < 4, 2, z - 1))
    lax.fori_loop(0, slots, combine, 0)

    lhs, rhs = [], []
    for q in range(T * H // 4):
        both = jnp.concatenate([heads[4 * q + a] for a in range(4)], axis=0).T
        for e in range(2):
            lhs.append(both[e * dh : (e + 1) * dh].astype(bf16))
            for a in range(4):
                base = (4 * q + a) * dh + e * (dh // 2)
                rhs.append(wg[base : base + dh // 2])
    projected = jnp.dot(
        jnp.concatenate(lhs, axis=1), jnp.concatenate(rhs, axis=0), preferred_element_type=f32
    )
    out[...] = scaled_rows(projected, gain_out[...])

    for copy in started:
        copy.wait_send()
    each_q(lambda copy: copy.wait_send())

    for i in range(H):
        stays, copy = kv_first(i)

        @pl.when(jnp.logical_not(stays))
        def _():
            copy.wait_send()

    for row in range(2):
        for copy in kv_spread(row):
            copy.wait_send()

    def sent(u, valid, block):
        @pl.when(valid)
        def _():
            for e in range(1, T):
                for copy in o_copies(u, 0, e, 0, (s, t)):
                    copy.wait_send()

            @pl.when(block != s)
            def _():
                for copy in o_copies(u, 0, 0, 0, (s, t)):
                    copy.wait_send()

    def sent_low(zq, unused):
        sent(zq, jnp.logical_or(zq == kz, jnp.logical_and(zq > kz, c == 1)), zq * XS + x)

        @pl.when(jnp.logical_and(zq > kz, c == 0))
        def _():
            q_forward(zq).wait_send()
            remote(mbuf.at[zq], mbuf.at[zq], m_send.at[zq], m_recv.at[zq], (s, partner)).wait_send()

        return unused

    def sent_high(zq, unused):
        sent(zq + 3, zq + kz >= Z, zq * XS + x)
        return unused

    lax.fori_loop(0, Z, sent_low, 0)
    lax.fori_loop(5, Z, sent_high, 0)
    sent(LAST, z >= 0, (Z - 1 - kz) * XS + XS - 1 - x)


def solution(mesh):
    S, T = mesh.shape["sp"], mesh.shape["tp"]

    def local(act, gain_in, wq, wk, wv, off, wo, gain_out):
        R, D = act.shape
        H = off.shape[0]
        dh = wq.shape[1] // H
        B = R * T
        Z = S // XS
        vmem = pl.BlockSpec(memory_space=pltpu.VMEM)
        hbm = pl.BlockSpec(memory_space=pl.ANY)
        smem = pl.BlockSpec(memory_space=pltpu.SMEM)
        dma = pltpu.SemaphoreType.DMA
        return pl.pallas_call(
            functools.partial(layer_kernel, S, T, H, dh),
            out_shape=jax.ShapeDtypeStruct((R, D), bf16),
            in_specs=[hbm, hbm, hbm, hbm, hbm, smem, hbm, hbm],
            out_specs=vmem,
            scratch_shapes=[
                pltpu.VMEM((R, D), bf16),
                pltpu.VMEM((1, D), f32),
                pltpu.VMEM((1, D), f32),
                pltpu.VMEM((D, 3 * H * dh), bf16),
                pltpu.VMEM((B, 3 * H * dh), f32),
                pltpu.VMEM((B, D), bf16),
                pltpu.VMEM((wo.shape[0] * T, D), bf16),
                pltpu.VMEM((B, B), bf16),
                pltpu.VMEM((H, B, 128), bf16),
                pltpu.VMEM((H, dh, B), bf16),
                pltpu.VMEM((2, XS, B, 128), bf16),
                pltpu.VMEM((Z + 1, dh, B), bf16),
                pltpu.VMEM((16, B), bf16),
                pltpu.VMEM((2, B, B // 2), bf16),
                pltpu.VMEM((dh, B), f32),
                pltpu.VMEM((2, dh, B), f32),
                pltpu.VMEM((8, B), f32),
                pltpu.VMEM((Z, dh + 8, B), f32),
                pltpu.VMEM((2 * H, 1, 128), f32),
                pltpu.VMEM((LAST + 1, T, dh // 2 + 8, 128), bf16),
                pltpu.VMEM((6 * T * H, dh // 2 + 8, 128), bf16),
                pltpu.VMEM((T * H, dh // 2, 128), f32),
                dma((2 * T,)),
                dma((2 * T,)),
                dma((T,)),
                dma((T,)),
                dma((16,)),
                dma((4 * XS,)),
                dma((3 * H,)),
                dma((Z + 1,)),
                dma((Z + 1,)),
                dma((Z,)),
                dma((Z,)),
                dma((1,)),
                dma((1,)),
                dma(((LAST + 1) * T,)),
                dma((6 * T * H,)),
                dma((7,)),
            ],
            compiler_params=pltpu.CompilerParams(collective_id=0, has_side_effects=True, vmem_limit_bytes=67043328),
        )(act, gain_in.reshape(1, D), wq, wk, wv, off, wo, gain_out.reshape(1, D))

    in_specs = (
        P(("sp", "tp"), None),
        P(),
        P(None, "tp"),
        P(None, "tp"),
        P(None, "tp"),
        P("tp"),
        P("tp", None),
        P(),
    )
    out_specs = P(("sp", "tp"), None)
    return jax.shard_map(local, mesh=mesh, in_specs=in_specs, out_specs=out_specs, check_vma=False)
```
